32 devices in a mesh: sp: 16 (over z, y, x), tp: 2 (over core).
Axes of the slice: x: 2, y: 2, z: 4, core: 2. Of those that a mesh axis runs over, the one named last changes fastest.
Arguments:
- latent: bfloat16 [4096, 2048], P(('sp', 'tp')), may hold values from -6 to 6
- context: bfloat16 [512, 2048], P('sp'), may hold values from -6 to 6
- condition: float32 [2048], P('tp'), may hold values from -6 to 6
- context_condition: float32 [2048], P('tp'), may hold values from -6 to 6
- modulation_weight: bfloat16 [2048, 6144], P('tp', 'sp'), may hold values from -0.125 to 0.125
- query_first: bfloat16 [2048, 512], P(None, 'tp'), may hold values from -1 to 1
- query_second: bfloat16 [2048, 512], P(None, 'tp'), may hold values from -1 to 1
- key_first: bfloat16 [2048, 512], P(None, 'tp'), may hold values from -1 to 1
- key_second: bfloat16 [2048, 512], P(None, 'tp'), may hold values from -1 to 1
- value_weight: bfloat16 [2048, 1024], P(None, 'tp'), may hold values from -0.125 to 0.125
- lambda_head: float32 [8], P('tp'), may hold values from 0.3 to 0.8
- context_score_boost: float32 [8], P('tp'), may hold values from 1.5 to 3
- head_gain: float32 [128], replicated, may hold values from 0.1 to 1.9
- output_weight: bfloat16 [1024, 2048], P('tp'), may hold values from -0.1875 to 0.1875
Outputs:
- updated: bfloat16 [4096, 2048], P(('sp', 'tp'))
The draws below stay inside these ranges and needn't reach their ends.
All inputs are finite; a program needn't handle non-finite values.
Results may differ from the reference program's by a relative error of at most 0.0095.
Values may be sent and summed in bfloat16 or wider, within the bound.
A program may use at most 64 MiB of HBM per device.

```python
import jax
import jax.numpy as jnp
from jax import lax

D = 2048
HEADS = 8
HEAD_DIM = 64
VALUE_DIM = 128
GRID_W = 64
CTX = 512
TOKENS = 4096


def drawn_weight(key, stream):
    jitter = jax.random.normal(jax.random.fold_in(key, stream), (D, HEADS * HEAD_DIM), jnp.float32)
    return jnp.clip(jitter, -6.0, 6.0) * D ** (-0.5)


def draw_latent(key, part):
    jitter = jax.random.normal(jax.random.fold_in(key, 21), (TOKENS, D), jnp.float32)
    result = jnp.clip(jitter, -6.0, 6.0)
    return result.astype(jnp.bfloat16)


def draw_query_first(key, part):
    result = drawn_weight(key, 31)
    return jnp.clip(result, -1.0, 1.0).astype(jnp.bfloat16)


def draw_key_first(key, part):
    result = drawn_weight(key, 32)
    return jnp.clip(result, -1.0, 1.0).astype(jnp.bfloat16)


def draw_query_second(key, part):
    result = drawn_weight(key, 33)
    return jnp.clip(result, -1.0, 1.0).astype(jnp.bfloat16)


def draw_key_second(key, part):
    result = drawn_weight(key, 34)
    return jnp.clip(result, -1.0, 1.0).astype(jnp.bfloat16)


def shard_levels(stream_key, extent, cuts, smallest, largest):
    def one(position, shards_of):
        draws = jax.random.uniform(jax.random.fold_in(jax.random.fold_in(stream_key, 6), position), (shards_of,), jnp.float32, smallest / len(cuts), largest / len(cuts))
        return jnp.repeat(jnp.exp(draws), extent[position] // shards_of).reshape((-1,) + (1,) * (len(extent) - position - 1))

    factor_of = one(*cuts[0])
    for cut in cuts[1:]:
        factor_of = factor_of * one(*cut)
    return factor_of


def gaussian(stream_key, dims, scale, limit, split=(), kind=jnp.bfloat16):
    loudness = shard_levels(stream_key, dims, split, -0.22, 0.18) if split else 1.0
    values = jax.random.normal(stream_key, dims, jnp.float32) * scale * loudness
    return jnp.minimum(jnp.maximum(values, -limit), limit).astype(kind)


def setup_inputs(seed: int = 0) -> dict:
    key_list = jax.random.split(jax.random.key(seed), 15)
    latent = draw_latent(jax.random.fold_in(key_list[14], 71), 0)
    context = gaussian(key_list[1], (CTX, D), 1.0, 6.0, ((0, 16),))
    condition = gaussian(key_list[2], (D,), 1.0, 6.0, ((0, 2),), jnp.float32)
    context_condition = gaussian(key_list[3], (D,), 1.0, 6.0, ((0, 2),), jnp.float32)
    modulation_weight = gaussian(key_list[4], (D, 3 * D), D ** -0.5, 0.125, ((0, 2), (1, 16)))
    query_first = draw_query_first(jax.random.fold_in(key_list[14], 71), 0)
    query_second = draw_query_second(jax.random.fold_in(key_list[14], 71), 0)
    key_first = draw_key_first(jax.random.fold_in(key_list[14], 71), 0)
    key_second = draw_key_second(jax.random.fold_in(key_list[14], 71), 0)
    value_weight = gaussian(key_list[9], (D, HEADS * VALUE_DIM), D ** -0.5, 0.125, ((1, 2),))
    lambda_head = jnp.clip(0.3 + 0.5 * jax.random.uniform(key_list[10], (HEADS,), jnp.float32) ** shard_levels(key_list[10], (HEADS,), ((0, 2),), -0.2, 0.2), 0.3, 0.8)
    context_score_boost = jnp.clip(1.5 + 1.5 * jax.random.uniform(key_list[11], (HEADS,), jnp.float32) ** shard_levels(key_list[11], (HEADS,), ((0, 2),), -0.2, 0.2), 1.5, 3.0)
    head_gain = jnp.clip(1.0 + 0.18 * jax.random.normal(key_list[12], (VALUE_DIM,), jnp.float32), 0.1, 1.9)
    output_weight = gaussian(key_list[13], (HEADS * VALUE_DIM, D), (HEADS * VALUE_DIM) ** -0.5, 0.1875, ((0, 2),))
    return {"latent": latent, "context": context, "condition": condition, "context_condition": context_condition, "modulation_weight": modulation_weight, "query_first": query_first, "query_second": query_second, "key_first": key_first, "key_second": key_second, "value_weight": value_weight, "lambda_head": lambda_head, "context_score_boost": context_score_boost, "head_gain": head_gain, "output_weight": output_weight}


EPSILON = 1e-06
THETA = 10000.0

def norm_rows(rows):
    values = rows.astype(jnp.float32)
    return values * lax.rsqrt(lax.optimization_barrier(jnp.mean(values * values, axis=-1, keepdims=True)) + EPSILON)

def rotate_pairs(values, positions):
    half = values.shape[-1] // 2
    quarter = half // 2
    reciprocal_norm = THETA ** (-jnp.arange(quarter, dtype=jnp.float32) / quarter)

    def turn(part, where):
        angle = where.astype(jnp.float32)[:, None] * reciprocal_norm[None, :]
        cosine_table = jnp.concatenate([jnp.cos(angle)] * 2, -1)[:, None, :]
        sine = jnp.concatenate([jnp.sin(angle)] * 2, -1)[:, None, :]
        flipped = jnp.concatenate([-part[..., quarter:], part[..., :quarter]], -1)
        return part * cosine_table + flipped * sine
    grid_row = positions // GRID_W
    grid_col = positions % GRID_W
    return jnp.concatenate([turn(values[..., :half], grid_row), turn(values[..., half:], grid_col)], -1)

def project(rows, weight):
    return jnp.dot(rows, weight, preferred_element_type=jnp.float32).reshape(rows.shape[0], HEADS, -1)

def reference(latent, context, condition, context_condition, modulation_weight, query_first, query_second, key_first, key_second, value_weight, lambda_head, context_score_boost, head_gain, output_weight):
    signal = jax.nn.silu(jnp.stack([condition, context_condition])).astype(jnp.bfloat16)
    modulation = jnp.dot(signal, modulation_weight, preferred_element_type=jnp.float32)
    shift = modulation[:, :D]
    scale = modulation[:, D:2 * D]
    gate = modulation[:, 2 * D:]
    h_latent = (norm_rows(latent) * (1.0 + scale[0]) + shift[0]).astype(jnp.bfloat16)
    h_context = (norm_rows(context) * (1.0 + scale[1]) + shift[1]).astype(jnp.bfloat16)
    positions = jnp.arange(TOKENS, dtype=jnp.int32)
    queries_one = rotate_pairs(project(h_latent, query_first), positions).astype(jnp.bfloat16)
    queries_two = rotate_pairs(project(h_latent, query_second), positions).astype(jnp.bfloat16)
    latent_one = rotate_pairs(project(h_latent, key_first), positions).astype(jnp.bfloat16)
    latent_two = rotate_pairs(project(h_latent, key_second), positions).astype(jnp.bfloat16)
    latent_values = project(h_latent, value_weight).astype(jnp.bfloat16)
    context_one = project(h_context, key_first).astype(jnp.bfloat16)
    context_two = project(h_context, key_second).astype(jnp.bfloat16)
    context_values = project(h_context, value_weight).astype(jnp.bfloat16)
    keys_one = jnp.concatenate([context_one, latent_one], 0).astype(jnp.float32)
    keys_two = jnp.concatenate([context_two, latent_two], 0).astype(jnp.float32)
    values_all = jnp.concatenate([context_values, latent_values], 0).astype(jnp.float32)
    lift = jnp.concatenate([jnp.broadcast_to(context_score_boost[:, None], (HEADS, CTX)), jnp.zeros((HEADS, TOKENS), jnp.float32)], 1)[:, None, :]
    block = 256 if TOKENS % 256 == 0 else TOKENS
    count = TOKENS // block

    def attend(pair):
        query_one, query_two = pair
        outcomes = []
        for query, keys in ((query_one, keys_one), (query_two, keys_two)):
            scores = jnp.einsum('qhd,khd->hqk', query.astype(jnp.float32), keys) * HEAD_DIM ** (-0.5) + lift
            highest = lax.optimization_barrier(jnp.max(scores, axis=-1, keepdims=True))
            exp_weights = jnp.exp(scores - highest)
            totals = lax.optimization_barrier(jnp.sum(exp_weights, axis=-1))
            rounded = lax.optimization_barrier(exp_weights.astype(jnp.bfloat16))
            weighted = jnp.einsum('hqk,khe->qhe', rounded.astype(jnp.float32), values_all)
            outcomes.append(weighted / jnp.transpose(totals)[:, :, None])
        return outcomes[0] - lambda_head[None, :, None] * outcomes[1]
    blocks = (queries_one.reshape(count, block, HEADS, HEAD_DIM), queries_two.reshape(count, block, HEADS, HEAD_DIM))
    mixed = lax.map(attend, blocks).reshape(TOKENS, HEADS, VALUE_DIM)
    normed = mixed * lax.rsqrt(lax.optimization_barrier(jnp.mean(mixed * mixed, axis=-1, keepdims=True)) + EPSILON) * head_gain
    heads_out = normed.astype(jnp.bfloat16).reshape(TOKENS, HEADS * VALUE_DIM)
    branch = jnp.dot(heads_out, output_weight, preferred_element_type=jnp.float32)
    return (latent.astype(jnp.float32) + gate[0] * branch).astype(jnp.bfloat16)
```

```python
import functools
import math

import jax
import jax.numpy as jnp
import numpy as np
from jax import lax
from jax.experimental import pallas as pl
from jax.experimental.pallas import tpu as pltpu
from jax.sharding import PartitionSpec as P

HEAD_DIM = 64
VALUE_DIM = 128
GRID_W = 64
EPSILON = 1e-06
THETA = 10000.0
NEGATIVE = -1e30
LOG2E = math.log2(math.e)
MESH = pl.DeviceIdType.MESH
BF16 = jnp.bfloat16
F32 = jnp.float32
LANES = 128


def rotation_tables(grid_rows):
    half = HEAD_DIM // 2
    quarter = half // 2
    lane = np.arange(LANES) % HEAD_DIM
    rate = (THETA ** (-(lane % quarter) / quarter)).astype(np.float32)
    sign = np.where(lane % half < quarter, -1.0, 1.0)
    tables = []
    for count, mask in ((grid_rows, lane < half), (GRID_W, lane >= half)):
        angle = np.arange(count, dtype=np.float32)[:, None] * rate[None, :]
        for table in (np.cos(angle), np.sin(angle) * sign):
            tables.append(np.where(mask, table, 0.0).astype(np.float32))
    return tables


def rotate(x, cosine, sine):
    quarter = HEAD_DIM // 4
    lane = lax.broadcasted_iota(jnp.int32, x.shape, 1)
    ahead = pltpu.roll(x, LANES - quarter, 1)
    behind = pltpu.roll(x, quarter, 1)
    flipped = jnp.where(lane % (2 * quarter) < quarter, ahead, behind)
    return x * cosine + flipped * sine


def normed_rows(rows):
    v = rows.astype(F32)
    return v * lax.rsqrt(jnp.mean(v * v, axis=-1, keepdims=True) + EPSILON)


def flip(v, k, span):
    out = 0
    bit = 1
    while bit < span:
        out = out + bit * ((v // bit + k // bit) % 2)
        bit *= 2
    return out


def kernel(
    dims,
    lat_hbm, ctx_hbm, cond_hbm, ccond_hbm, modw_hbm,
    wq1_hbm, wq2_hbm, wk1_hbm, wk2_hbm, wv_hbm,
    lam_ref, boost_ref, gain_ref, wo_hbm, crow_ref, srow_ref, ccol_ref, scol_ref,
    out_ref,
    wq1, wq2, wk1, wk2, wv, wo,
    ctx, cond, modw, cos_ref, sin_ref, mp, modall, modrow, lat, nrm, h,
    qs, kvs, q, kv, vts, mx, acc, ho, hr, lb,
    wsem, isem, mp_s, mp_r, ma_s, ma_r, lt_s, lt_r, lb_s, lb_r, wo_s, wo_r,
    q_s, q_r, kz_s, kv_r, fx_s, fd_s, ho_s, ho_r,
):
    S, T, G, R, A, B, Cr, cw = dims
    P = T * G
    near = max(P // 2, 1)
    s, t = lax.axis_index("sp"), lax.axis_index("tp")
    p0, r = s // R, s % R
    a0, b0 = s // B, s % B
    prim, hown = p0 // G, p0 % G
    _, rows, D = lat.shape
    Lr = rows * T
    Cp = ctx.shape[0]

    def remote(src, dst, send, recv, sp, tp):
        return pltpu.make_async_remote_copy(
            src_ref=src, dst_ref=dst, send_sem=send, recv_sem=recv,
            device_id=(sp, tp), device_id_type=MESH,
        )

    f0 = b0 * T + t
    FB = B * T

    def plane(j):
        f = (f0 + j) % FB
        return f, a0 * B + f // T, f % T

    barrier = pltpu.get_barrier_semaphore()
    for j in range(1, FB):
        _, sp, tp = plane(j)
        pl.semaphore_signal(barrier, inc=1, device_id=(sp, tp), device_id_type=MESH)
    for i in range(1, A):
        pl.semaphore_signal(
            barrier, inc=1, device_id=((a0 + i) % A * B + b0, t), device_id_type=MESH
        )

    inputs = [
        pltpu.make_async_copy(a, b, isem.at[i])
        for i, (a, b) in enumerate(
            [(cond_hbm, cond.at[0:1]), (ccond_hbm, cond.at[1:2]), (modw_hbm, modw),
             (lat_hbm, lat.at[t]), (ctx_hbm, ctx)]
        )
    ]
    for load in inputs:
        load.start()
    loads = [
        pltpu.make_async_copy(a, b, wsem.at[i])
        for i, (a, b) in enumerate(
            [(wk1_hbm, wk1), (wk2_hbm, wk2), (wv_hbm, wv), (wq1_hbm, wq1), (wq2_hbm, wq2), (wo_hbm, wo.at[t])]
        )
    ]
    for load in loads:
        load.start()

    for i in range(G):
        lb[t, i : i + 1, :] = jnp.full((1, LANES), lam_ref[i], F32)
        lb[t, G + i : G + i + 1, :] = jnp.full((1, LANES), boost_ref[i] * LOG2E, F32)

    for i in range(3):
        inputs[i].wait()
    v = cond[...]
    sig = v / (1.0 + jnp.exp(-v))
    mp[f0] = jnp.dot(sig.astype(BF16), modw[...], preferred_element_type=F32)
    for i in range(3, 5):
        inputs[i].wait()

    pl.semaphore_wait(barrier, FB - 1 + A - 1)

    def mp_copy(j):
        _, sp, tp = plane(j)
        return remote(mp.at[f0], mp.at[f0], mp_s.at[j], mp_r.at[f0], sp, tp)

    def lat_copy(i):
        return remote(lat.at[t], lat.at[t], lt_s.at[i], lt_r.at[t], s, (t + i) % T)

    def lb_copy(i):
        return remote(lb.at[t], lb.at[t], lb_s.at[i], lb_r.at[t], s, (t + i) % T)

    def wo_copy(i):
        return remote(wo.at[t], wo.at[t], wo_s.at[i], wo_r.at[t], s, (t + i) % T)

    def from_core(buf, recv, i):
        o = (t + i) % T
        remote(buf.at[o], buf.at[o], lt_s.at[i], recv.at[o], s, o).wait_recv()

    for j in range(1, FB):
        mp_copy(j).start()
    for i in range(1, T):
        lat_copy(i).start()
        lb_copy(i).start()

    for i in range(Lr // GRID_W):
        span, at = slice(i * GRID_W, (i + 1) * GRID_W), pl.ds(s * (Lr // GRID_W) + i, 1)
        cos_ref[span, :] = ccol_ref[...] + crow_ref[at, :]
        sin_ref[span, :] = scol_ref[...] + srow_ref[at, :]
    cos_ref[Lr:, :] = jnp.ones((Cp, LANES), F32)
    sin_ref[Lr:, :] = jnp.zeros((Cp, LANES), F32)

    for j in range(1, FB):
        f, sp, tp = plane(j)
        remote(mp.at[f], mp.at[f], mp_s.at[j], mp_r.at[f], sp, tp).wait_recv()
    for b in range(B):
        total = mp[b * T]
        for i in range(1, T):
            total = total + mp[b * T + i]
        modall[a0, b] = total

    def mod_copy(i, src):
        return remote(
            modall.at[src], modall.at[src], ma_s.at[i], ma_r.at[src], (a0 + i) % A * B + b0, t
        )

    for i in range(1, A):
        mod_copy(i, a0).start()

    step = math.gcd(rows, 32)

    def norm_lat(i):
        @pl.loop(0, rows // step)
        def _(j):
            at = pl.multiple_of(j * step, step)
            nrm[pl.ds(i * rows + at, step), :] = normed_rows(lat[i, pl.ds(at, step), :])

    nrm[Lr:, :] = normed_rows(ctx[...])
    norm_lat(t)
    for i in range(1, T):
        from_core(lat, lt_r, i)
        norm_lat((t + i) % T)

    for i in range(1, A):
        mod_copy(i, (a0 + i) % A).wait_recv()
    for a in range(A):
        for b in range(B):
            i = a * B + b
            modrow[:, i * cw : (i + 1) * cw] = modall[a, b][:, :cw]

    @pl.loop(0, Lr // step)
    def _(j):
        at = pl.ds(pl.multiple_of(j * step, step), step)
        h[at, :] = (nrm[at, :] * (1.0 + modrow[0:1, D : 2 * D]) + modrow[0:1, :D]).astype(BF16)

    h[Lr:, :] = (nrm[Lr:, :] * (1.0 + modrow[1:2, D : 2 * D]) + modrow[1:2, :D]).astype(BF16)

    for i in range(3):
        loads[i].wait()
    hh = h[...]
    one = jnp.dot(hh, wk1[...], preferred_element_type=F32)
    two = jnp.dot(hh, wk2[...], preferred_element_type=F32)
    for i in range(G):
        cut = slice(i * HEAD_DIM, (i + 1) * HEAD_DIM)
        pair = jnp.concatenate([one[:, cut], two[:, cut]], axis=1)
        kvs[i, :, :LANES] = rotate(pair, cos_ref[...], sin_ref[...]).astype(BF16)
    val = jnp.dot(hh, wv[...], preferred_element_type=F32)
    for i in range(G):
        kvs[i, :, LANES:] = val[:, i * VALUE_DIM : (i + 1) * VALUE_DIM].astype(BF16)

    mine = t == prim

    def kv_out(i):
        hl = flip(hown, i, G)
        return remote(kvs.at[hl], kv.at[s], kz_s.at[i], kv_r.at[s], (t * G + hl) * R + r, t)

    @pl.when(mine)
    def _():
        kv[s] = kvs[hown]

    @pl.when(jnp.logical_not(mine))
    def _():
        kv_out(0).start()

    for i in range(1, G):
        kv_out(i).start()

    for i in range(3, 5):
        loads[i].wait()
    lh = h[:Lr, :]
    one = jnp.dot(lh, wq1[...], preferred_element_type=F32)
    two = jnp.dot(lh, wq2[...], preferred_element_type=F32)
    for i in range(G):
        cut = slice(i * HEAD_DIM, (i + 1) * HEAD_DIM)
        pair = jnp.concatenate([one[:, cut], two[:, cut]], axis=1)
        turned = rotate(pair, cos_ref[:Lr, :], sin_ref[:Lr, :])
        qs[i] = (turned * (LOG2E * HEAD_DIM**-0.5)).astype(BF16)

    def q_out(i, j):
        hl = flip(hown, i, G)
        to = (t + j) % T
        part = pl.ds(pl.multiple_of(to * rows, rows), rows)
        return remote(
            qs.at[hl, part], q.at[p0], q_s.at[i, j], q_r.at[p0], (t * G + hl) * R + r, to
        )

    @pl.when(mine)
    def _():
        q[p0] = qs[hown, pl.ds(pl.multiple_of(t * rows, rows), rows), :]

    @pl.when(jnp.logical_not(mine))
    def _():
        q_out(0, 0).start()

    for j in range(1, T):
        q_out(0, j).start()
    for i in range(1, G):
        for j in range(T):
            q_out(i, j).start()

    loads[5].wait()
    for i in range(1, T):
        wo_copy(i).start()

    def landed(src):
        remote(kv.at[src], kv.at[src], kz_s.at[0], kv_r.at[src], s, t).wait_recv()

    def to_pair(u, j):
        src = u * R + r
        return remote(kv.at[src], kv.at[src], fx_s.at[u, j], kv_r.at[src], p0 * R + (r + j) % R, t)

    def to_core(src, j):
        return remote(kv.at[src], kv.at[src], fd_s.at[src, j], kv_r.at[src], s, (t + j) % T)

    mx[...] = jnp.full(mx.shape, NEGATIVE, F32)
    acc[...] = jnp.zeros(acc.shape, F32)
    vts[:, VALUE_DIM:, :] = jnp.ones((P, vts.shape[1] - VALUE_DIM, vts.shape[2]), BF16)
    for i in range(1, T):
        from_core(lb, lb_r, i)
    lam = lb[prim, pl.ds(hown, 1), :]
    boost = lb[prim, pl.ds(G + hown, 1), :]
    boost = jnp.concatenate([boost, boost], axis=1)[:, : 2 * rows]
    gain = jnp.broadcast_to(gain_ref[...], (VALUE_DIM, LANES)).T
    nt = (((1,), (1,)), ((), ()))

    def turn_values(u):
        at = pl.ds(u * R, R)
        vals = jnp.concatenate(
            [
                kv[at, :Lr, LANES:].reshape(R * Lr, VALUE_DIM),
                kv[at, Lr:, LANES:].reshape(R * Cp, VALUE_DIM),
            ],
            axis=0,
        )
        vts[u, :VALUE_DIM, :] = vals.astype(F32).T.astype(BF16)

    def attend(blocks, u):
        at = pl.ds(u * R, R)
        keys = jnp.concatenate(
            [kv[at, :Lr, :LANES].reshape(R * Lr, LANES), kv[at, Lr:, :LANES].reshape(R * Cp, LANES)],
            axis=0,
        )
        vals = vts[u]
        for j in blocks:
            qq = q[j]
            lane = lax.broadcasted_iota(jnp.int32, qq.shape, 1)
            zero = jnp.zeros_like(qq)
            both = jnp.concatenate(
                [jnp.where(lane < HEAD_DIM, qq, zero), jnp.where(lane < HEAD_DIM, zero, qq)], axis=0
            )
            sc = lax.dot_general(keys, both, nt, preferred_element_type=F32)
            s_l, s_c = sc[: R * Lr], sc[R * Lr :] + boost
            if Cp != Cr:
                spot = lax.broadcasted_iota(jnp.int32, s_c.shape, 0)
                s_c = jnp.where(spot % Cp < Cr, s_c, NEGATIVE)
            old = mx[j]
            peak = jnp.maximum(
                old,
                jnp.maximum(
                    jnp.max(s_l, axis=0, keepdims=True), jnp.max(s_c, axis=0, keepdims=True)
                ),
            )
            pr = jnp.concatenate(
                [jnp.exp2(s_l - peak).astype(BF16), jnp.exp2(s_c - peak).astype(BF16)], axis=0
            )
            mx[j] = peak
            acc[j] = jnp.exp2(old - peak) * acc[j] + jnp.dot(vals, pr, preferred_element_type=F32)

    def finish(j):
        u = acc[j, :VALUE_DIM, :] / acc[j, VALUE_DIM : VALUE_DIM + 1, :]
        mixed = u[:, :rows] - lam[:, :rows] * u[:, rows:]
        mixed = mixed * lax.rsqrt(jnp.mean(mixed * mixed, axis=0, keepdims=True) + EPSILON)
        ho[j] = (mixed * gain[:, :rows]).T.astype(BF16)

    def ho_out(j):
        return remote(ho.at[j], hr.at[p0], ho_s.at[j], ho_r.at[p0], j * R + r, t)

    def q_landed(j):
        remote(q.at[j], q.at[j], q_s.at[0, 0], q_r.at[j], s, t).wait_recv()

    @pl.loop(0, P + 1)
    def _(k):
        @pl.when(jnp.logical_and(mine, k < P))
        def _():
            u = flip(p0, k, P)
            src = u * R + r

            @pl.when(k > 0)
            def _():
                landed(src)

            for j in range(1, R):
                to_pair(u, j).start()
            for j in range(1, T):
                to_core(src, j).start()

        @pl.when(k > 0)
        def _():
            u = flip(p0, k - 1, P)

            @pl.when(mine)
            def _():
                for j in range(1, R):
                    src = u * R + (r + j) % R
                    landed(src)
                    for i in range(1, T):
                        to_core(src, i).start()

            @pl.when(jnp.logical_not(mine))
            def _():
                for j in range(R):
                    landed(u * R + (r + j) % R)

            @pl.when(k == 1)
            def _():
                @pl.when(jnp.logical_not(mine))
                def _():
                    q_landed(p0)

                for i in range(1, near):
                    q_landed(flip(p0, i, P))

            turn_values(u)
            attend([flip(p0, i, P) for i in range(near)], u)

    for i in range(near):
        j = flip(p0, i, P)
        finish(j)
        if i == 0:
            hr[p0] = ho[p0]
        else:
            ho_out(j).start()

    size = 2 if (P - near) % 2 == 0 else 1

    @pl.loop(0, (P - near) // size)
    def _(m):
        blocks = [flip(p0, near + m * size + i, P) for i in range(size)]
        for j in blocks:
            q_landed(j)

        @pl.loop(0, P)
        def _(u):
            attend(blocks, u)

        for j in blocks:
            finish(j)
            ho_out(j).start()

    for i in range(1, T):
        from_core(wo, wo_r, i)
    for i in range(1, P):
        o = flip(p0, i, P)
        remote(hr.at[o], hr.at[o], ho_s.at[o], ho_r.at[o], s, t).wait_recv()

    branch = None
    for i in range(T):
        part = jnp.concatenate([hr[i * G + j] for j in range(G)], axis=1)
        term = jnp.dot(part, wo[i], preferred_element_type=F32)
        branch = term if branch is None else branch + term
    out_ref[...] = (lat[t].astype(F32) + modrow[0:1, 2 * D :] * branch).astype(BF16)

    for j in range(1, FB):
        mp_copy(j).wait_send()
    for i in range(1, T):
        lat_copy(i).wait_send()
        lb_copy(i).wait_send()
        wo_copy(i).wait_send()
    for i in range(1, A):
        mod_copy(i, a0).wait_send()

    @pl.when(jnp.logical_not(mine))
    def _():
        kv_out(0).wait_send()
        q_out(0, 0).wait_send()

    for i in range(1, G):
        kv_out(i).wait_send()
    for i in range(G):
        for j in range(T):
            if i + j > 0:
                q_out(i, j).wait_send()
    for i in range(1, P):
        ho_out(flip(p0, i, P)).wait_send()

    @pl.when(mine)
    def _():
        @pl.loop(0, P)
        def _(u):
            for j in range(1, R):
                to_pair(u, j).wait_send()
            for i in range(R):
                for j in range(1, T):
                    to_core(u * R + i, j).wait_send()


def body(
    S, T,
    latent, context, condition, context_condition, modulation_weight,
    query_first, query_second, key_first, key_second, value_weight,
    lambda_head, context_score_boost, head_gain, output_weight,
):
    rows, D = latent.shape
    Lr = rows * T
    G = value_weight.shape[1] // VALUE_DIM
    P = T * G
    assert S % P == 0 and P & (P - 1) == 0 and rows <= LANES
    R = S // P
    B = max(d for d in range(1, S + 1) if S % d == 0 and d * d <= S)
    A = S // B
    Cr = context.shape[0]
    Cp = -(-Cr // 16) * 16
    if Cp != Cr:
        context = jnp.pad(context, ((0, Cp - Cr), (0, 0)))
    cw = modulation_weight.shape[1]
    cp = -(-cw // LANES) * LANES
    if cp != cw:
        modulation_weight = jnp.pad(modulation_weight, ((0, 0), (0, cp - cw)))
    depth = modulation_weight.shape[0]
    assert Lr % GRID_W == 0
    tables = rotation_tables(S * Lr // GRID_W)
    vm = pl.BlockSpec(memory_space=pltpu.VMEM)
    sm = pl.BlockSpec(memory_space=pltpu.SMEM)
    hb = pl.BlockSpec(memory_space=pl.ANY)
    V = pltpu.VMEM
    dma = pltpu.SemaphoreType.DMA
    keys = Lr + Cp
    weights = (query_first, query_second, key_first, key_second, value_weight)
    return pl.pallas_call(
        functools.partial(kernel, (S, T, G, R, A, B, Cr, cw)),
        out_shape=jax.ShapeDtypeStruct((rows, D), BF16),
        in_specs=[hb] * 10 + [sm, sm, vm, hb, vm, vm, vm, vm],
        out_specs=vm,
        scratch_shapes=[V(w.shape, BF16) for w in weights]
        + [
            V((T,) + output_weight.shape, BF16),
            V((Cp, D), BF16),
            V((2, depth), F32),
            V((depth, cp), BF16),
            V((keys, LANES), F32),
            V((keys, LANES), F32),
            V((B * T, 2, cp), F32),
            V((A, B, 2, cp), F32),
            V((2, 3 * D), F32),
            V((T, rows, D), BF16),
            V((keys, D), F32),
            V((keys, D), BF16),
            V((G, Lr, LANES), BF16),
            V((G, keys, LANES + VALUE_DIM), BF16),
            V((P, rows, LANES), BF16),
            V((S, keys, LANES + VALUE_DIM), BF16),
            V((P, VALUE_DIM + 16, R * keys), BF16),
            V((P, 1, 2 * rows), F32),
            V((P, VALUE_DIM + 16, 2 * rows), F32),
            V((P, rows, VALUE_DIM), BF16),
            V((P, rows, VALUE_DIM), BF16),
            V((T, 2 * G, LANES), F32),
            dma((6,)), dma((5,)),
            dma((B * T,)), dma((B * T,)), dma((A,)), dma((A,)),
            dma((T,)), dma((T,)), dma((T,)), dma((T,)), dma((T,)), dma((T,)),
            dma((G, T)), dma((P,)), dma((G,)), dma((S,)), dma((P, R)), dma((S, T)),
            dma((P,)), dma((P,)),
        ],
        compiler_params=pltpu.CompilerParams(
            collective_id=0, has_side_effects=True, vmem_limit_bytes=62 * 1024 * 1024
        ),
    )(
        latent, context, condition[None, :], context_condition[None, :], modulation_weight,
        query_first, query_second, key_first, key_second, value_weight,
        lambda_head, context_score_boost, head_gain[None, :], output_weight, *tables,
    )


def solution(mesh):
    in_specs = (
        P(("sp", "tp"), None),
        P("sp", None),
        P("tp"),
        P("tp"),
        P("tp", "sp"),
        P(None, "tp"),
        P(None, "tp"),
        P(None, "tp"),
        P(None, "tp"),
        P(None, "tp"),
        P("tp"),
        P("tp"),
        P(),
        P("tp", None),
    )
    out_specs = P(("sp", "tp"), None)
    run = functools.partial(body, mesh.shape["sp"], mesh.shape["tp"])
    return jax.shard_map(run, mesh=mesh, in_specs=in_specs, out_specs=out_specs, check_vma=False)
```

```python
import functools
import math

import jax
import jax.numpy as jnp
import numpy as np
from jax import lax
from jax.experimental import pallas as pl
from jax.experimental.pallas import tpu as pltpu
from jax.sharding import PartitionSpec as P

HEAD_DIM = 64
VALUE_DIM = 128
GRID_W = 64
EPSILON = 1e-06
THETA = 10000.0
NEGATIVE = -1e30
LOG2E = math.log2(math.e)
MESH = pl.DeviceIdType.MESH
BF16 = jnp.bfloat16
F32 = jnp.float32
LANES = 128


def rotation_tables(grid_rows):
    half = HEAD_DIM // 2
    quarter = half // 2
    lane = np.arange(LANES) % HEAD_DIM
    rate = (THETA ** (-(lane % quarter) / quarter)).astype(np.float32)
    sign = np.where(lane % half < quarter, -1.0, 1.0)
    tables = []
    for count, mask in ((grid_rows, lane < half), (GRID_W, lane >= half)):
        angle = np.arange(count, dtype=np.float32)[:, None] * rate[None, :]
        for table in (np.cos(angle), np.sin(angle) * sign):
            tables.append(np.where(mask, table, 0.0).astype(np.float32))
    return tables


def rotate(x, cosine, sine):
    quarter = HEAD_DIM // 4
    lane = lax.broadcasted_iota(jnp.int32, x.shape, 1)
    ahead = pltpu.roll(x, LANES - quarter, 1)
    behind = pltpu.roll(x, quarter, 1)
    flipped = jnp.where(lane % (2 * quarter) < quarter, ahead, behind)
    return x * cosine + flipped * sine


def normed_rows(rows):
    v = rows.astype(F32)
    return v * lax.rsqrt(jnp.mean(v * v, axis=-1, keepdims=True) + EPSILON)


def flip(v, k, span):
    out = 0
    bit = 1
    while bit < span:
        out = out + bit * ((v // bit + k // bit) % 2)
        bit *= 2
    return out


def kernel(
    dims,
    lat_hbm, ctx_hbm, cond_hbm, ccond_hbm, modw_hbm,
    wq1_hbm, wq2_hbm, wk1_hbm, wk2_hbm, wv_hbm,
    lam_ref, boost_ref, gain_ref, wo_hbm, crow_ref, srow_ref, ccol_ref, scol_ref,
    out_ref,
    wq1, wq2, wk1, wk2, wv, wo,
    ctx, cond, modw, tab, cos_ref, sin_ref, mp, modall, modrow, lat, raw, nrm, h, hraw,
    qs, kvs, kvrs, q, qb, kvn, kvr, kvf, s0, s1, vt0, vt1, pk0, pk1, mx, acc, ho, hr, lb,
    wsem, isem, mp_s, mp_r, ma_s, ma_r, lt_s, lt_r, lb_s, lb_r, wo_s, wo_r,
    rw_s, rw_r, rf_s, rf_r, q_s, q_r, kn_s, kn_r, kf_s, kf_r, kr_s, kr_r, fn_s, ff_s, fr_s, ho_s, ho_r,
):
    S, T, G, R, A, B, Cr, cw = dims
    P = T * G
    s, t = lax.axis_index("sp"), lax.axis_index("tp")
    g, p0 = s // P, s % P
    a0, b0 = s // B, s % B
    prim, hown = p0 // G, p0 % G
    mine = t == prim
    other = jnp.logical_not(mine)
    _, rows, D = lat.shape
    Lr = rows * T
    Cp = ctx.shape[0]
    Q = R - 1
    chunks, rc = raw.shape[2], raw.shape[3]
    rw = chunks * rc
    Rr = T * rw
    N = 2 * P * rows

    def remote(src, dst, send, recv, sp, tp):
        return pltpu.make_async_remote_copy(
            src_ref=src, dst_ref=dst, send_sem=send, recv_sem=recv,
            device_id=(sp, tp), device_id_type=MESH,
        )

    def arrived(buf, recv):
        remote(buf, buf, lt_s.at[0], recv, s, t).wait_recv()

    f0 = b0 * T + t
    FB = B * T

    def plane(j):
        f = (f0 + j) % FB
        return f, a0 * B + f // T, f % T

    barrier = pltpu.get_barrier_semaphore()
    for i in range(1, A):
        pl.semaphore_signal(
            barrier, inc=1, device_id=((a0 + i) % A * B + b0, t), device_id_type=MESH
        )
    for j in range(1, FB):
        _, sp, tp = plane(j)
        pl.semaphore_signal(barrier, inc=1, device_id=(sp, tp), device_id_type=MESH)

    inputs = [
        pltpu.make_async_copy(a, b, isem.at[i])
        for i, (a, b) in enumerate(
            [(cond_hbm, cond.at[0:1]), (ccond_hbm, cond.at[1:2]), (modw_hbm, modw),
             (lat_hbm, lat.at[t]), (ctx_hbm, ctx)]
        )
    ]
    for load in inputs:
        load.start()
    loads = [
        pltpu.make_async_copy(a, b, wsem.at[i])
        for i, (a, b) in enumerate(
            [(wk1_hbm, wk1), (wk2_hbm, wk2), (wv_hbm, wv), (wq1_hbm, wq1), (wq2_hbm, wq2), (wo_hbm, wo.at[t])]
        )
    ]
    for load in loads:
        load.start()

    for i in range(G):
        lb[t, i : i + 1, :] = jnp.full((1, LANES), lam_ref[i], F32)
        lb[t, G + i : G + i + 1, :] = jnp.full((1, LANES), boost_ref[i] * LOG2E, F32)

    for i in range(3):
        inputs[i].wait()
    v = cond[...]
    sig = v / (1.0 + jnp.exp(-v))
    mp[f0] = jnp.dot(sig.astype(BF16), modw[...], preferred_element_type=F32)
    for i in range(3, 5):
        inputs[i].wait()

    pl.semaphore_wait(barrier, FB - 1 + A - 1)

    def mp_copy(j):
        _, sp, tp = plane(j)
        return remote(mp.at[f0], mp.at[f0], mp_s.at[j], mp_r.at[f0], sp, tp)

    def lat_copy(i):
        return remote(lat.at[t], lat.at[t], lt_s.at[i], lt_r.at[t], s, (t + i) % T)

    def lb_copy(i):
        return remote(lb.at[t], lb.at[t], lb_s.at[i], lb_r.at[t], s, (t + i) % T)

    def wo_copy(i):
        return remote(wo.at[t], wo.at[t], wo_s.at[i], wo_r.at[t], s, (t + i) % T)

    def raw_copy(j, c):
        return remote(
            lat.at[t, pl.ds(c * rc, rc)], raw.at[j - 1, t, c], rw_s.at[j - 1, c],
            rw_r.at[j - 1, c], (g + R - j) % R * P + p0, t,
        )

    def raw_pass(j, c, i):
        part = raw.at[j - 1, t, c]
        return remote(
            part, part, rf_s.at[j - 1, c, i], rf_r.at[j - 1, c, t], s, (t + i) % T
        )

    for j in range(1, FB):
        mp_copy(j).start()
    for i in range(1, T):
        lat_copy(i).start()
        lb_copy(i).start()
    for j in range(1, R):
        raw_copy(j, 0).start()

    def table(src, out, order):
        for n, (col, row) in enumerate(((ccol_ref, crow_ref), (scol_ref, srow_ref))):
            for i in range(Lr // GRID_W):
                at = pl.ds(src * (Lr // GRID_W) + i, 1)
                tab[n, i * GRID_W : (i + 1) * GRID_W, :] = col[...] + row[at, :]
            at = out
            for low, high in order:
                ref = sin_ref if n else cos_ref
                ref[at : at + high - low, :] = tab[n, low:high, :]
                at += high - low

    head = [(i * rows, i * rows + rw) for i in range(T)]
    rest = [(i * rows + rw, (i + 1) * rows) for i in range(T)]
    table(s, 0, head + rest)
    cos_ref[Lr : Lr + Cp, :] = jnp.ones((Cp, LANES), F32)
    sin_ref[Lr : Lr + Cp, :] = jnp.zeros((Cp, LANES), F32)
    for j in range(1, R):
        table((g + j) % R * P + p0, Lr + Cp + (j - 1) * Rr, head)

    for j in range(1, FB):
        f, _, _ = plane(j)
        arrived(mp.at[f], mp_r.at[f])
    for b in range(B):
        total = mp[b * T]
        for i in range(1, T):
            total = total + mp[b * T + i]
        modall[a0, b] = total

    def mod_copy(i):
        return remote(
            modall.at[a0], modall.at[a0], ma_s.at[i], ma_r.at[a0], (a0 + i) % A * B + b0, t
        )

    for i in range(1, A):
        mod_copy(i).start()
    for c in range(1, chunks):
        for j in range(1, R):
            raw_copy(j, c).start()

    step = math.gcd(rw, rows - rw, 32)

    def norm_lat(i):
        for low, size, at in ((0, rw, i * rw), (rw, rows - rw, Rr + i * (rows - rw))):

            @pl.loop(0, size // step)
            def _(j):
                off = pl.multiple_of(j * step, step)
                to = pl.ds(pl.multiple_of(at + off, step), step)
                nrm[to, :] = normed_rows(lat[i, pl.ds(low + off, step), :])

    nrm[Lr:, :] = normed_rows(ctx[...])
    norm_lat(t)
    for i in range(1, T):
        o = (t + i) % T
        arrived(lat.at[o], lt_r.at[o])
        norm_lat(o)

    for i in range(1, A):
        o = (a0 + i) % A
        arrived(modall.at[o], ma_r.at[o])
    for a in range(A):
        for b in range(B):
            i = a * B + b
            modrow[:, i * cw : (i + 1) * cw] = modall[a, b][:, :cw]

    @pl.loop(0, Lr // step)
    def _(j):
        at = pl.ds(pl.multiple_of(j * step, step), step)
        h[at, :] = (nrm[at, :] * (1.0 + modrow[0:1, D : 2 * D]) + modrow[0:1, :D]).astype(BF16)

    h[Lr:, :] = (nrm[Lr:, :] * (1.0 + modrow[1:2, D : 2 * D]) + modrow[1:2, :D]).astype(BF16)

    def project(hh, at, out):
        n = hh.shape[0]
        one = jnp.dot(hh, wk1[...], preferred_element_type=F32)
        two = jnp.dot(hh, wk2[...], preferred_element_type=F32)
        for i in range(G):
            cut = slice(i * HEAD_DIM, (i + 1) * HEAD_DIM)
            pair = jnp.concatenate([one[:, cut], two[:, cut]], axis=1)
            turned = rotate(pair, cos_ref[at : at + n, :], sin_ref[at : at + n, :])
            out[i, :, :LANES] = turned.astype(BF16)
        val = jnp.dot(hh, wv[...], preferred_element_type=F32)
        for i in range(G):
            out[i, :, LANES:] = val[:, i * VALUE_DIM : (i + 1) * VALUE_DIM].astype(BF16)

    for i in range(3):
        loads[i].wait()
    project(h[...], 0, kvs)

    def near_out(i):
        hl = flip(hown, i, G)
        return remote(kvs.at[hl], kvn.at[p0], kn_s.at[i], kn_r.at[p0], g * P + t * G + hl, t)

    def far_out(i, j):
        hl = flip(hown, i, G)
        to = (g + R - j) % R
        slot = (j - 1) * P + p0
        return remote(
            kvs.at[hl, pl.ds(Rr, Lr + Cp - Rr)], kvf.at[slot], kf_s.at[i, j - 1], kf_r.at[slot],
            to * P + t * G + hl, t,
        )

    def raw_out(i):
        hl = flip(hown, i, G)
        return remote(kvrs.at[hl], kvr.at[p0], kr_s.at[i], kr_r.at[p0], g * P + t * G + hl, t)

    @pl.when(mine)
    def _():
        kvn[p0] = kvs[hown]

    @pl.when(other)
    def _():
        near_out(0).start()

    for i in range(1, G):
        near_out(i).start()

    for i in range(3, 5):
        loads[i].wait()
    lh = h[:Lr, :]
    one = jnp.dot(lh, wq1[...], preferred_element_type=F32)
    two = jnp.dot(lh, wq2[...], preferred_element_type=F32)
    for i in range(G):
        cut = slice(i * HEAD_DIM, (i + 1) * HEAD_DIM)
        pair = jnp.concatenate([one[:, cut], two[:, cut]], axis=1)
        turned = rotate(pair, cos_ref[:Lr, :], sin_ref[:Lr, :])
        turned = (turned * (LOG2E * HEAD_DIM**-0.5)).astype(BF16)
        at = 0
        for low, high in head + rest:
            qs[i, low:high, :] = turned[at : at + high - low]
            at += high - low

    def q_out(i, j):
        hl = flip(hown, i, G)
        to = (t + j) % T
        part = pl.ds(pl.multiple_of(to * rows, rows), rows)
        return remote(qs.at[hl, part], q.at[p0], q_s.at[i, j], q_r.at[p0], g * P + t * G + hl, to)

    @pl.when(mine)
    def _():
        q[p0] = qs[hown, pl.ds(pl.multiple_of(t * rows, rows), rows), :]

    @pl.when(other)
    def _():
        q_out(0, 0).start()

    for j in range(1, T):
        q_out(0, j).start()
    for i in range(1, G):
        for j in range(T):
            q_out(i, j).start()
    for i in range(G):
        for j in range(1, R):
            far_out(i, j).start()

    for c in range(chunks):
        for j in range(1, R):
            arrived(raw.at[j - 1, t, c], rw_r.at[j - 1, c])
            for i in range(1, T):
                raw_pass(j, c, i).start()

    def lift(j, o, c):
        part = normed_rows(raw[j - 1, o, c])
        part = part * (1.0 + modrow[0:1, D : 2 * D]) + modrow[0:1, :D]
        at = pl.multiple_of((j - 1) * Rr + o * rw + c * rc, rc)
        hraw[pl.ds(at, rc), :] = part.astype(BF16)

    for j in range(1, R):
        for c in range(chunks):
            lift(j, t, c)
    for i in range(1, T):
        o = (t + i) % T
        for c in range(chunks):
            for j in range(1, R):
                arrived(raw.at[j - 1, o, c], rf_r.at[j - 1, c, o])
                lift(j, o, c)
    project(hraw[...], Lr + Cp, kvrs)

    @pl.when(mine)
    def _():
        kvr[p0] = kvrs[hown]

    @pl.when(other)
    def _():
        raw_out(0).start()

    for i in range(1, G):
        raw_out(i).start()

    loads[5].wait()
    for i in range(1, T):
        wo_copy(i).start()

    mx[...] = jnp.full(mx.shape, NEGATIVE, F32)
    acc[...] = jnp.zeros(acc.shape, F32)
    for vt in (vt0, vt1):
        vt[VALUE_DIM:, :] = jnp.ones((vt.shape[0] - VALUE_DIM, vt.shape[1]), BF16)
    for i in range(1, T):
        o = (t + i) % T
        arrived(lb.at[o], lb_r.at[o])
    lam = lb[prim, pl.ds(hown, 1), :][:, :rows]
    boost = lb[prim, pl.ds(G + hown, 1), :][:, :1]
    gain = jnp.broadcast_to(gain_ref[...], (VALUE_DIM, LANES)).T[:, :rows]
    nt = (((1,), (1,)), ((), ()))

    def to_core(buf, slot, send, recv, i):
        return remote(
            buf.at[slot], buf.at[slot], send.at[slot, i], recv.at[slot], s, (t + i) % T
        )

    def fetch(buf, slots, send, recv, own):
        @pl.when(mine)
        def _():
            for n, slot in enumerate(slots):
                if own:

                    @pl.when(slot != p0)
                    def _():
                        arrived(buf.at[slot], recv.at[slot])

                else:
                    arrived(buf.at[slot], recv.at[slot])
                for i in range(1, T):
                    to_core(buf, slot, send, recv, i).start()

        @pl.when(other)
        def _():
            for slot in slots:
                arrived(buf.at[slot], recv.at[slot])

    def scores(buf, base, count, low, s_ref, vt_ref, pk_ref):
        span = buf.shape[1]
        at = pl.ds(base, count)
        keys = buf[at, :low, :LANES].reshape(count * low, LANES)
        vals = buf[at, :low, LANES:].reshape(count * low, VALUE_DIM)
        sc = lax.dot_general(keys, qb[...], nt, preferred_element_type=F32)
        n = count * low
        s_ref[:n, :] = sc
        peak = jnp.max(sc, axis=0, keepdims=True)
        vt_ref[:VALUE_DIM, :n] = vals.astype(F32).T.astype(BF16)
        if span > low:
            m = count * (span - low)
            keys = buf[at, low:, :LANES].reshape(m, LANES)
            vals = buf[at, low:, LANES:].reshape(m, VALUE_DIM)
            sc = lax.dot_general(keys, qb[...], nt, preferred_element_type=F32) + boost
            if Cp != Cr:
                spot = lax.broadcasted_iota(jnp.int32, sc.shape, 0)
                sc = jnp.where(spot % Cp < Cr, sc, NEGATIVE)
            s_ref[n : n + m, :] = sc
            peak = jnp.maximum(peak, jnp.max(sc, axis=0, keepdims=True))
            vt_ref[:VALUE_DIM, n : n + m] = vals.astype(F32).T.astype(BF16)
        pk_ref[...] = peak

    def weigh(n, s_ref, vt_ref, pk_ref):
        old = mx[...]
        peak = jnp.maximum(old, pk_ref[...])
        pr = jnp.exp2(s_ref[:n, :] - peak).astype(BF16)
        mx[...] = peak
        acc[...] = jnp.exp2(old - peak) * acc[...] + jnp.dot(
            vt_ref[:, :n], pr, preferred_element_type=F32
        )

    def finish(j):
        u = acc[:VALUE_DIM, j * 2 * rows : (j + 1) * 2 * rows]
        u = u / acc[VALUE_DIM : VALUE_DIM + 1, j * 2 * rows : (j + 1) * 2 * rows]
        mixed = u[:, :rows] - lam * u[:, rows:]
        mixed = mixed * lax.rsqrt(jnp.mean(mixed * mixed, axis=0, keepdims=True) + EPSILON)
        ho[j] = (mixed * gain).T.astype(BF16)

    def ho_out(j):
        return remote(ho.at[j], hr.at[p0], ho_s.at[j], ho_r.at[p0], g * P + j, t)

    for j in range(P):

        @pl.when(jnp.logical_or(other, p0 != j))
        def _():
            arrived(q.at[j], q_r.at[j])

        qq = q[j]
        lane = lax.broadcasted_iota(jnp.int32, qq.shape, 1)
        zero = jnp.zeros_like(qq)
        qb[j * 2 * rows : j * 2 * rows + rows, :] = jnp.where(lane < HEAD_DIM, qq, zero)
        qb[j * 2 * rows + rows : (j + 1) * 2 * rows, :] = jnp.where(lane < HEAD_DIM, zero, qq)

    units = []
    pair = min(2, P)
    for k in range(P // pair):
        units.append((kvn, flip(p0 // pair, k, P // pair) * pair, pair, Lr, fn_s, kn_r, True))
    quad = math.gcd(P, max(1, 640 // (Q * Rr)))
    for k in range(P // quad):
        units.append((kvr, flip(p0 // quad, k, P // quad) * quad, quad, Q * Rr, fr_s, kr_r, True))
    wide = math.gcd(P, max(1, 640 // kvf.shape[1]))
    for j in range(Q):
        for k in range(P // wide):
            base = j * P + flip(p0 // wide, k, P // wide) * wide
            units.append((kvf, base, wide, Lr - Rr, ff_s, kf_r, False))
    banks = ((s0, vt0, pk0), (s1, vt1, pk1))
    last = None
    for n, (buf, base, count, low, send, recv, own) in enumerate(units):
        fetch(buf, [base + i for i in range(count)], send, recv, own)
        scores(buf, base, count, low, *banks[n % 2])
        if last is not None:
            weigh(last, *banks[(n - 1) % 2])
        last = count * buf.shape[1]
    weigh(last, *banks[(len(units) - 1) % 2])

    for j in range(P):
        finish(j)

        @pl.when(p0 == j)
        def _():
            hr[j] = ho[j]

        @pl.when(p0 != j)
        def _():
            ho_out(j).start()

    for i in range(1, T):
        o = (t + i) % T
        arrived(wo.at[o], wo_r.at[o])
    for i in range(1, P):
        o = flip(p0, i, P)
        arrived(hr.at[o], ho_r.at[o])

    branch = None
    for i in range(T):
        part = jnp.concatenate([hr[i * G + j] for j in range(G)], axis=1)
        term = jnp.dot(part, wo[i], preferred_element_type=F32)
        branch = term if branch is None else branch + term
    out_ref[...] = (lat[t].astype(F32) + modrow[0:1, 2 * D :] * branch).astype(BF16)

    for j in range(1, FB):
        mp_copy(j).wait_send()
    for i in range(1, T):
        lat_copy(i).wait_send()
        lb_copy(i).wait_send()
        wo_copy(i).wait_send()
    for i in range(1, A):
        mod_copy(i).wait_send()
    for j in range(1, R):
        for c in range(chunks):
            raw_copy(j, c).wait_send()
            for i in range(1, T):
                raw_pass(j, c, i).wait_send()

    @pl.when(other)
    def _():
        near_out(0).wait_send()
        raw_out(0).wait_send()
        q_out(0, 0).wait_send()

    for i in range(1, G):
        near_out(i).wait_send()
        raw_out(i).wait_send()
    for i in range(G):
        for j in range(1, R):
            far_out(i, j).wait_send()
        for j in range(T):
            if i + j > 0:
                q_out(i, j).wait_send()
    for i in range(1, P):
        ho_out(flip(p0, i, P)).wait_send()

    @pl.when(mine)
    def _():
        for buf, send, recv in ((kvn, fn_s, kn_r), (kvr, fr_s, kr_r), (kvf, ff_s, kf_r)):

            @pl.loop(0, buf.shape[0])
            def _(slot):
                for i in range(1, T):
                    to_core(buf, slot, send, recv, i).wait_send()


def body(
    S, T,
    latent, context, condition, context_condition, modulation_weight,
    query_first, query_second, key_first, key_second, value_weight,
    lambda_head, context_score_boost, head_gain, output_weight,
):
    rows, D = latent.shape
    Lr = rows * T
    G = value_weight.shape[1] // VALUE_DIM
    P = T * G
    assert S % P == 0 and P & (P - 1) == 0 and rows <= LANES
    R = S // P
    B = max(d for d in range(1, S + 1) if S % d == 0 and d * d <= S)
    A = S // B
    assert R > 1 and P % B == 0
    rc = 16
    chunks = rows * 5 // 8 // rc
    Rr = T * chunks * rc
    Cr = context.shape[0]
    Cp = -(-Cr // 16) * 16
    if Cp != Cr:
        context = jnp.pad(context, ((0, Cp - Cr), (0, 0)))
    cw = modulation_weight.shape[1]
    cp = -(-cw // LANES) * LANES
    if cp != cw:
        modulation_weight = jnp.pad(modulation_weight, ((0, 0), (0, cp - cw)))
    depth = modulation_weight.shape[0]
    assert Lr % GRID_W == 0
    tables = rotation_tables(S * Lr // GRID_W)
    vm = pl.BlockSpec(memory_space=pltpu.VMEM)
    sm = pl.BlockSpec(memory_space=pltpu.SMEM)
    hb = pl.BlockSpec(memory_space=pl.ANY)
    V = pltpu.VMEM
    dma = pltpu.SemaphoreType.DMA
    keys = Lr + Cp
    Q = R - 1
    N = 2 * P * rows
    pairw = LANES + VALUE_DIM
    most = max(2 * keys, Q * Rr, 640)
    weights = (query_first, query_second, key_first, key_second, value_weight)
    return pl.pallas_call(
        functools.partial(kernel, (S, T, G, R, A, B, Cr, cw)),
        out_shape=jax.ShapeDtypeStruct((rows, D), BF16),
        in_specs=[hb] * 10 + [sm, sm, vm, hb, vm, vm, vm, vm],
        out_specs=vm,
        scratch_shapes=[V(w.shape, BF16) for w in weights]
        + [
            V((T,) + output_weight.shape, BF16),
            V((Cp, D), BF16),
            V((2, depth), F32),
            V((depth, cp), BF16),
            V((2, Lr, LANES), F32),
            V((keys + Q * Rr, LANES), F32),
            V((keys + Q * Rr, LANES), F32),
            V((B * T, 2, cp), F32),
            V((A, B, 2, cp), F32),
            V((2, 3 * D), F32),
            V((T, rows, D), BF16),
            V((Q, T, chunks, rc, D), BF16),
            V((keys, D), F32),
            V((keys, D), BF16),
            V((Q * Rr, D), BF16),
            V((G, Lr, LANES), BF16),
            V((G, keys, pairw), BF16),
            V((G, Q * Rr, pairw), BF16),
            V((P, rows, LANES), BF16),
            V((N, LANES), BF16),
            V((P, keys, pairw), BF16),
            V((P, Q * Rr, pairw), BF16),
            V((Q * P, keys - Rr, pairw), BF16),
            V((most, N), F32),
            V((most, N), F32),
            V((VALUE_DIM + 16, most), BF16),
            V((VALUE_DIM + 16, most), BF16),
            V((1, N), F32),
            V((1, N), F32),
            V((1, N), F32),
            V((VALUE_DIM + 16, N), F32),
            V((P, rows, VALUE_DIM), BF16),
            V((P, rows, VALUE_DIM), BF16),
            V((T, 2 * G, LANES), F32),
            dma((6,)), dma((5,)),
            dma((B * T,)), dma((B * T,)), dma((A,)), dma((A,)),
            dma((T,)), dma((T,)), dma((T,)), dma((T,)), dma((T,)), dma((T,)),
            dma((Q, chunks)), dma((Q, chunks)), dma((Q, chunks, T)), dma((Q, chunks, T)),
            dma((G, T)), dma((P,)),
            dma((G,)), dma((P,)), dma((G, Q)), dma((Q * P,)), dma((G,)), dma((P,)),
            dma((P, T)), dma((Q * P, T)), dma((P, T)),
            dma((P,)), dma((P,)),
        ],
        compiler_params=pltpu.CompilerParams(
            collective_id=0, has_side_effects=True, vmem_limit_bytes=62 * 1024 * 1024
        ),
    )(
        latent, context, condition[None, :], context_condition[None, :], modulation_weight,
        query_first, query_second, key_first, key_second, value_weight,
        lambda_head, context_score_boost, head_gain[None, :], output_weight, *tables,
    )


def solution(mesh):
    in_specs = (
        P(("sp", "tp"), None),
        P("sp", None),
        P("tp"),
        P("tp"),
        P("tp", "sp"),
        P(None, "tp"),
        P(None, "tp"),
        P(None, "tp"),
        P(None, "tp"),
        P(None, "tp"),
        P("tp"),
        P("tp"),
        P(),
        P("tp", None),
    )
    out_specs = P(("sp", "tp"), None)
    run = functools.partial(body, mesh.shape["sp"], mesh.shape["tp"])
    return jax.shard_map(run, mesh=mesh, in_specs=in_specs, out_specs=out_specs, check_vma=False)
```

```python
import functools
import math

import jax
import jax.numpy as jnp
import numpy as np
from jax import lax
from jax.experimental import pallas as pl
from jax.experimental.pallas import tpu as pltpu
from jax.sharding import PartitionSpec as P

HEAD_DIM = 64
VALUE_DIM = 128
GRID_W = 64
EPSILON = 1e-06
THETA = 10000.0
NEGATIVE = -1e30
LOG2E = math.log2(math.e)
MESH = pl.DeviceIdType.MESH
BF16 = jnp.bfloat16
F32 = jnp.float32
LANES = 128
QROWS = 256


def rotation_tables(grid_rows):
    half = HEAD_DIM // 2
    quarter = half // 2
    lane = np.arange(LANES) % HEAD_DIM
    rate = (THETA ** (-(lane % quarter) / quarter)).astype(np.float32)
    sign = np.where(lane % half < quarter, -1.0, 1.0)
    tables = []
    for count, mask in ((grid_rows, lane < half), (GRID_W, lane >= half)):
        angle = np.arange(count, dtype=np.float32)[:, None] * rate[None, :]
        for table in (np.cos(angle), np.sin(angle) * sign):
            tables.append(np.where(mask, table, 0.0).astype(np.float32))
    return tables


def rotate(x, cosine, sine):
    quarter = HEAD_DIM // 4
    lane = lax.broadcasted_iota(jnp.int32, x.shape, 1)
    ahead = pltpu.roll(x, LANES - quarter, 1)
    behind = pltpu.roll(x, quarter, 1)
    flipped = jnp.where(lane % (2 * quarter) < quarter, ahead, behind)
    return x * cosine + flipped * sine


def normed_rows(rows):
    v = rows.astype(F32)
    return v * lax.rsqrt(jnp.mean(v * v, axis=-1, keepdims=True) + EPSILON)


def flip(v, k, span):
    out = 0
    bit = 1
    while bit < span:
        out = out + bit * ((v // bit + k // bit) % 2)
        bit *= 2
    return out


def groups(P, raw_rows, far_rows):
    return math.gcd(P, max(1, 400 // raw_rows)), math.gcd(P, max(1, 512 // far_rows))


def kernel(
    dims,
    lat_hbm, ctx_hbm, cond_hbm, ccond_hbm, modw_hbm,
    wq1_hbm, wq2_hbm, wk1_hbm, wk2_hbm, wv_hbm,
    lam_ref, boost_ref, gain_ref, wo_hbm, crow_ref, srow_ref, ccol_ref, scol_ref,
    out_ref,
    wq1, wq2, wk1, wk2, wv, wo,
    ctx, cond, modw, tab, cos_ref, sin_ref, mp, modrow, lat, raw, nrm, h, hraw,
    qs, kvs, kvrs, q, qb, kvn, kvr, kvf, s0, s1, vt0, vt1, pk0, pk1, mx, acc, ho, hr, lb,
    wsem, isem, mp_s, mp_r, lt_s, lt_r, lb_s, lb_r, wo_s, wo_r,
    rw_s, rw_r, rf_s, rf_r, q_s, q_r, kn_s, kn_r, kf_s, kf_r, kr_s, kr_r, fn_s, ff_s, fr_s, ho_s, ho_r,
):
    S, T, G, R, Cr, cw = dims
    P = T * G
    s, t = lax.axis_index("sp"), lax.axis_index("tp")
    g, p0 = s // P, s % P
    prim, hown = p0 // G, p0 % G
    mine = t == prim
    other = jnp.logical_not(mine)
    _, rows, D = lat.shape
    Lr = rows * T
    Cp = ctx.shape[0]
    keys = Lr + Cp
    Q = R - 1
    chunks, rc = raw.shape[2], raw.shape[3]
    rw = chunks * rc
    Rr = T * rw
    N = 2 * P * rows
    quad, wide = groups(P, Q * Rr, keys - Rr)

    def remote(src, dst, send, recv, sp, tp):
        return pltpu.make_async_remote_copy(
            src_ref=src, dst_ref=dst, send_sem=send, recv_sem=recv,
            device_id=(sp, tp), device_id_type=MESH,
        )

    def arrived(buf, recv):
        remote(buf, buf, lt_s.at[0], recv, s, t).wait_recv()

    f0 = s * T + t
    F = S * T
    barrier = pltpu.get_barrier_semaphore()

    @pl.loop(1, F)
    def _(i):
        f = (f0 + i) % F
        pl.semaphore_signal(barrier, inc=1, device_id=(f // T, f % T), device_id_type=MESH)

    inputs = [
        pltpu.make_async_copy(a, b, isem.at[i])
        for i, (a, b) in enumerate(
            [(cond_hbm, cond.at[0:1]), (ccond_hbm, cond.at[1:2]), (modw_hbm, modw),
             (lat_hbm, lat.at[t]), (ctx_hbm, ctx)]
        )
    ]
    for load in inputs:
        load.start()
    loads = [
        pltpu.make_async_copy(a, b, wsem.at[i])
        for i, (a, b) in enumerate(
            [(wk1_hbm, wk1), (wk2_hbm, wk2), (wv_hbm, wv), (wq1_hbm, wq1), (wq2_hbm, wq2), (wo_hbm, wo.at[t])]
        )
    ]
    for load in loads:
        load.start()

    for i in range(G):
        lb[t, i : i + 1, :] = jnp.full((1, LANES), lam_ref[i], F32)
        lb[t, G + i : G + i + 1, :] = jnp.full((1, LANES), boost_ref[i] * LOG2E, F32)

    for i in range(3):
        inputs[i].wait()
    v = cond[...]
    sig = v / (1.0 + jnp.exp(-v))
    mp[f0] = jnp.dot(sig.astype(BF16), modw[...], preferred_element_type=F32)
    for i in range(3, 5):
        inputs[i].wait()

    pl.semaphore_wait(barrier, F - 1)

    def mp_copy(i):
        f = (f0 + i) % F
        return remote(mp.at[f0], mp.at[f0], mp_s.at[i], mp_r.at[f0], f // T, f % T)

    def lat_copy(i):
        return remote(lat.at[t], lat.at[t], lt_s.at[i], lt_r.at[t], s, (t + i) % T)

    def lb_copy(i):
        return remote(lb.at[t], lb.at[t], lb_s.at[i], lb_r.at[t], s, (t + i) % T)

    def wo_copy(i):
        return remote(wo.at[t], wo.at[t], wo_s.at[i], wo_r.at[t], s, (t + i) % T)

    def raw_copy(j, c):
        return remote(
            lat.at[t, pl.ds(c * rc, rc)], raw.at[j - 1, t, c], rw_s.at[j - 1, c],
            rw_r.at[j - 1, c], (g + R - j) % R * P + p0, t,
        )

    def raw_pass(j, c, i):
        part = raw.at[j - 1, t, c]
        return remote(
            part, part, rf_s.at[j - 1, c, i], rf_r.at[j - 1, c, t], s, (t + i) % T
        )

    @pl.loop(1, F)
    def _(i):
        mp_copy(i).start()

    for i in range(1, T):
        lat_copy(i).start()
        lb_copy(i).start()
    for c in range(chunks):
        for j in range(1, R):
            raw_copy(j, c).start()
    loads[5].wait()
    for i in range(1, T):
        wo_copy(i).start()

    def table(src, out, order):
        for n, (col, row) in enumerate(((ccol_ref, crow_ref), (scol_ref, srow_ref))):
            for i in range(Lr // GRID_W):
                at = pl.ds(src * (Lr // GRID_W) + i, 1)
                tab[n, i * GRID_W : (i + 1) * GRID_W, :] = col[...] + row[at, :]
            at = out
            for low, high in order:
                ref = sin_ref if n else cos_ref
                ref[at : at + high - low, :] = tab[n, low:high, :]
                at += high - low

    head = [(i * rows, i * rows + rw) for i in range(T)]
    rest = [(i * rows + rw, (i + 1) * rows) for i in range(T)]
    table(s, 0, head + rest)
    cos_ref[Lr : Lr + Cp, :] = jnp.ones((Cp, LANES), F32)
    sin_ref[Lr : Lr + Cp, :] = jnp.zeros((Cp, LANES), F32)
    for j in range(1, R):
        table((g + j) % R * P + p0, Lr + Cp + (j - 1) * Rr, head)

    step = math.gcd(rw, rows - rw, 32)

    def norm_lat(i):
        for low, size, at in ((0, rw, i * rw), (rw, rows - rw, Rr + i * (rows - rw))):

            @pl.loop(0, size // step)
            def _(j):
                off = pl.multiple_of(j * step, step)
                to = pl.ds(pl.multiple_of(at + off, step), step)
                nrm[to, :] = normed_rows(lat[i, pl.ds(low + off, step), :])

    nrm[Lr:, :] = normed_rows(ctx[...])
    norm_lat(t)
    for i in range(1, T):
        o = (t + i) % T
        arrived(lat.at[o], lt_r.at[o])
        norm_lat(o)

    @pl.loop(1, F)
    def _(i):
        f = (f0 + i) % F
        arrived(mp.at[f], mp_r.at[f])

    for i in range(S):
        total = mp[i * T]
        for j in range(1, T):
            total = total + mp[i * T + j]
        modrow[:, i * cw : (i + 1) * cw] = total[:, :cw]

    @pl.loop(0, Lr // step)
    def _(j):
        at = pl.ds(pl.multiple_of(j * step, step), step)
        h[at, :] = (nrm[at, :] * (1.0 + modrow[0:1, D : 2 * D]) + modrow[0:1, :D]).astype(BF16)

    h[Lr:, :] = (nrm[Lr:, :] * (1.0 + modrow[1:2, D : 2 * D]) + modrow[1:2, :D]).astype(BF16)

    def project(hh, at, out):
        n = hh.shape[0]
        one = jnp.dot(hh, wk1[...], preferred_element_type=F32)
        two = jnp.dot(hh, wk2[...], preferred_element_type=F32)
        for i in range(G):
            cut = slice(i * HEAD_DIM, (i + 1) * HEAD_DIM)
            pair = jnp.concatenate([one[:, cut], two[:, cut]], axis=1)
            turned = rotate(pair, cos_ref[at : at + n, :], sin_ref[at : at + n, :])
            out[i, :, :LANES] = turned.astype(BF16)
        val = jnp.dot(hh, wv[...], preferred_element_type=F32)
        for i in range(G):
            out[i, :, LANES:] = val[:, i * VALUE_DIM : (i + 1) * VALUE_DIM].astype(BF16)

    for i in range(3, 5):
        loads[i].wait()
    lh = h[:Lr, :]
    one = jnp.dot(lh, wq1[...], preferred_element_type=F32)
    two = jnp.dot(lh, wq2[...], preferred_element_type=F32)
    for i in range(G):
        cut = slice(i * HEAD_DIM, (i + 1) * HEAD_DIM)
        pair = jnp.concatenate([one[:, cut], two[:, cut]], axis=1)
        turned = rotate(pair, cos_ref[:Lr, :], sin_ref[:Lr, :])
        turned = (turned * (LOG2E * HEAD_DIM**-0.5)).astype(BF16)
        at = 0
        for low, high in head + rest:
            qs[i, low:high, :] = turned[at : at + high - low]
            at += high - low

    def q_out(i, j):
        hl = flip(hown, i, G)
        to = (t + j) % T
        part = pl.ds(pl.multiple_of(to * rows, rows), rows)
        return remote(qs.at[hl, part], q.at[p0], q_s.at[i, j], q_r.at[p0], g * P + t * G + hl, to)

    @pl.when(mine)
    def _():
        q[p0] = qs[hown, pl.ds(pl.multiple_of(t * rows, rows), rows), :]

    @pl.when(other)
    def _():
        q_out(0, 0).start()

    for j in range(1, T):
        q_out(0, j).start()
    for i in range(1, G):
        for j in range(T):
            q_out(i, j).start()
    for i in range(3):
        loads[i].wait()
    project(h[...], 0, kvs)

    def near_out(i):
        hl = flip(hown, i, G)
        return remote(kvs.at[hl], kvn.at[p0], kn_s.at[i], kn_r.at[p0], g * P + t * G + hl, t)

    def far_out(i, j):
        hl = flip(hown, i, G)
        to = (g + R - j) % R
        slot = (j - 1) * P + p0
        return remote(
            kvs.at[hl, pl.ds(Rr, Lr + Cp - Rr)], kvf.at[slot], kf_s.at[i, j - 1], kf_r.at[slot],
            to * P + t * G + hl, t,
        )

    def raw_out(i):
        hl = flip(hown, i, G)
        return remote(kvrs.at[hl], kvr.at[p0], kr_s.at[i], kr_r.at[p0], g * P + t * G + hl, t)

    @pl.when(mine)
    def _():
        kvn[p0] = kvs[hown]

    @pl.when(other)
    def _():
        near_out(0).start()

    for i in range(1, G):
        near_out(i).start()
    for i in range(G):
        for j in range(1, R):
            far_out(i, j).start()


    for c in range(chunks):
        for j in range(1, R):
            arrived(raw.at[j - 1, t, c], rw_r.at[j - 1, c])
            for i in range(1, T):
                raw_pass(j, c, i).start()

    def lift(j, o, c):
        part = normed_rows(raw[j - 1, o, c])
        part = part * (1.0 + modrow[0:1, D : 2 * D]) + modrow[0:1, :D]
        at = pl.multiple_of((j - 1) * Rr + o * rw + c * rc, rc)
        hraw[pl.ds(at, rc), :] = part.astype(BF16)

    for j in range(1, R):
        for c in range(chunks):
            lift(j, t, c)
    for i in range(1, T):
        o = (t + i) % T
        for c in range(chunks):
            for j in range(1, R):
                arrived(raw.at[j - 1, o, c], rf_r.at[j - 1, c, o])
                lift(j, o, c)
    project(hraw[...], Lr + Cp, kvrs)

    @pl.when(mine)
    def _():
        kvr[p0] = kvrs[hown]

    @pl.when(other)
    def _():
        raw_out(0).start()

    for i in range(1, G):
        raw_out(i).start()

    mx[...] = jnp.full(mx.shape, NEGATIVE, F32)
    acc[...] = jnp.zeros(acc.shape, F32)
    for vt in (vt0, vt1):
        vt[VALUE_DIM:, :] = jnp.ones((vt.shape[0] - VALUE_DIM, vt.shape[1]), BF16)
    for i in range(1, T):
        o = (t + i) % T
        arrived(lb.at[o], lb_r.at[o])
    lam = lb[prim, pl.ds(hown, 1), :][:, :rows]
    boost = lb[prim, pl.ds(G + hown, 1), :][:, :1]
    gain = jnp.broadcast_to(gain_ref[...], (VALUE_DIM, LANES)).T[:, :rows]
    nt = (((1,), (1,)), ((), ()))

    def to_core(buf, slot, send, recv, i):
        return remote(
            buf.at[slot], buf.at[slot], send.at[slot, i], recv.at[slot], s, (t + i) % T
        )

    def spread(buf, slots, send, recv, own):
        @pl.when(mine)
        def _():
            for slot in slots:
                if own:

                    @pl.when(slot != p0)
                    def _():
                        arrived(buf.at[slot], recv.at[slot])

                else:
                    arrived(buf.at[slot], recv.at[slot])
                for i in range(1, T):
                    to_core(buf, slot, send, recv, i).start()

    def settle(buf, slots, recv):
        @pl.when(other)
        def _():
            for slot in slots:
                arrived(buf.at[slot], recv.at[slot])

    def scores(buf, base, count, low, s_ref, vt_ref, pk_ref):
        span = buf.shape[1]
        at = pl.ds(base, count)
        keys = buf[at, :low, :LANES].reshape(count * low, LANES)
        vals = buf[at, :low, LANES:].reshape(count * low, VALUE_DIM)
        sc = lax.dot_general(keys, qb[...], nt, preferred_element_type=F32)
        n = count * low
        s_ref[:n, :] = sc
        peak = jnp.max(sc, axis=0, keepdims=True)
        vt_ref[:VALUE_DIM, :n] = vals.astype(F32).T.astype(BF16)
        if span > low:
            m = count * (span - low)
            keys = buf[at, low:, :LANES].reshape(m, LANES)
            vals = buf[at, low:, LANES:].reshape(m, VALUE_DIM)
            sc = lax.dot_general(keys, qb[...], nt, preferred_element_type=F32) + boost
            if Cp != Cr:
                spot = lax.broadcasted_iota(jnp.int32, sc.shape, 0)
                sc = jnp.where(spot % Cp < Cr, sc, NEGATIVE)
            s_ref[n : n + m, :] = sc
            peak = jnp.maximum(peak, jnp.max(sc, axis=0, keepdims=True))
            vt_ref[:VALUE_DIM, n : n + m] = vals.astype(F32).T.astype(BF16)
        pk_ref[...] = peak

    def weigh(n, s_ref, vt_ref, pk_ref):
        old = mx[...]
        peak = jnp.maximum(old, pk_ref[...])
        pr = jnp.exp2(s_ref[:n, :] - peak).astype(BF16)
        mx[...] = peak
        acc[...] = jnp.exp2(old - peak) * acc[...] + jnp.dot(
            vt_ref[:, :n], pr, preferred_element_type=F32
        )

    def finish(j):
        u = acc[:VALUE_DIM, j * 2 * rows : (j + 1) * 2 * rows]
        u = u / acc[VALUE_DIM : VALUE_DIM + 1, j * 2 * rows : (j + 1) * 2 * rows]
        mixed = u[:, :rows] - lam * u[:, rows:]
        mixed = mixed * lax.rsqrt(jnp.mean(mixed * mixed, axis=0, keepdims=True) + EPSILON)
        ho[j] = (mixed * gain).T.astype(BF16)

    def ho_out(j):
        return remote(ho.at[j], hr.at[p0], ho_s.at[j], ho_r.at[p0], g * P + j, t)

    for j in range(P):

        @pl.when(jnp.logical_or(other, p0 != j))
        def _():
            arrived(q.at[j], q_r.at[j])

        qq = q[j]
        lane = lax.broadcasted_iota(jnp.int32, qq.shape, 1)
        zero = jnp.zeros_like(qq)
        qb[j * 2 * rows : j * 2 * rows + rows, :] = jnp.where(lane < HEAD_DIM, qq, zero)
        qb[j * 2 * rows + rows : (j + 1) * 2 * rows, :] = jnp.where(lane < HEAD_DIM, zero, qq)

    units = []
    for k in [*range(0, P // 2, 2), *range(1, P // 2, 2)]:
        units.append((kvn, flip(p0 // 2, k, P // 2) * 2, 2, Lr, fn_s, kn_r, True))
    for j in range(Q):
        for k in range(P // wide):
            base = j * P + flip(p0 // wide, k, P // wide) * wide
            units.append((kvf, base, wide, Lr - Rr, ff_s, kf_r, False))
    for k in range(P // quad):
        units.append((kvr, flip(p0 // quad, k, P // quad) * quad, quad, Q * Rr, fr_s, kr_r, True))
    banks = ((s0, vt0, pk0), (s1, vt1, pk1))
    last = None
    for n, (buf, base, count, low, send, recv, own) in enumerate(units):
        spread(buf, [base + i for i in range(count)], send, recv, own)
        settle(buf, [base + i for i in range(count)], recv)
        scores(buf, base, count, low, *banks[n % 2])
        if last is not None:
            weigh(last, *banks[(n - 1) % 2])
        last = count * buf.shape[1]
    weigh(last, *banks[(len(units) - 1) % 2])

    for j in range(P):
        finish(j)

        @pl.when(p0 == j)
        def _():
            hr[j] = ho[j]

        @pl.when(p0 != j)
        def _():
            ho_out(j).start()

    for i in range(1, T):
        o = (t + i) % T
        arrived(wo.at[o], wo_r.at[o])
    for i in range(1, P):
        o = flip(p0, i, P)
        arrived(hr.at[o], ho_r.at[o])

    branch = None
    for i in range(T):
        part = jnp.concatenate([hr[i * G + j] for j in range(G)], axis=1)
        term = jnp.dot(part, wo[i], preferred_element_type=F32)
        branch = term if branch is None else branch + term
    out_ref[...] = (lat[t].astype(F32) + modrow[0:1, 2 * D :] * branch).astype(BF16)

    @pl.loop(1, F)
    def _(i):
        mp_copy(i).wait_send()

    for i in range(1, T):
        lat_copy(i).wait_send()
        lb_copy(i).wait_send()
        wo_copy(i).wait_send()
    for j in range(1, R):
        for c in range(chunks):
            raw_copy(j, c).wait_send()
            for i in range(1, T):
                raw_pass(j, c, i).wait_send()

    @pl.when(other)
    def _():
        near_out(0).wait_send()
        raw_out(0).wait_send()
        q_out(0, 0).wait_send()

    for i in range(1, G):
        near_out(i).wait_send()
        raw_out(i).wait_send()
    for i in range(G):
        for j in range(1, R):
            far_out(i, j).wait_send()
        for j in range(T):
            if i + j > 0:
                q_out(i, j).wait_send()
    for i in range(1, P):
        ho_out(flip(p0, i, P)).wait_send()

    @pl.when(mine)
    def _():
        for buf, send, recv in ((kvn, fn_s, kn_r), (kvr, fr_s, kr_r), (kvf, ff_s, kf_r)):

            @pl.loop(0, buf.shape[0])
            def _(slot):
                for i in range(1, T):
                    to_core(buf, slot, send, recv, i).wait_send()


def body(
    S, T,
    latent, context, condition, context_condition, modulation_weight,
    query_first, query_second, key_first, key_second, value_weight,
    lambda_head, context_score_boost, head_gain, output_weight,
):
    rows, D = latent.shape
    Lr = rows * T
    G = value_weight.shape[1] // VALUE_DIM
    P = T * G
    assert S % P == 0 and P & (P - 1) == 0 and rows <= LANES
    R = S // P
    assert R > 1 and P > 1
    rc = 16
    chunks = rows * 3 // 8 // rc
    Rr = T * chunks * rc
    Cr = context.shape[0]
    Cp = -(-Cr // 16) * 16
    if Cp != Cr:
        context = jnp.pad(context, ((0, Cp - Cr), (0, 0)))
    cw = modulation_weight.shape[1]
    cp = -(-cw // LANES) * LANES
    if cp != cw:
        modulation_weight = jnp.pad(modulation_weight, ((0, 0), (0, cp - cw)))
    depth = modulation_weight.shape[0]
    assert Lr % GRID_W == 0
    tables = rotation_tables(S * Lr // GRID_W)
    vm = pl.BlockSpec(memory_space=pltpu.VMEM)
    sm = pl.BlockSpec(memory_space=pltpu.SMEM)
    hb = pl.BlockSpec(memory_space=pl.ANY)
    V = pltpu.VMEM
    dma = pltpu.SemaphoreType.DMA
    keys = Lr + Cp
    Q = R - 1
    N = 2 * P * rows
    pairw = LANES + VALUE_DIM
    quad, wide = groups(P, Q * Rr, keys - Rr)
    most = max(2 * keys, quad * Q * Rr, wide * (keys - Rr))
    weights = (query_first, query_second, key_first, key_second, value_weight)
    return pl.pallas_call(
        functools.partial(kernel, (S, T, G, R, Cr, cw)),
        out_shape=jax.ShapeDtypeStruct((rows, D), BF16),
        in_specs=[hb] * 10 + [sm, sm, vm, hb, vm, vm, vm, vm],
        out_specs=vm,
        scratch_shapes=[V(w.shape, BF16) for w in weights]
        + [
            V((T,) + output_weight.shape, BF16),
            V((Cp, D), BF16),
            V((2, depth), F32),
            V((depth, cp), BF16),
            V((2, Lr, LANES), F32),
            V((keys + Q * Rr, LANES), F32),
            V((keys + Q * Rr, LANES), F32),
            V((S * T, 2, cp), F32),
            V((2, 3 * D), F32),
            V((T, rows, D), BF16),
            V((Q, T, chunks, rc, D), BF16),
            V((keys, D), F32),
            V((keys, D), BF16),
            V((Q * Rr, D), BF16),
            V((G, Lr, LANES), BF16),
            V((G, keys, pairw), BF16),
            V((G, Q * Rr, pairw), BF16),
            V((P, rows, LANES), BF16),
            V((N, LANES), BF16),
            V((P, keys, pairw), BF16),
            V((P, Q * Rr, pairw), BF16),
            V((Q * P, keys - Rr, pairw), BF16),
            V((most, N), F32),
            V((most, N), F32),
            V((VALUE_DIM + 16, most), BF16),
            V((VALUE_DIM + 16, most), BF16),
            V((1, N), F32),
            V((1, N), F32),
            V((1, N), F32),
            V((VALUE_DIM + 16, N), F32),
            V((P, rows, VALUE_DIM), BF16),
            V((P, rows, VALUE_DIM), BF16),
            V((T, 2 * G, LANES), F32),
            dma((6,)), dma((5,)),
            dma((S * T,)), dma((S * T,)),
            dma((T,)), dma((T,)), dma((T,)), dma((T,)), dma((T,)), dma((T,)),
            dma((Q, chunks)), dma((Q, chunks)), dma((Q, chunks, T)), dma((Q, chunks, T)),
            dma((G, T)), dma((P,)),
            dma((G,)), dma((P,)), dma((G, Q)), dma((Q * P,)), dma((G,)), dma((P,)),
            dma((P, T)), dma((Q * P, T)), dma((P, T)),
            dma((P,)), dma((P,)),
        ],
        compiler_params=pltpu.CompilerParams(
            collective_id=0, has_side_effects=True, vmem_limit_bytes=62 * 1024 * 1024
        ),
    )(
        latent, context, condition[None, :], context_condition[None, :], modulation_weight,
        query_first, query_second, key_first, key_second, value_weight,
        lambda_head, context_score_boost, head_gain[None, :], output_weight, *tables,
    )


def general_kernel(
    dims,
    latent_ref, context_ref, cond_ref, ccond_ref, modw_ref,
    wq1_hbm, wq2_hbm, wk1_hbm, wk2_hbm, wv_hbm,
    lam_ref, boost_ref, gain_ref, wo_hbm, crow_ref, srow_ref, ccol_ref, scol_ref,
    out_ref,
    wq1, wq2, wk1, wk2, wv, wo,
    cos_ref, sin_ref, sig, modp, modall, modrow, lat, nrm, h,
    qs, kvs, q, kv, mx, acc, ho, hr, rsend, rs,
    wsem, mp_s, mp_r, lt_s, lt_r, ma_s, ma_r,
    q_s, q_r, kz_s, kv_s, kv_r, ho_s, ho_r, rs_s, rs_r,
):
    S, T, G, R, B, Cr, cw = dims
    s, t = lax.axis_index("sp"), lax.axis_index("tp")
    g, r = s // R, s % R
    rows, D = latent_ref.shape
    Lr = rows * T
    Cp = context_ref.shape[0]

    def remote(src, dst, send, recv, sp, tp):
        return pltpu.make_async_remote_copy(
            src_ref=src, dst_ref=dst, send_sem=send, recv_sem=recv,
            device_id=(sp, tp), device_id_type=MESH,
        )

    loads = [
        pltpu.make_async_copy(a, b, wsem.at[i])
        for i, (a, b) in enumerate(
            [(wq1_hbm, wq1), (wq2_hbm, wq2), (wk1_hbm, wk1), (wk2_hbm, wk2), (wv_hbm, wv), (wo_hbm, wo)]
        )
    ]
    for load in loads:
        load.start()

    barrier = pltpu.get_barrier_semaphore()

    @pl.loop(1, S)
    def _(i):
        pl.semaphore_signal(barrier, inc=1, device_id=((s + i) % S, t), device_id_type=MESH)

    for i in range(1, T):
        pl.semaphore_signal(barrier, inc=1, device_id=(s, (t + i) % T), device_id_type=MESH)

    for i in range(Lr // GRID_W):
        span, at = slice(i * GRID_W, (i + 1) * GRID_W), pl.ds(s * (Lr // GRID_W) + i, 1)
        cos_ref[span, :] = ccol_ref[...] + crow_ref[at, :]
        sin_ref[span, :] = scol_ref[...] + srow_ref[at, :]
    cos_ref[Lr:, :] = jnp.ones((Cp, LANES), F32)
    sin_ref[Lr:, :] = jnp.zeros((Cp, LANES), F32)

    for i, ref in enumerate((cond_ref, ccond_ref)):
        v = ref[...]
        sig[i : i + 1, :] = v / (1.0 + jnp.exp(-v))
    modp[t] = jnp.dot(sig[...].astype(BF16), modw_ref[...], preferred_element_type=F32)

    pl.semaphore_wait(barrier, S - 1 + T - 1)

    def part_copy(i):
        return remote(modp.at[t], modp.at[t], mp_s.at[i], mp_r.at[t], s, (t + i) % T)

    def latent_copy(i):
        return remote(latent_ref, lat.at[t], lt_s.at[i], lt_r.at[t], s, (t + i) % T)

    for i in range(1, T):
        part_copy(i).start()
    for i in range(1, T):
        latent_copy(i).start()
    lat[t] = latent_ref[...]
    for i in range(1, T):
        o = (t + i) % T
        remote(modp.at[o], modp.at[o], mp_s.at[i], mp_r.at[o], s, o).wait_recv()
    total = modp[0]
    for i in range(1, T):
        total = total + modp[i]
    modall[s] = total

    def mod_copy(i, src):
        return remote(modall.at[src], modall.at[src], ma_s.at[i], ma_r.at[src], (s + i) % S, t)

    @pl.loop(1, S)
    def _(i):
        mod_copy(i, s).start()

    for i in range(1, T):
        o = (t + i) % T
        remote(lat.at[o], lat.at[o], lt_s.at[i], lt_r.at[o], s, o).wait_recv()
    step = math.gcd(rows, 32)
    for i in range(T):

        @pl.loop(0, rows // step)
        def _(j):
            at = pl.multiple_of(j * step, step)
            nrm[pl.ds(i * rows + at, step), :] = normed_rows(lat[i, pl.ds(at, step), :])

    nrm[Lr:, :] = normed_rows(context_ref[...])

    @pl.loop(1, S)
    def _(i):
        mod_copy(i, (s + i) % S).wait_recv()

    for i in range(S):
        modrow[:, i * cw : (i + 1) * cw] = modall[i][:, :cw]

    @pl.loop(0, Lr // step)
    def _(j):
        at = pl.ds(pl.multiple_of(j * step, step), step)
        h[at, :] = (nrm[at, :] * (1.0 + modrow[0:1, D : 2 * D]) + modrow[0:1, :D]).astype(BF16)

    h[Lr:, :] = (nrm[Lr:, :] * (1.0 + modrow[1:2, D : 2 * D]) + modrow[1:2, :D]).astype(BF16)

    for i in range(2):
        loads[i].wait()
    lh = h[:Lr, :]
    one = jnp.dot(lh, wq1[...], preferred_element_type=F32)
    two = jnp.dot(lh, wq2[...], preferred_element_type=F32)
    for i in range(G):
        cut = slice(i * HEAD_DIM, (i + 1) * HEAD_DIM)
        pair = jnp.concatenate([one[:, cut], two[:, cut]], axis=1)
        turned = rotate(pair, cos_ref[:Lr, :], sin_ref[:Lr, :])
        qs[i] = (turned * (LOG2E * HEAD_DIM**-0.5)).astype(BF16)

    def q_out(i):
        to = (g + i) % G
        return remote(qs.at[to], q.at[g], q_s.at[i], q_r.at[g], to * R + r, t)

    for i in range(1, G):
        q_out(i).start()
    q[g] = qs[g]

    for i in range(2, 5):
        loads[i].wait()
    hh = h[...]
    one = jnp.dot(hh, wk1[...], preferred_element_type=F32)
    two = jnp.dot(hh, wk2[...], preferred_element_type=F32)
    for i in range(G):
        cut = slice(i * HEAD_DIM, (i + 1) * HEAD_DIM)
        pair = jnp.concatenate([one[:, cut], two[:, cut]], axis=1)
        kvs[i, :, :LANES] = rotate(pair, cos_ref[...], sin_ref[...]).astype(BF16)
    val = jnp.dot(hh, wv[...], preferred_element_type=F32)
    for i in range(G):
        kvs[i, :, LANES:] = val[:, i * VALUE_DIM : (i + 1) * VALUE_DIM].astype(BF16)

    def kv_out(i):
        to = (g + i) % G
        return remote(kvs.at[to], kv.at[s], kz_s.at[i], kv_r.at[s], to * R + r, t)

    for i in range(1, G):
        kv_out(i).start()
    kv[s] = kvs[g]

    def forward(i, j):
        src = ((g + G - i) % G) * R + r
        return remote(kv.at[src], kv.at[src], kv_s.at[i, j], kv_r.at[src], g * R + (r + j) % R, t)

    def landed(src):
        remote(kv.at[src], kv.at[src], kz_s.at[0], kv_r.at[src], s, t).wait_recv()

    def forward_all(i):
        @pl.loop(1, R)
        def _(j):
            forward(i, j).start()

    forward_all(0)
    mx[...] = jnp.full(mx.shape, NEGATIVE, F32)
    acc[...] = jnp.zeros(acc.shape, F32)
    boost = boost_ref[g] * LOG2E

    for i in range(1, G):
        o = (g + i) % G
        remote(q.at[o], q.at[o], q_s.at[i], q_r.at[o], s, t).wait_recv()

    def attend(n, at):
        k_l = kv[pl.ds(at, B), :Lr, :LANES].reshape(B * Lr, LANES)
        v_l = kv[pl.ds(at, B), :Lr, LANES:].reshape(B * Lr, VALUE_DIM)
        k_c = kv[pl.ds(at, B), Lr:, :LANES].reshape(B * Cp, LANES)
        v_c = kv[pl.ds(at, B), Lr:, LANES:].reshape(B * Cp, VALUE_DIM)
        v_l = jnp.concatenate([v_l, jnp.ones_like(v_l)], axis=1)
        v_c = jnp.concatenate([v_c, jnp.ones_like(v_c)], axis=1)
        nt = (((1,), (1,)), ((), ()))
        QB = min(Lr, QROWS)
        for m, c in [(m, c) for c in range(Lr // QB) for m in range(2)]:
            part = slice(c * QB, (c + 1) * QB)
            qq = q[n, part, :]
            lane = lax.broadcasted_iota(jnp.int32, qq.shape, 1)
            qm = jnp.where(lane // HEAD_DIM == m, qq, jnp.zeros_like(qq))
            s_l = lax.dot_general(qm, k_l, nt, preferred_element_type=F32)
            s_c = lax.dot_general(qm, k_c, nt, preferred_element_type=F32) + boost
            if Cp != Cr:
                spot = lax.broadcasted_iota(jnp.int32, s_c.shape, 1)
                s_c = jnp.where(spot % Cp < Cr, s_c, NEGATIVE)
            old = mx[m, n, part, :]
            peak = jnp.maximum(
                old,
                jnp.maximum(
                    jnp.max(s_l, axis=-1, keepdims=True), jnp.max(s_c, axis=-1, keepdims=True)
                ),
            )
            p_l = jnp.exp2(s_l - peak).astype(BF16)
            p_c = jnp.exp2(s_c - peak).astype(BF16)
            mx[m, n, part, :] = peak
            acc[m, n, part, :] = (
                jnp.exp2(old - peak) * acc[m, n, part, :]
                + jnp.dot(p_l, v_l, preferred_element_type=F32)
                + jnp.dot(p_c, v_c, preferred_element_type=F32)
            )

    lam = lam_ref[g]
    gain = gain_ref[...]

    def finish(n):
        one = acc[0, n, :, :VALUE_DIM] / acc[0, n, :, VALUE_DIM:]
        two = acc[1, n, :, :VALUE_DIM] / acc[1, n, :, VALUE_DIM:]
        mixed = one - lam * two
        mixed = mixed * lax.rsqrt(jnp.mean(mixed * mixed, axis=-1, keepdims=True) + EPSILON) * gain
        return mixed.astype(BF16)

    def ho_out(i):
        to = (g + i) % G
        return remote(ho.at[to], hr.at[g], ho_s.at[i], ho_r.at[g], to * R + r, t)

    def pass_on(i):
        landed(((g + G - i) % G) * R + r)
        forward_all(i)

    for i in range(G):
        if i == 1 and G > 2:
            pass_on(2)
        base = ((g + G - i) % G) * R

        @pl.loop(1, R)
        def _(j):
            landed(base + (r + j) % R)

        if i + 1 < G:
            half = G // 2
            for low, high in ((0, half), (half, G)):
                if low and i == 0:
                    pass_on(1)
                elif low and i + 2 < G:
                    pass_on(i + 2)

                @pl.loop(low * (R // B), high * (R // B))
                def _(x):
                    attend(x // (R // B), base + x % (R // B) * B)

        else:

            @pl.loop(1, G + 1)
            def _(y):
                n = (g + y) % G

                @pl.loop(0, R // B)
                def _(x):
                    attend(n, base + x * B)

                ho[n] = finish(n)

                @pl.when(y < G)
                def _():
                    ho_out(y).start()

    hr[g] = ho[g]
    loads[5].wait()
    for i in range(1, G):
        o = (g + i) % G
        remote(hr.at[o], hr.at[o], ho_s.at[i], ho_r.at[o], s, t).wait_recv()

    def branch_rows(o):
        at = pl.multiple_of(o * rows, rows)
        mine = jnp.concatenate([hr[i, pl.ds(at, rows), :] for i in range(G)], axis=1)
        return jnp.dot(mine, wo[...], preferred_element_type=F32)

    def rs_out(i):
        o = (t + i) % T
        return remote(rsend.at[o], rs.at[t], rs_s.at[i], rs_r.at[t], s, o)

    for i in range(1, T):
        o = (t + i) % T
        rsend[o] = branch_rows(o).astype(BF16)
        rs_out(i).start()
    branch = branch_rows(t)
    for i in range(1, T):
        o = (t + i) % T
        remote(rs.at[o], rs.at[o], rs_s.at[i], rs_r.at[o], s, o).wait_recv()
        branch = branch + rs[o].astype(F32)
    out_ref[...] = (latent_ref[...].astype(F32) + modrow[0:1, 2 * D :] * branch).astype(BF16)

    for i in range(1, T):
        part_copy(i).wait_send()
        latent_copy(i).wait_send()
        rs_out(i).wait_send()

    @pl.loop(1, S)
    def _(i):
        mod_copy(i, s).wait_send()

    for i in range(1, G):
        kv_out(i).wait_send()
        q_out(i).wait_send()
        ho_out(i).wait_send()
    for i in range(G):

        @pl.loop(1, R)
        def _(j):
            forward(i, j).wait_send()


def general_body(
    S, T,
    latent, context, condition, context_condition, modulation_weight,
    query_first, query_second, key_first, key_second, value_weight,
    lambda_head, context_score_boost, head_gain, output_weight,
):
    rows, D = latent.shape
    Lr = rows * T
    G = value_weight.shape[1] // VALUE_DIM
    assert S % G == 0
    R = S // G
    B = math.gcd(R, 4)
    Cr = context.shape[0]
    Cp = -(-Cr // 16) * 16
    if Cp != Cr:
        context = jnp.pad(context, ((0, Cp - Cr), (0, 0)))
    cw = modulation_weight.shape[1]
    cp = -(-cw // LANES) * LANES
    if cp != cw:
        modulation_weight = jnp.pad(modulation_weight, ((0, 0), (0, cp - cw)))
    depth = modulation_weight.shape[0]
    assert Lr % GRID_W == 0
    tables = rotation_tables(S * Lr // GRID_W)
    vm = pl.BlockSpec(memory_space=pltpu.VMEM)
    sm = pl.BlockSpec(memory_space=pltpu.SMEM)
    hb = pl.BlockSpec(memory_space=pl.ANY)
    V = pltpu.VMEM
    dma = pltpu.SemaphoreType.DMA
    weights = (query_first, query_second, key_first, key_second, value_weight, output_weight)
    return pl.pallas_call(
        functools.partial(general_kernel, (S, T, G, R, B, Cr, cw)),
        out_shape=jax.ShapeDtypeStruct((rows, D), BF16),
        in_specs=[vm] * 5 + [hb] * 5 + [sm, sm, vm, hb, vm, vm, vm, vm],
        out_specs=vm,
        scratch_shapes=[V(w.shape, BF16) for w in weights]
        + [
            V((Lr + Cp, LANES), F32),
            V((Lr + Cp, LANES), F32),
            V((2, depth), F32),
            V((T, 2, cp), F32),
            V((S, 2, cp), F32),
            V((2, 3 * D), F32),
            V((T, rows, D), BF16),
            V((Lr + Cp, D), F32),
            V((Lr + Cp, D), BF16),
            V((G, Lr, LANES), BF16),
            V((G, Lr + Cp, LANES + VALUE_DIM), BF16),
            V((G, Lr, LANES), BF16),
            V((S, Lr + Cp, LANES + VALUE_DIM), BF16),
            V((2, G, Lr, 1), F32),
            V((2, G, Lr, 2 * VALUE_DIM), F32),
            V((G, Lr, VALUE_DIM), BF16),
            V((G, Lr, VALUE_DIM), BF16),
            V((T, rows, D), BF16),
            V((T, rows, D), BF16),
            dma((6,)),
            dma((T,)), dma((T,)), dma((T,)), dma((T,)), dma((S,)), dma((S,)),
            dma((G,)), dma((G,)), dma((G,)), dma((G, R)), dma((S,)),
            dma((G,)), dma((G,)), dma((T,)), dma((T,)),
        ],
        compiler_params=pltpu.CompilerParams(
            collective_id=0, has_side_effects=True, vmem_limit_bytes=62 * 1024 * 1024
        ),
    )(
        latent, context, condition[None, :], context_condition[None, :], modulation_weight,
        query_first, query_second, key_first, key_second, value_weight,
        lambda_head, context_score_boost, head_gain[None, :], output_weight, *tables,
    )


def solution(mesh):
    in_specs = (
        P(("sp", "tp"), None),
        P("sp", None),
        P("tp"),
        P("tp"),
        P("tp", "sp"),
        P(None, "tp"),
        P(None, "tp"),
        P(None, "tp"),
        P(None, "tp"),
        P(None, "tp"),
        P("tp"),
        P("tp"),
        P(),
        P("tp", None),
    )
    out_specs = P(("sp", "tp"), None)
    S, T = mesh.shape["sp"], mesh.shape["tp"]
    run = functools.partial(body if T == 2 else general_body, S, T)
    return jax.shard_map(run, mesh=mesh, in_specs=in_specs, out_specs=out_specs, check_vma=False)
```

```python
import functools
import math

import jax
import jax.numpy as jnp
import numpy as np
from jax import lax
from jax.experimental import pallas as pl
from jax.experimental.pallas import tpu as pltpu
from jax.sharding import PartitionSpec as P

HEAD_DIM = 64
VALUE_DIM = 128
GRID_W = 64
EPSILON = 1e-06
THETA = 10000.0
NEGATIVE = -1e30
LOG2E = math.log2(math.e)
MESH = pl.DeviceIdType.MESH
BF16 = jnp.bfloat16
F32 = jnp.float32
LANES = 128
QROWS = 256


def rotation_tables(grid_rows):
    half = HEAD_DIM // 2
    quarter = half // 2
    lane = np.arange(LANES) % HEAD_DIM
    rate = (THETA ** (-(lane % quarter) / quarter)).astype(np.float32)
    sign = np.where(lane % half < quarter, -1.0, 1.0)
    tables = []
    for count, mask in ((grid_rows, lane < half), (GRID_W, lane >= half)):
        angle = np.arange(count, dtype=np.float32)[:, None] * rate[None, :]
        for table in (np.cos(angle), np.sin(angle) * sign):
            tables.append(np.where(mask, table, 0.0).astype(np.float32))
    return tables


def rotate(x, cosine, sine):
    quarter = HEAD_DIM // 4
    lane = lax.broadcasted_iota(jnp.int32, x.shape, 1)
    ahead = pltpu.roll(x, LANES - quarter, 1)
    behind = pltpu.roll(x, quarter, 1)
    flipped = jnp.where(lane % (2 * quarter) < quarter, ahead, behind)
    return x * cosine + flipped * sine


def normed_rows(rows):
    v = rows.astype(F32)
    return v * lax.rsqrt(jnp.mean(v * v, axis=-1, keepdims=True) + EPSILON)


def flip(v, k, span):
    out = 0
    bit = 1
    while bit < span:
        out = out + bit * ((v // bit + k // bit) % 2)
        bit *= 2
    return out


def groups(P, raw_rows, far_rows):
    return math.gcd(P, max(1, 400 // raw_rows)), math.gcd(P, max(1, 512 // far_rows))


def kernel(
    dims,
    lat_hbm, ctx_hbm, cond_hbm, ccond_hbm, modw_hbm,
    wq1_hbm, wq2_hbm, wk1_hbm, wk2_hbm, wv_hbm,
    lam_ref, boost_ref, gain_ref, wo_hbm, crow_ref, srow_ref, ccol_ref, scol_ref,
    out_ref,
    wq1, wq2, wk1, wk2, wv, wo,
    ctx, cond, modw, tab, cos_ref, sin_ref, mt, mp, modrow, lat, raw, nrm, h, hraw,
    qs, kvs, kvrs, q, qb, kvn, kvr, kvf, s0, s1, vt0, pk0, mx, acc, ho, hr, lb,
    wsem, isem, mt_s, mt_r, mp_s, mp_r, lt_s, lt_r, lb_s, lb_r, wo_s, wo_r,
    rw_s, rw_r, rf_s, rf_r, q_s, q_r, kn_s, kn_r, kf_s, kf_r, kr_s, kr_r, fn_s, ff_s, fr_s, ho_s, ho_r,
):
    S, T, G, R, Cr, cw = dims
    P = T * G
    s, t = lax.axis_index("sp"), lax.axis_index("tp")
    g, p0 = s // P, s % P
    prim, hown = p0 // G, p0 % G
    mine = t == prim
    other = jnp.logical_not(mine)
    _, rows, D = lat.shape
    Lr = rows * T
    Cp = ctx.shape[0]
    keys = Lr + Cp
    Q = R - 1
    chunks, rc = raw.shape[2], raw.shape[3]
    rw = chunks * rc
    Rr = T * rw
    N = 2 * P * rows
    quad, wide = groups(P, Q * Rr, keys - Rr)

    def remote(src, dst, send, recv, sp, tp):
        return pltpu.make_async_remote_copy(
            src_ref=src, dst_ref=dst, send_sem=send, recv_sem=recv,
            device_id=(sp, tp), device_id_type=MESH,
        )

    def arrived(buf, recv):
        remote(buf, buf, lt_s.at[0], recv, s, t).wait_recv()

    barrier = pltpu.get_barrier_semaphore()

    @pl.loop(1, S)
    def _(i):
        pl.semaphore_signal(barrier, inc=1, device_id=((s + i) % S, t), device_id_type=MESH)

    for i in range(1, T):
        pl.semaphore_signal(barrier, inc=1, device_id=(s, (t + i) % T), device_id_type=MESH)

    inputs = [
        pltpu.make_async_copy(a, b, isem.at[i])
        for i, (a, b) in enumerate(
            [(cond_hbm, cond.at[0:1]), (ccond_hbm, cond.at[1:2]), (modw_hbm, modw),
             (lat_hbm, lat.at[t]), (ctx_hbm, ctx)]
        )
    ]
    for load in inputs:
        load.start()
    loads = [
        pltpu.make_async_copy(a, b, wsem.at[i])
        for i, (a, b) in enumerate(
            [(wk1_hbm, wk1), (wk2_hbm, wk2), (wv_hbm, wv), (wq1_hbm, wq1), (wq2_hbm, wq2), (wo_hbm, wo.at[t])]
        )
    ]
    for load in loads:
        load.start()

    for i in range(G):
        lb[t, i : i + 1, :] = jnp.full((1, LANES), lam_ref[i], F32)
        lb[t, G + i : G + i + 1, :] = jnp.full((1, LANES), boost_ref[i] * LOG2E, F32)

    for i in range(3):
        inputs[i].wait()
    v = cond[...]
    sig = v / (1.0 + jnp.exp(-v))
    mt[t] = jnp.dot(sig.astype(BF16), modw[...], preferred_element_type=F32)
    for i in range(3, 5):
        inputs[i].wait()

    pl.semaphore_wait(barrier, S - 1 + T - 1)

    def mt_copy(i):
        return remote(mt.at[t], mt.at[t], mt_s.at[i], mt_r.at[t], s, (t + i) % T)

    def mp_copy(i):
        return remote(mp.at[s], mp.at[s], mp_s.at[i], mp_r.at[s], (s + i) % S, t)

    def lat_copy(i):
        return remote(lat.at[t], lat.at[t], lt_s.at[i], lt_r.at[t], s, (t + i) % T)

    def lb_copy(i):
        return remote(lb.at[t], lb.at[t], lb_s.at[i], lb_r.at[t], s, (t + i) % T)

    def wo_copy(i):
        return remote(wo.at[t], wo.at[t], wo_s.at[i], wo_r.at[t], s, (t + i) % T)

    def raw_copy(j, c):
        return remote(
            lat.at[t, pl.ds(c * rc, rc)], raw.at[j - 1, t, c], rw_s.at[j - 1, c],
            rw_r.at[j - 1, c], (g + R - j) % R * P + p0, t,
        )

    def raw_pass(j, c, i):
        part = raw.at[j - 1, t, c]
        return remote(
            part, part, rf_s.at[j - 1, c, i], rf_r.at[j - 1, c, t], s, (t + i) % T
        )

    for i in range(1, T):
        mt_copy(i).start()
    for i in range(1, T):
        o = (t + i) % T
        arrived(mt.at[o], mt_r.at[o])
    total = mt[0]
    for i in range(1, T):
        total = total + mt[i]
    mp[s] = total

    @pl.loop(1, S)
    def _(i):
        mp_copy(i).start()

    for i in range(1, T):
        lat_copy(i).start()
        lb_copy(i).start()
    for c in range(chunks):
        for j in range(1, R):
            raw_copy(j, c).start()
    loads[5].wait()
    for i in range(1, T):
        wo_copy(i).start()

    def table(src, out, order):
        for n, (col, row) in enumerate(((ccol_ref, crow_ref), (scol_ref, srow_ref))):
            for i in range(Lr // GRID_W):
                at = pl.ds(src * (Lr // GRID_W) + i, 1)
                tab[n, i * GRID_W : (i + 1) * GRID_W, :] = col[...] + row[at, :]
            at = out
            for low, high in order:
                ref = sin_ref if n else cos_ref
                ref[at : at + high - low, :] = tab[n, low:high, :]
                at += high - low

    head = [(i * rows, i * rows + rw) for i in range(T)]
    rest = [(i * rows + rw, (i + 1) * rows) for i in range(T)]
    table(s, 0, head + rest)
    cos_ref[Lr : Lr + Cp, :] = jnp.ones((Cp, LANES), F32)
    sin_ref[Lr : Lr + Cp, :] = jnp.zeros((Cp, LANES), F32)
    for j in range(1, R):
        table((g + j) % R * P + p0, Lr + Cp + (j - 1) * Rr, head)

    step = math.gcd(rw, rows - rw, 32)

    def norm_lat(i):
        for low, size, at in ((0, rw, i * rw), (rw, rows - rw, Rr + i * (rows - rw))):

            @pl.loop(0, size // step)
            def _(j):
                off = pl.multiple_of(j * step, step)
                to = pl.ds(pl.multiple_of(at + off, step), step)
                nrm[to, :] = normed_rows(lat[i, pl.ds(low + off, step), :])

    nrm[Lr:, :] = normed_rows(ctx[...])
    norm_lat(t)
    for i in range(1, T):
        o = (t + i) % T
        arrived(lat.at[o], lt_r.at[o])
        norm_lat(o)

    @pl.loop(1, S)
    def _(i):
        o = (s + i) % S
        arrived(mp.at[o], mp_r.at[o])

    for i in range(S):
        modrow[:, i * cw : (i + 1) * cw] = mp[i][:, :cw]

    @pl.loop(0, Lr // step)
    def _(j):
        at = pl.ds(pl.multiple_of(j * step, step), step)
        h[at, :] = (nrm[at, :] * (1.0 + modrow[0:1, D : 2 * D]) + modrow[0:1, :D]).astype(BF16)

    h[Lr:, :] = (nrm[Lr:, :] * (1.0 + modrow[1:2, D : 2 * D]) + modrow[1:2, :D]).astype(BF16)

    def project(hh, at, out):
        n = hh.shape[0]
        one = jnp.dot(hh, wk1[...], preferred_element_type=F32)
        two = jnp.dot(hh, wk2[...], preferred_element_type=F32)
        for i in range(G):
            cut = slice(i * HEAD_DIM, (i + 1) * HEAD_DIM)
            pair = jnp.concatenate([one[:, cut], two[:, cut]], axis=1)
            turned = rotate(pair, cos_ref[at : at + n, :], sin_ref[at : at + n, :])
            out[i, :, :LANES] = turned.astype(BF16)
        val = jnp.dot(hh, wv[...], preferred_element_type=F32)
        for i in range(G):
            out[i, :, LANES:] = val[:, i * VALUE_DIM : (i + 1) * VALUE_DIM].astype(BF16)

    for i in range(3, 5):
        loads[i].wait()
    lh = h[:Lr, :]
    one = jnp.dot(lh, wq1[...], preferred_element_type=F32)
    two = jnp.dot(lh, wq2[...], preferred_element_type=F32)
    for i in range(G):
        cut = slice(i * HEAD_DIM, (i + 1) * HEAD_DIM)
        pair = jnp.concatenate([one[:, cut], two[:, cut]], axis=1)
        turned = rotate(pair, cos_ref[:Lr, :], sin_ref[:Lr, :])
        turned = (turned * (LOG2E * HEAD_DIM**-0.5)).astype(BF16)
        at = 0
        for low, high in head + rest:
            qs[i, low:high, :] = turned[at : at + high - low]
            at += high - low

    def q_out(i, j):
        hl = flip(hown, i, G)
        to = (t + j) % T
        part = pl.ds(pl.multiple_of(to * rows, rows), rows)
        return remote(qs.at[hl, part], q.at[p0], q_s.at[i, j], q_r.at[p0], g * P + t * G + hl, to)

    @pl.when(mine)
    def _():
        q[p0] = qs[hown, pl.ds(pl.multiple_of(t * rows, rows), rows), :]

    @pl.when(other)
    def _():
        q_out(0, 0).start()

    for j in range(1, T):
        q_out(0, j).start()
    for i in range(1, G):
        for j in range(T):
            q_out(i, j).start()
    for i in range(3):
        loads[i].wait()
    project(h[...], 0, kvs)

    def near_out(i):
        hl = flip(hown, i, G)
        return remote(kvs.at[hl], kvn.at[p0], kn_s.at[i], kn_r.at[p0], g * P + t * G + hl, t)

    def far_out(i, j):
        hl = flip(hown, i, G)
        to = (g + R - j) % R
        slot = (j - 1) * P + p0
        return remote(
            kvs.at[hl, pl.ds(Rr, Lr + Cp - Rr)], kvf.at[slot], kf_s.at[i, j - 1], kf_r.at[slot],
            to * P + t * G + hl, t,
        )

    def raw_out(i):
        hl = flip(hown, i, G)
        return remote(kvrs.at[hl], kvr.at[p0], kr_s.at[i], kr_r.at[p0], g * P + t * G + hl, t)

    @pl.when(mine)
    def _():
        kvn[p0] = kvs[hown]

    @pl.when(other)
    def _():
        near_out(0).start()

    for i in range(1, G):
        near_out(i).start()
    for i in range(G):
        for j in range(1, R):
            far_out(i, j).start()


    for c in range(chunks):
        for j in range(1, R):
            arrived(raw.at[j - 1, t, c], rw_r.at[j - 1, c])
            for i in range(1, T):
                raw_pass(j, c, i).start()

    def lift(j, o, c):
        part = normed_rows(raw[j - 1, o, c])
        part = part * (1.0 + modrow[0:1, D : 2 * D]) + modrow[0:1, :D]
        at = pl.multiple_of((j - 1) * Rr + o * rw + c * rc, rc)
        hraw[pl.ds(at, rc), :] = part.astype(BF16)

    for j in range(1, R):
        for c in range(chunks):
            lift(j, t, c)
    for i in range(1, T):
        o = (t + i) % T
        for c in range(chunks):
            for j in range(1, R):
                arrived(raw.at[j - 1, o, c], rf_r.at[j - 1, c, o])
                lift(j, o, c)
    project(hraw[...], Lr + Cp, kvrs)

    @pl.when(mine)
    def _():
        kvr[p0] = kvrs[hown]

    @pl.when(other)
    def _():
        raw_out(0).start()

    for i in range(1, G):
        raw_out(i).start()

    mx[...] = jnp.full(mx.shape, NEGATIVE, F32)
    acc[...] = jnp.zeros(acc.shape, F32)
    vt0[VALUE_DIM:, :] = jnp.ones((vt0.shape[0] - VALUE_DIM, vt0.shape[1]), BF16)
    for i in range(1, T):
        o = (t + i) % T
        arrived(lb.at[o], lb_r.at[o])
    lam = lb[prim, pl.ds(hown, 1), :][:, :rows]
    boost = lb[prim, pl.ds(G + hown, 1), :][:, :1]
    gain = jnp.broadcast_to(gain_ref[...], (VALUE_DIM, LANES)).T[:, :rows]
    nt = (((1,), (1,)), ((), ()))

    def to_core(buf, slot, send, recv, i):
        return remote(
            buf.at[slot], buf.at[slot], send.at[slot, i], recv.at[slot], s, (t + i) % T
        )

    def spread(buf, slots, send, recv, own):
        @pl.when(mine)
        def _():
            for slot in slots:
                if own:

                    @pl.when(slot != p0)
                    def _():
                        arrived(buf.at[slot], recv.at[slot])

                else:
                    arrived(buf.at[slot], recv.at[slot])
                for i in range(1, T):
                    to_core(buf, slot, send, recv, i).start()

    def settle(buf, slots, recv):
        @pl.when(other)
        def _():
            for slot in slots:
                arrived(buf.at[slot], recv.at[slot])

    half = N // 2
    banks = (s0, s1)

    def scores(buf, base, count, low, c):
        cols = slice(c * half, (c + 1) * half)
        at = pl.ds(base, count)
        n = count * low
        m = count * (buf.shape[1] - low)
        s_ref, vt = banks[c], vt0
        keys = buf[at, :low, :LANES].reshape(n, LANES)
        sc = lax.dot_general(keys, qb[cols, :], nt, preferred_element_type=F32)
        s_ref[:n, :] = sc
        peak = jnp.max(sc, axis=0, keepdims=True)
        if c == 0:
            vals = buf[at, :low, LANES:].reshape(n, VALUE_DIM)
            vt[:VALUE_DIM, :n] = vals.astype(F32).T.astype(BF16)
        if m:
            keys = buf[at, low:, :LANES].reshape(m, LANES)
            sc = lax.dot_general(keys, qb[cols, :], nt, preferred_element_type=F32) + boost
            if Cp != Cr:
                spot = lax.broadcasted_iota(jnp.int32, sc.shape, 0)
                sc = jnp.where(spot % Cp < Cr, sc, NEGATIVE)
            s_ref[n : n + m, :] = sc
            peak = jnp.maximum(peak, jnp.max(sc, axis=0, keepdims=True))
            if c == 0:
                vals = buf[at, low:, LANES:].reshape(m, VALUE_DIM)
                vt[:VALUE_DIM, n : n + m] = vals.astype(F32).T.astype(BF16)
        pk0[:, cols] = peak

    def weigh(n, c):
        cols = slice(c * half, (c + 1) * half)
        old = mx[:, cols]
        peak = jnp.maximum(old, pk0[:, cols])
        pr = jnp.exp2(banks[c][:n, :] - peak).astype(BF16)
        mx[:, cols] = peak
        acc[:, cols] = jnp.exp2(old - peak) * acc[:, cols] + jnp.dot(
            vt0[:, :n], pr, preferred_element_type=F32
        )

    def finish(j):
        u = acc[:VALUE_DIM, j * 2 * rows : (j + 1) * 2 * rows]
        u = u / acc[VALUE_DIM : VALUE_DIM + 1, j * 2 * rows : (j + 1) * 2 * rows]
        mixed = u[:, :rows] - lam * u[:, rows:]
        mixed = mixed * lax.rsqrt(jnp.mean(mixed * mixed, axis=0, keepdims=True) + EPSILON)
        ho[j] = (mixed * gain).T.astype(BF16)

    def ho_out(j):
        return remote(ho.at[j], hr.at[p0], ho_s.at[j], ho_r.at[p0], g * P + j, t)

    for j in range(P):

        @pl.when(jnp.logical_or(other, p0 != j))
        def _():
            arrived(q.at[j], q_r.at[j])

        qq = q[j]
        lane = lax.broadcasted_iota(jnp.int32, qq.shape, 1)
        zero = jnp.zeros_like(qq)
        qb[j * 2 * rows : j * 2 * rows + rows, :] = jnp.where(lane < HEAD_DIM, qq, zero)
        qb[j * 2 * rows + rows : (j + 1) * 2 * rows, :] = jnp.where(lane < HEAD_DIM, zero, qq)

    units = []
    for k in [*range(0, P // 2, 2), *range(1, P // 2, 2)]:
        units.append((kvn, flip(p0 // 2, k, P // 2) * 2, 2, Lr, fn_s, kn_r, True))
    for j in range(Q):
        for k in range(P // wide):
            base = j * P + flip(p0 // wide, k, P // wide) * wide
            units.append((kvf, base, wide, Lr - Rr, ff_s, kf_r, False))
    for k in range(P // quad):
        units.append((kvr, flip(p0 // quad, k, P // quad) * quad, quad, Q * Rr, fr_s, kr_r, True))
    def deliver(c):
        for j in range(c * P // 2, (c + 1) * P // 2):
            finish(j)

            @pl.when(p0 == j)
            def _():
                hr[j] = ho[j]

            @pl.when(p0 != j)
            def _():
                ho_out(j).start()

    for n, (buf, base, count, low, send, recv, own) in enumerate(units):
        spread(buf, [base + i for i in range(count)], send, recv, own)
        settle(buf, [base + i for i in range(count)], recv)
        size = count * buf.shape[1]
        scores(buf, base, count, low, 0)
        scores(buf, base, count, low, 1)
        weigh(size, 0)
        if n == len(units) - 1:
            deliver(0)
        weigh(size, 1)
    deliver(1)

    for i in range(1, T):
        o = (t + i) % T
        arrived(wo.at[o], wo_r.at[o])
    for i in range(1, P):
        o = flip(p0, i, P)
        arrived(hr.at[o], ho_r.at[o])

    branch = None
    for i in range(T):
        part = jnp.concatenate([hr[i * G + j] for j in range(G)], axis=1)
        term = jnp.dot(part, wo[i], preferred_element_type=F32)
        branch = term if branch is None else branch + term
    out_ref[...] = (lat[t].astype(F32) + modrow[0:1, 2 * D :] * branch).astype(BF16)

    for i in range(1, T):
        mt_copy(i).wait_send()

    @pl.loop(1, S)
    def _(i):
        mp_copy(i).wait_send()

    for i in range(1, T):
        lat_copy(i).wait_send()
        lb_copy(i).wait_send()
        wo_copy(i).wait_send()
    for j in range(1, R):
        for c in range(chunks):
            raw_copy(j, c).wait_send()
            for i in range(1, T):
                raw_pass(j, c, i).wait_send()

    @pl.when(other)
    def _():
        near_out(0).wait_send()
        raw_out(0).wait_send()
        q_out(0, 0).wait_send()

    for i in range(1, G):
        near_out(i).wait_send()
        raw_out(i).wait_send()
    for i in range(G):
        for j in range(1, R):
            far_out(i, j).wait_send()
        for j in range(T):
            if i + j > 0:
                q_out(i, j).wait_send()
    for i in range(1, P):
        ho_out(flip(p0, i, P)).wait_send()

    @pl.when(mine)
    def _():
        for buf, send, recv in ((kvn, fn_s, kn_r), (kvr, fr_s, kr_r), (kvf, ff_s, kf_r)):

            @pl.loop(0, buf.shape[0])
            def _(slot):
                for i in range(1, T):
                    to_core(buf, slot, send, recv, i).wait_send()


def body(
    S, T,
    latent, context, condition, context_condition, modulation_weight,
    query_first, query_second, key_first, key_second, value_weight,
    lambda_head, context_score_boost, head_gain, output_weight,
):
    rows, D = latent.shape
    Lr = rows * T
    G = value_weight.shape[1] // VALUE_DIM
    P = T * G
    assert S % P == 0 and P & (P - 1) == 0 and rows <= LANES
    R = S // P
    assert R > 1 and P > 1
    rc = 16
    chunks = rows * 3 // 8 // rc
    Rr = T * chunks * rc
    Cr = context.shape[0]
    Cp = -(-Cr // 16) * 16
    if Cp != Cr:
        context = jnp.pad(context, ((0, Cp - Cr), (0, 0)))
    cw = modulation_weight.shape[1]
    cp = -(-cw // LANES) * LANES
    if cp != cw:
        modulation_weight = jnp.pad(modulation_weight, ((0, 0), (0, cp - cw)))
    depth = modulation_weight.shape[0]
    assert Lr % GRID_W == 0
    tables = rotation_tables(S * Lr // GRID_W)
    vm = pl.BlockSpec(memory_space=pltpu.VMEM)
    sm = pl.BlockSpec(memory_space=pltpu.SMEM)
    hb = pl.BlockSpec(memory_space=pltpu.HBM)
    V = pltpu.VMEM
    dma = pltpu.SemaphoreType.DMA
    keys = Lr + Cp
    Q = R - 1
    N = 2 * P * rows
    pairw = LANES + VALUE_DIM
    quad, wide = groups(P, Q * Rr, keys - Rr)
    most = max(2 * keys, quad * Q * Rr, wide * (keys - Rr))
    weights = (query_first, query_second, key_first, key_second, value_weight)
    latent, context, modulation_weight, output_weight, *weights = (
        pltpu.with_memory_space_constraint(a, pltpu.HBM)
        for a in (latent, context, modulation_weight, output_weight, *weights)
    )
    query_first, query_second, key_first, key_second, value_weight = weights
    return pl.pallas_call(
        functools.partial(kernel, (S, T, G, R, Cr, cw)),
        out_shape=pltpu.VMEM((rows, D), BF16),
        in_specs=[hb] * 10 + [sm, sm, vm, hb, vm, vm, vm, vm],
        out_specs=vm,
        scratch_shapes=[V(w.shape, BF16) for w in weights]
        + [
            V((T,) + output_weight.shape, BF16),
            V((Cp, D), BF16),
            V((2, depth), F32),
            V((depth, cp), BF16),
            V((2, Lr, LANES), F32),
            V((keys + Q * Rr, LANES), F32),
            V((keys + Q * Rr, LANES), F32),
            V((T, 2, cp), F32),
            V((S, 2, cp), F32),
            V((2, 3 * D), F32),
            V((T, rows, D), BF16),
            V((Q, T, chunks, rc, D), BF16),
            V((keys, D), F32),
            V((keys, D), BF16),
            V((Q * Rr, D), BF16),
            V((G, Lr, LANES), BF16),
            V((G, keys, pairw), BF16),
            V((G, Q * Rr, pairw), BF16),
            V((P, rows, LANES), BF16),
            V((N, LANES), BF16),
            V((P, keys, pairw), BF16),
            V((P, Q * Rr, pairw), BF16),
            V((Q * P, keys - Rr, pairw), BF16),
            V((most, N // 2), F32),
            V((most, N // 2), F32),
            V((VALUE_DIM + 16, most), BF16),
            V((1, N), F32),
            V((1, N), F32),
            V((VALUE_DIM + 16, N), F32),
            V((P, rows, VALUE_DIM), BF16),
            V((P, rows, VALUE_DIM), BF16),
            V((T, 2 * G, LANES), F32),
            dma((6,)), dma((5,)),
            dma((T,)), dma((T,)), dma((S,)), dma((S,)),
            dma((T,)), dma((T,)), dma((T,)), dma((T,)), dma((T,)), dma((T,)),
            dma((Q, chunks)), dma((Q, chunks)), dma((Q, chunks, T)), dma((Q, chunks, T)),
            dma((G, T)), dma((P,)),
            dma((G,)), dma((P,)), dma((G, Q)), dma((Q * P,)), dma((G,)), dma((P,)),
            dma((P, T)), dma((Q * P, T)), dma((P, T)),
            dma((P,)), dma((P,)),
        ],
        compiler_params=pltpu.CompilerParams(
            collective_id=0, has_side_effects=True, vmem_limit_bytes=56 * 1024 * 1024
        ),
    )(
        latent, context, condition[None, :], context_condition[None, :], modulation_weight,
        query_first, query_second, key_first, key_second, value_weight,
        lambda_head, context_score_boost, head_gain[None, :], output_weight, *tables,
    )


def general_kernel(
    dims,
    latent_ref, context_ref, cond_ref, ccond_ref, modw_ref,
    wq1_hbm, wq2_hbm, wk1_hbm, wk2_hbm, wv_hbm,
    lam_ref, boost_ref, gain_ref, wo_hbm, crow_ref, srow_ref, ccol_ref, scol_ref,
    out_ref,
    wq1, wq2, wk1, wk2, wv, wo,
    cos_ref, sin_ref, sig, modp, modall, modrow, lat, nrm, h,
    qs, kvs, q, kv, mx, acc, ho, hr, rsend, rs,
    wsem, mp_s, mp_r, lt_s, lt_r, ma_s, ma_r,
    q_s, q_r, kz_s, kv_s, kv_r, ho_s, ho_r, rs_s, rs_r,
):
    S, T, G, R, B, Cr, cw = dims
    s, t = lax.axis_index("sp"), lax.axis_index("tp")
    g, r = s // R, s % R
    rows, D = latent_ref.shape
    Lr = rows * T
    Cp = context_ref.shape[0]

    def remote(src, dst, send, recv, sp, tp):
        return pltpu.make_async_remote_copy(
            src_ref=src, dst_ref=dst, send_sem=send, recv_sem=recv,
            device_id=(sp, tp), device_id_type=MESH,
        )

    loads = [
        pltpu.make_async_copy(a, b, wsem.at[i])
        for i, (a, b) in enumerate(
            [(wq1_hbm, wq1), (wq2_hbm, wq2), (wk1_hbm, wk1), (wk2_hbm, wk2), (wv_hbm, wv), (wo_hbm, wo)]
        )
    ]
    for load in loads:
        load.start()

    barrier = pltpu.get_barrier_semaphore()

    @pl.loop(1, S)
    def _(i):
        pl.semaphore_signal(barrier, inc=1, device_id=((s + i) % S, t), device_id_type=MESH)

    for i in range(1, T):
        pl.semaphore_signal(barrier, inc=1, device_id=(s, (t + i) % T), device_id_type=MESH)

    for i in range(Lr // GRID_W):
        span, at = slice(i * GRID_W, (i + 1) * GRID_W), pl.ds(s * (Lr // GRID_W) + i, 1)
        cos_ref[span, :] = ccol_ref[...] + crow_ref[at, :]
        sin_ref[span, :] = scol_ref[...] + srow_ref[at, :]
    cos_ref[Lr:, :] = jnp.ones((Cp, LANES), F32)
    sin_ref[Lr:, :] = jnp.zeros((Cp, LANES), F32)

    for i, ref in enumerate((cond_ref, ccond_ref)):
        v = ref[...]
        sig[i : i + 1, :] = v / (1.0 + jnp.exp(-v))
    modp[t] = jnp.dot(sig[...].astype(BF16), modw_ref[...], preferred_element_type=F32)

    pl.semaphore_wait(barrier, S - 1 + T - 1)

    def part_copy(i):
        return remote(modp.at[t], modp.at[t], mp_s.at[i], mp_r.at[t], s, (t + i) % T)

    def latent_copy(i):
        return remote(latent_ref, lat.at[t], lt_s.at[i], lt_r.at[t], s, (t + i) % T)

    for i in range(1, T):
        part_copy(i).start()
    for i in range(1, T):
        latent_copy(i).start()
    lat[t] = latent_ref[...]
    for i in range(1, T):
        o = (t + i) % T
        remote(modp.at[o], modp.at[o], mp_s.at[i], mp_r.at[o], s, o).wait_recv()
    total = modp[0]
    for i in range(1, T):
        total = total + modp[i]
    modall[s] = total

    def mod_copy(i, src):
        return remote(modall.at[src], modall.at[src], ma_s.at[i], ma_r.at[src], (s + i) % S, t)

    @pl.loop(1, S)
    def _(i):
        mod_copy(i, s).start()

    for i in range(1, T):
        o = (t + i) % T
        remote(lat.at[o], lat.at[o], lt_s.at[i], lt_r.at[o], s, o).wait_recv()
    step = math.gcd(rows, 32)
    for i in range(T):

        @pl.loop(0, rows // step)
        def _(j):
            at = pl.multiple_of(j * step, step)
            nrm[pl.ds(i * rows + at, step), :] = normed_rows(lat[i, pl.ds(at, step), :])

    nrm[Lr:, :] = normed_rows(context_ref[...])

    @pl.loop(1, S)
    def _(i):
        mod_copy(i, (s + i) % S).wait_recv()

    for i in range(S):
        modrow[:, i * cw : (i + 1) * cw] = modall[i][:, :cw]

    @pl.loop(0, Lr // step)
    def _(j):
        at = pl.ds(pl.multiple_of(j * step, step), step)
        h[at, :] = (nrm[at, :] * (1.0 + modrow[0:1, D : 2 * D]) + modrow[0:1, :D]).astype(BF16)

    h[Lr:, :] = (nrm[Lr:, :] * (1.0 + modrow[1:2, D : 2 * D]) + modrow[1:2, :D]).astype(BF16)

    for i in range(2):
        loads[i].wait()
    lh = h[:Lr, :]
    one = jnp.dot(lh, wq1[...], preferred_element_type=F32)
    two = jnp.dot(lh, wq2[...], preferred_element_type=F32)
    for i in range(G):
        cut = slice(i * HEAD_DIM, (i + 1) * HEAD_DIM)
        pair = jnp.concatenate([one[:, cut], two[:, cut]], axis=1)
        turned = rotate(pair, cos_ref[:Lr, :], sin_ref[:Lr, :])
        qs[i] = (turned * (LOG2E * HEAD_DIM**-0.5)).astype(BF16)

    def q_out(i):
        to = (g + i) % G
        return remote(qs.at[to], q.at[g], q_s.at[i], q_r.at[g], to * R + r, t)

    for i in range(1, G):
        q_out(i).start()
    q[g] = qs[g]

    for i in range(2, 5):
        loads[i].wait()
    hh = h[...]
    one = jnp.dot(hh, wk1[...], preferred_element_type=F32)
    two = jnp.dot(hh, wk2[...], preferred_element_type=F32)
    for i in range(G):
        cut = slice(i * HEAD_DIM, (i + 1) * HEAD_DIM)
        pair = jnp.concatenate([one[:, cut], two[:, cut]], axis=1)
        kvs[i, :, :LANES] = rotate(pair, cos_ref[...], sin_ref[...]).astype(BF16)
    val = jnp.dot(hh, wv[...], preferred_element_type=F32)
    for i in range(G):
        kvs[i, :, LANES:] = val[:, i * VALUE_DIM : (i + 1) * VALUE_DIM].astype(BF16)

    def kv_out(i):
        to = (g + i) % G
        return remote(kvs.at[to], kv.at[s], kz_s.at[i], kv_r.at[s], to * R + r, t)

    for i in range(1, G):
        kv_out(i).start()
    kv[s] = kvs[g]

    def forward(i, j):
        src = ((g + G - i) % G) * R + r
        return remote(kv.at[src], kv.at[src], kv_s.at[i, j], kv_r.at[src], g * R + (r + j) % R, t)

    def landed(src):
        remote(kv.at[src], kv.at[src], kz_s.at[0], kv_r.at[src], s, t).wait_recv()

    def forward_all(i):
        @pl.loop(1, R)
        def _(j):
            forward(i, j).start()

    forward_all(0)
    mx[...] = jnp.full(mx.shape, NEGATIVE, F32)
    acc[...] = jnp.zeros(acc.shape, F32)
    boost = boost_ref[g] * LOG2E

    for i in range(1, G):
        o = (g + i) % G
        remote(q.at[o], q.at[o], q_s.at[i], q_r.at[o], s, t).wait_recv()

    def attend(n, at):
        k_l = kv[pl.ds(at, B), :Lr, :LANES].reshape(B * Lr, LANES)
        v_l = kv[pl.ds(at, B), :Lr, LANES:].reshape(B * Lr, VALUE_DIM)
        k_c = kv[pl.ds(at, B), Lr:, :LANES].reshape(B * Cp, LANES)
        v_c = kv[pl.ds(at, B), Lr:, LANES:].reshape(B * Cp, VALUE_DIM)
        v_l = jnp.concatenate([v_l, jnp.ones_like(v_l)], axis=1)
        v_c = jnp.concatenate([v_c, jnp.ones_like(v_c)], axis=1)
        nt = (((1,), (1,)), ((), ()))
        QB = min(Lr, QROWS)
        for m, c in [(m, c) for c in range(Lr // QB) for m in range(2)]:
            part = slice(c * QB, (c + 1) * QB)
            qq = q[n, part, :]
            lane = lax.broadcasted_iota(jnp.int32, qq.shape, 1)
            qm = jnp.where(lane // HEAD_DIM == m, qq, jnp.zeros_like(qq))
            s_l = lax.dot_general(qm, k_l, nt, preferred_element_type=F32)
            s_c = lax.dot_general(qm, k_c, nt, preferred_element_type=F32) + boost
            if Cp != Cr:
                spot = lax.broadcasted_iota(jnp.int32, s_c.shape, 1)
                s_c = jnp.where(spot % Cp < Cr, s_c, NEGATIVE)
            old = mx[m, n, part, :]
            peak = jnp.maximum(
                old,
                jnp.maximum(
                    jnp.max(s_l, axis=-1, keepdims=True), jnp.max(s_c, axis=-1, keepdims=True)
                ),
            )
            p_l = jnp.exp2(s_l - peak).astype(BF16)
            p_c = jnp.exp2(s_c - peak).astype(BF16)
            mx[m, n, part, :] = peak
            acc[m, n, part, :] = (
                jnp.exp2(old - peak) * acc[m, n, part, :]
                + jnp.dot(p_l, v_l, preferred_element_type=F32)
                + jnp.dot(p_c, v_c, preferred_element_type=F32)
            )

    lam = lam_ref[g]
    gain = gain_ref[...]

    def finish(n):
        one = acc[0, n, :, :VALUE_DIM] / acc[0, n, :, VALUE_DIM:]
        two = acc[1, n, :, :VALUE_DIM] / acc[1, n, :, VALUE_DIM:]
        mixed = one - lam * two
        mixed = mixed * lax.rsqrt(jnp.mean(mixed * mixed, axis=-1, keepdims=True) + EPSILON) * gain
        return mixed.astype(BF16)

    def ho_out(i):
        to = (g + i) % G
        return remote(ho.at[to], hr.at[g], ho_s.at[i], ho_r.at[g], to * R + r, t)

    def pass_on(i):
        landed(((g + G - i) % G) * R + r)
        forward_all(i)

    for i in range(G):
        if i == 1 and G > 2:
            pass_on(2)
        base = ((g + G - i) % G) * R

        @pl.loop(1, R)
        def _(j):
            landed(base + (r + j) % R)

        if i + 1 < G:
            half = G // 2
            for low, high in ((0, half), (half, G)):
                if low and i == 0:
                    pass_on(1)
                elif low and i + 2 < G:
                    pass_on(i + 2)

                @pl.loop(low * (R // B), high * (R // B))
                def _(x):
                    attend(x // (R // B), base + x % (R // B) * B)

        else:

            @pl.loop(1, G + 1)
            def _(y):
                n = (g + y) % G

                @pl.loop(0, R // B)
                def _(x):
                    attend(n, base + x * B)

                ho[n] = finish(n)

                @pl.when(y < G)
                def _():
                    ho_out(y).start()

    hr[g] = ho[g]
    loads[5].wait()
    for i in range(1, G):
        o = (g + i) % G
        remote(hr.at[o], hr.at[o], ho_s.at[i], ho_r.at[o], s, t).wait_recv()

    def branch_rows(o):
        at = pl.multiple_of(o * rows, rows)
        mine = jnp.concatenate([hr[i, pl.ds(at, rows), :] for i in range(G)], axis=1)
        return jnp.dot(mine, wo[...], preferred_element_type=F32)

    def rs_out(i):
        o = (t + i) % T
        return remote(rsend.at[o], rs.at[t], rs_s.at[i], rs_r.at[t], s, o)

    for i in range(1, T):
        o = (t + i) % T
        rsend[o] = branch_rows(o).astype(BF16)
        rs_out(i).start()
    branch = branch_rows(t)
    for i in range(1, T):
        o = (t + i) % T
        remote(rs.at[o], rs.at[o], rs_s.at[i], rs_r.at[o], s, o).wait_recv()
        branch = branch + rs[o].astype(F32)
    out_ref[...] = (latent_ref[...].astype(F32) + modrow[0:1, 2 * D :] * branch).astype(BF16)

    for i in range(1, T):
        part_copy(i).wait_send()
        latent_copy(i).wait_send()
        rs_out(i).wait_send()

    @pl.loop(1, S)
    def _(i):
        mod_copy(i, s).wait_send()

    for i in range(1, G):
        kv_out(i).wait_send()
        q_out(i).wait_send()
        ho_out(i).wait_send()
    for i in range(G):

        @pl.loop(1, R)
        def _(j):
            forward(i, j).wait_send()


def general_body(
    S, T,
    latent, context, condition, context_condition, modulation_weight,
    query_first, query_second, key_first, key_second, value_weight,
    lambda_head, context_score_boost, head_gain, output_weight,
):
    rows, D = latent.shape
    Lr = rows * T
    G = value_weight.shape[1] // VALUE_DIM
    assert S % G == 0
    R = S // G
    B = math.gcd(R, 4)
    Cr = context.shape[0]
    Cp = -(-Cr // 16) * 16
    if Cp != Cr:
        context = jnp.pad(context, ((0, Cp - Cr), (0, 0)))
    cw = modulation_weight.shape[1]
    cp = -(-cw // LANES) * LANES
    if cp != cw:
        modulation_weight = jnp.pad(modulation_weight, ((0, 0), (0, cp - cw)))
    depth = modulation_weight.shape[0]
    assert Lr % GRID_W == 0
    tables = rotation_tables(S * Lr // GRID_W)
    vm = pl.BlockSpec(memory_space=pltpu.VMEM)
    sm = pl.BlockSpec(memory_space=pltpu.SMEM)
    hb = pl.BlockSpec(memory_space=pl.ANY)
    V = pltpu.VMEM
    dma = pltpu.SemaphoreType.DMA
    weights = (query_first, query_second, key_first, key_second, value_weight, output_weight)
    return pl.pallas_call(
        functools.partial(general_kernel, (S, T, G, R, B, Cr, cw)),
        out_shape=jax.ShapeDtypeStruct((rows, D), BF16),
        in_specs=[vm] * 5 + [hb] * 5 + [sm, sm, vm, hb, vm, vm, vm, vm],
        out_specs=vm,
        scratch_shapes=[V(w.shape, BF16) for w in weights]
        + [
            V((Lr + Cp, LANES), F32),
            V((Lr + Cp, LANES), F32),
            V((2, depth), F32),
            V((T, 2, cp), F32),
            V((S, 2, cp), F32),
            V((2, 3 * D), F32),
            V((T, rows, D), BF16),
            V((Lr + Cp, D), F32),
            V((Lr + Cp, D), BF16),
            V((G, Lr, LANES), BF16),
            V((G, Lr + Cp, LANES + VALUE_DIM), BF16),
            V((G, Lr, LANES), BF16),
            V((S, Lr + Cp, LANES + VALUE_DIM), BF16),
            V((2, G, Lr, 1), F32),
            V((2, G, Lr, 2 * VALUE_DIM), F32),
            V((G, Lr, VALUE_DIM), BF16),
            V((G, Lr, VALUE_DIM), BF16),
            V((T, rows, D), BF16),
            V((T, rows, D), BF16),
            dma((6,)),
            dma((T,)), dma((T,)), dma((T,)), dma((T,)), dma((S,)), dma((S,)),
            dma((G,)), dma((G,)), dma((G,)), dma((G, R)), dma((S,)),
            dma((G,)), dma((G,)), dma((T,)), dma((T,)),
        ],
        compiler_params=pltpu.CompilerParams(
            collective_id=0, has_side_effects=True, vmem_limit_bytes=62 * 1024 * 1024
        ),
    )(
        latent, context, condition[None, :], context_condition[None, :], modulation_weight,
        query_first, query_second, key_first, key_second, value_weight,
        lambda_head, context_score_boost, head_gain[None, :], output_weight, *tables,
    )


def solution(mesh):
    in_specs = (
        P(("sp", "tp"), None),
        P("sp", None),
        P("tp"),
        P("tp"),
        P("tp", "sp"),
        P(None, "tp"),
        P(None, "tp"),
        P(None, "tp"),
        P(None, "tp"),
        P(None, "tp"),
        P("tp"),
        P("tp"),
        P(),
        P("tp", None),
    )
    out_specs = P(("sp", "tp"), None)
    S, T = mesh.shape["sp"], mesh.shape["tp"]
    run = functools.partial(body if T == 2 else general_body, S, T)
    return jax.shard_map(run, mesh=mesh, in_specs=in_specs, out_specs=out_specs, check_vma=False)
```

```python
import functools
import math

import jax
import jax.numpy as jnp
import numpy as np
from jax import lax
from jax.experimental import pallas as pl
from jax.experimental.pallas import tpu as pltpu
from jax.sharding import PartitionSpec as P

HEAD_DIM = 64
VALUE_DIM = 128
GRID_W = 64
EPSILON = 1e-06
THETA = 10000.0
NEGATIVE = -1e30
LOG2E = math.log2(math.e)
MESH = pl.DeviceIdType.MESH
BF16 = jnp.bfloat16
F32 = jnp.float32
LANES = 128
QROWS = 256


def rotation_tables(grid_rows):
    half = HEAD_DIM // 2
    quarter = half // 2
    lane = np.arange(LANES) % HEAD_DIM
    rate = (THETA ** (-(lane % quarter) / quarter)).astype(np.float32)
    sign = np.where(lane % half < quarter, -1.0, 1.0)
    tables = []
    for count, mask in ((grid_rows, lane < half), (GRID_W, lane >= half)):
        angle = np.arange(count, dtype=np.float32)[:, None] * rate[None, :]
        for table in (np.cos(angle), np.sin(angle) * sign):
            tables.append(np.where(mask, table, 0.0).astype(np.float32))
    return tables


def rotate(x, cosine, sine):
    quarter = HEAD_DIM // 4
    lane = lax.broadcasted_iota(jnp.int32, x.shape, 1)
    ahead = pltpu.roll(x, LANES - quarter, 1)
    behind = pltpu.roll(x, quarter, 1)
    flipped = jnp.where(lane % (2 * quarter) < quarter, ahead, behind)
    return x * cosine + flipped * sine


def normed_rows(rows):
    v = rows.astype(F32)
    return v * lax.rsqrt(jnp.mean(v * v, axis=-1, keepdims=True) + EPSILON)


def flip(v, k, span):
    out = 0
    bit = 1
    while bit < span:
        out = out + bit * ((v // bit + k // bit) % 2)
        bit *= 2
    return out


def groups(P, raw_rows, far_rows):
    return math.gcd(P, max(1, 400 // raw_rows)), math.gcd(P, max(1, 512 // far_rows))


def kernel(
    dims,
    lat_hbm, ctx_hbm, cond_hbm, ccond_hbm, modw_hbm,
    wq1_hbm, wq2_hbm, wk1_hbm, wk2_hbm, wv_hbm,
    lam_ref, boost_ref, gain_ref, wo_hbm, crow_ref, srow_ref, ccol_ref, scol_ref,
    out_ref,
    wq1, wq2, wk1, wk2, wv, wo,
    ctx, cond, modw, tab, cos_ref, sin_ref, mt, mp, modrow, lat, raw, nrm, h, hraw,
    qs, kvs, kvrs, q, qb, kvn, kvr, kvf, s0, s1, vt0, pk0, mx, acc, ho, hr, lb,
    wsem, isem, mt_s, mt_r, mp_s, mp_r, lt_s, lt_r, lb_s, lb_r, wo_s, wo_r,
    rw_s, rw_r, rf_s, rf_r, q_s, q_r, kn_s, kn_r, kf_s, kf_r, kr_s, kr_r, fn_s, ff_s, fr_s, ho_s, ho_r,
):
    S, T, G, R, Cr, cw = dims
    P = T * G
    s, t = lax.axis_index("sp"), lax.axis_index("tp")
    g, p0 = s // P, s % P
    prim, hown = p0 // G, p0 % G
    mine = t == prim
    other = jnp.logical_not(mine)
    _, rows, D = lat.shape
    Lr = rows * T
    Cp = ctx.shape[0]
    keys = Lr + Cp
    Q = R - 1
    chunks, rc = raw.shape[2], raw.shape[3]
    rw = chunks * rc
    Rr = T * rw
    N = 2 * P * rows
    quad, wide = groups(P, Q * Rr, keys - Rr)

    def remote(src, dst, send, recv, sp, tp):
        return pltpu.make_async_remote_copy(
            src_ref=src, dst_ref=dst, send_sem=send, recv_sem=recv,
            device_id=(sp, tp), device_id_type=MESH,
        )

    def arrived(buf, recv):
        remote(buf, buf, lt_s.at[0], recv, s, t).wait_recv()

    barrier = pltpu.get_barrier_semaphore()

    @pl.loop(1, S)
    def _(i):
        pl.semaphore_signal(barrier, inc=1, device_id=((s + i) % S, t), device_id_type=MESH)

    for i in range(1, T):
        pl.semaphore_signal(barrier, inc=1, device_id=(s, (t + i) % T), device_id_type=MESH)

    inputs = [
        pltpu.make_async_copy(a, b, isem.at[i])
        for i, (a, b) in enumerate(
            [(cond_hbm, cond.at[0:1]), (ccond_hbm, cond.at[1:2]), (modw_hbm, modw),
             (lat_hbm, lat.at[t]), (ctx_hbm, ctx)]
        )
    ]
    for load in inputs:
        load.start()
    loads = [
        pltpu.make_async_copy(a, b, wsem.at[i])
        for i, (a, b) in enumerate(
            [(wk1_hbm, wk1), (wk2_hbm, wk2), (wv_hbm, wv), (wq1_hbm, wq1), (wq2_hbm, wq2), (wo_hbm, wo.at[t])]
        )
    ]
    for load in loads:
        load.start()

    for i in range(G):
        lb[t, i : i + 1, :] = jnp.full((1, LANES), lam_ref[i], F32)
        lb[t, G + i : G + i + 1, :] = jnp.full((1, LANES), boost_ref[i] * LOG2E, F32)

    for i in range(3):
        inputs[i].wait()
    v = cond[...]
    sig = v / (1.0 + jnp.exp(-v))
    mt[t] = jnp.dot(sig.astype(BF16), modw[...], preferred_element_type=F32)
    for i in range(3, 5):
        inputs[i].wait()

    pl.semaphore_wait(barrier, S - 1 + T - 1)

    def mt_copy(i):
        return remote(mt.at[t], mt.at[t], mt_s.at[i], mt_r.at[t], s, (t + i) % T)

    def mp_copy(i):
        return remote(mp.at[s], mp.at[s], mp_s.at[i], mp_r.at[s], (s + i) % S, t)

    def lat_copy(i):
        return remote(lat.at[t], lat.at[t], lt_s.at[i], lt_r.at[t], s, (t + i) % T)

    def lb_copy(i):
        return remote(lb.at[t], lb.at[t], lb_s.at[i], lb_r.at[t], s, (t + i) % T)

    def wo_copy(i):
        return remote(wo.at[t], wo.at[t], wo_s.at[i], wo_r.at[t], s, (t + i) % T)

    def raw_copy(j, c):
        return remote(
            lat.at[t, pl.ds(c * rc, rc)], raw.at[j - 1, t, c], rw_s.at[j - 1, c],
            rw_r.at[j - 1, c], (g + R - j) % R * P + p0, t,
        )

    def raw_pass(j, c, i):
        part = raw.at[j - 1, t, c]
        return remote(
            part, part, rf_s.at[j - 1, c, i], rf_r.at[j - 1, c, t], s, (t + i) % T
        )

    for i in range(1, T):
        mt_copy(i).start()
    for j in range(1, R):
        raw_copy(j, 0).start()
    for i in range(1, T):
        o = (t + i) % T
        arrived(mt.at[o], mt_r.at[o])
    total = mt[0]
    for i in range(1, T):
        total = total + mt[i]
    mp[s] = total

    @pl.loop(1, S)
    def _(i):
        mp_copy(i).start()

    for i in range(1, T):
        lat_copy(i).start()
        lb_copy(i).start()
    for c in range(1, chunks):
        for j in range(1, R):
            raw_copy(j, c).start()
    loads[5].wait()
    for i in range(1, T):
        wo_copy(i).start()

    def table(src, out, order):
        for n, (col, row) in enumerate(((ccol_ref, crow_ref), (scol_ref, srow_ref))):
            for i in range(Lr // GRID_W):
                at = pl.ds(src * (Lr // GRID_W) + i, 1)
                tab[n, i * GRID_W : (i + 1) * GRID_W, :] = col[...] + row[at, :]
            at = out
            for low, high in order:
                ref = sin_ref if n else cos_ref
                ref[at : at + high - low, :] = tab[n, low:high, :]
                at += high - low

    head = [(i * rows, i * rows + rw) for i in range(T)]
    rest = [(i * rows + rw, (i + 1) * rows) for i in range(T)]
    table(s, 0, head + rest)
    cos_ref[Lr : Lr + Cp, :] = jnp.ones((Cp, LANES), F32)
    sin_ref[Lr : Lr + Cp, :] = jnp.zeros((Cp, LANES), F32)
    for j in range(1, R):
        table((g + j) % R * P + p0, Lr + Cp + (j - 1) * Rr, head)

    step = math.gcd(rw, rows - rw, 32)

    def norm_lat(i):
        for low, size, at in ((0, rw, i * rw), (rw, rows - rw, Rr + i * (rows - rw))):

            @pl.loop(0, size // step)
            def _(j):
                off = pl.multiple_of(j * step, step)
                to = pl.ds(pl.multiple_of(at + off, step), step)
                nrm[to, :] = normed_rows(lat[i, pl.ds(low + off, step), :])

    nrm[Lr:, :] = normed_rows(ctx[...])
    norm_lat(t)
    for i in range(1, T):
        o = (t + i) % T
        arrived(lat.at[o], lt_r.at[o])
        norm_lat(o)

    @pl.loop(1, S)
    def _(i):
        o = (s + i) % S
        arrived(mp.at[o], mp_r.at[o])

    for i in range(S):
        modrow[:, i * cw : (i + 1) * cw] = mp[i][:, :cw]

    @pl.loop(0, Lr // step)
    def _(j):
        at = pl.ds(pl.multiple_of(j * step, step), step)
        h[at, :] = (nrm[at, :] * (1.0 + modrow[0:1, D : 2 * D]) + modrow[0:1, :D]).astype(BF16)

    h[Lr:, :] = (nrm[Lr:, :] * (1.0 + modrow[1:2, D : 2 * D]) + modrow[1:2, :D]).astype(BF16)

    def project(hh, at, out):
        n = hh.shape[0]
        one = jnp.dot(hh, wk1[...], preferred_element_type=F32)
        two = jnp.dot(hh, wk2[...], preferred_element_type=F32)
        for i in range(G):
            cut = slice(i * HEAD_DIM, (i + 1) * HEAD_DIM)
            pair = jnp.concatenate([one[:, cut], two[:, cut]], axis=1)
            turned = rotate(pair, cos_ref[at : at + n, :], sin_ref[at : at + n, :])
            out[i, :, :LANES] = turned.astype(BF16)
        val = jnp.dot(hh, wv[...], preferred_element_type=F32)
        for i in range(G):
            out[i, :, LANES:] = val[:, i * VALUE_DIM : (i + 1) * VALUE_DIM].astype(BF16)

    for i in range(3, 5):
        loads[i].wait()
    lh = h[:Lr, :]
    one = jnp.dot(lh, wq1[...], preferred_element_type=F32)
    two = jnp.dot(lh, wq2[...], preferred_element_type=F32)
    for i in range(G):
        cut = slice(i * HEAD_DIM, (i + 1) * HEAD_DIM)
        pair = jnp.concatenate([one[:, cut], two[:, cut]], axis=1)
        turned = rotate(pair, cos_ref[:Lr, :], sin_ref[:Lr, :])
        turned = (turned * (LOG2E * HEAD_DIM**-0.5)).astype(BF16)
        at = 0
        for low, high in head + rest:
            qs[i, low:high, :] = turned[at : at + high - low]
            at += high - low

    def q_out(i, j):
        hl = flip(hown, i, G)
        to = (t + j) % T
        part = pl.ds(pl.multiple_of(to * rows, rows), rows)
        return remote(qs.at[hl, part], q.at[p0], q_s.at[i, j], q_r.at[p0], g * P + t * G + hl, to)

    @pl.when(mine)
    def _():
        q[p0] = qs[hown, pl.ds(pl.multiple_of(t * rows, rows), rows), :]

    @pl.when(other)
    def _():
        q_out(0, 0).start()

    for j in range(1, T):
        q_out(0, j).start()
    for i in range(1, G):
        for j in range(T):
            q_out(i, j).start()
    for i in range(3):
        loads[i].wait()
    project(h[...], 0, kvs)

    def near_out(i):
        hl = flip(hown, i, G)
        return remote(kvs.at[hl], kvn.at[p0], kn_s.at[i], kn_r.at[p0], g * P + t * G + hl, t)

    def far_out(i, j):
        hl = flip(hown, i, G)
        to = (g + R - j) % R
        slot = (j - 1) * P + p0
        return remote(
            kvs.at[hl, pl.ds(Rr, Lr + Cp - Rr)], kvf.at[slot], kf_s.at[i, j - 1], kf_r.at[slot],
            to * P + t * G + hl, t,
        )

    def raw_out(i):
        hl = flip(hown, i, G)
        return remote(kvrs.at[hl], kvr.at[p0], kr_s.at[i], kr_r.at[p0], g * P + t * G + hl, t)

    @pl.when(mine)
    def _():
        kvn[p0] = kvs[hown]

    @pl.when(other)
    def _():
        near_out(0).start()

    for i in range(1, G):
        near_out(i).start()
    for i in range(G):
        for j in range(1, R):
            far_out(i, j).start()


    for c in range(chunks):
        for j in range(1, R):
            arrived(raw.at[j - 1, t, c], rw_r.at[j - 1, c])
            for i in range(1, T):
                raw_pass(j, c, i).start()

    def lift(j, o, c):
        part = normed_rows(raw[j - 1, o, c])
        part = part * (1.0 + modrow[0:1, D : 2 * D]) + modrow[0:1, :D]
        at = pl.multiple_of((j - 1) * Rr + o * rw + c * rc, rc)
        hraw[pl.ds(at, rc), :] = part.astype(BF16)

    for j in range(1, R):
        for c in range(chunks):
            lift(j, t, c)
    for i in range(1, T):
        o = (t + i) % T
        for c in range(chunks):
            for j in range(1, R):
                arrived(raw.at[j - 1, o, c], rf_r.at[j - 1, c, o])
                lift(j, o, c)
    project(hraw[...], Lr + Cp, kvrs)

    @pl.when(mine)
    def _():
        kvr[p0] = kvrs[hown]

    @pl.when(other)
    def _():
        raw_out(0).start()

    for i in range(1, G):
        raw_out(i).start()

    mx[...] = jnp.full(mx.shape, NEGATIVE, F32)
    acc[...] = jnp.zeros(acc.shape, F32)
    vt0[VALUE_DIM:, :] = jnp.ones((vt0.shape[0] - VALUE_DIM, vt0.shape[1]), BF16)
    for i in range(1, T):
        o = (t + i) % T
        arrived(lb.at[o], lb_r.at[o])
    lam = lb[prim, pl.ds(hown, 1), :][:, :rows]
    boost = lb[prim, pl.ds(G + hown, 1), :][:, :1]
    gain = jnp.broadcast_to(gain_ref[...], (VALUE_DIM, LANES)).T[:, :rows]
    nt = (((1,), (1,)), ((), ()))

    def to_core(buf, slot, send, recv, i):
        return remote(
            buf.at[slot], buf.at[slot], send.at[slot, i], recv.at[slot], s, (t + i) % T
        )

    def spread(buf, slots, send, recv, own):
        @pl.when(mine)
        def _():
            for slot in slots:
                if own:

                    @pl.when(slot != p0)
                    def _():
                        arrived(buf.at[slot], recv.at[slot])

                else:
                    arrived(buf.at[slot], recv.at[slot])
                for i in range(1, T):
                    to_core(buf, slot, send, recv, i).start()

    def settle(buf, slots, recv):
        @pl.when(other)
        def _():
            for slot in slots:
                arrived(buf.at[slot], recv.at[slot])

    half = N // 2
    banks = (s0, s1)

    def scores(buf, base, count, low, c):
        cols = slice(c * half, (c + 1) * half)
        at = pl.ds(base, count)
        n = count * low
        m = count * (buf.shape[1] - low)
        s_ref, vt = banks[c], vt0
        keys = buf[at, :low, :LANES].reshape(n, LANES)
        vals = buf[at, :low, LANES:].reshape(n, VALUE_DIM)
        if m:
            keys = jnp.concatenate([keys, buf[at, low:, :LANES].reshape(m, LANES)], axis=0)
            vals = jnp.concatenate([vals, buf[at, low:, LANES:].reshape(m, VALUE_DIM)], axis=0)
        if c == 0:
            vt[:VALUE_DIM, : n + m] = vals.astype(F32).T.astype(BF16)
        sc = lax.dot_general(keys, qb[cols, :], nt, preferred_element_type=F32)
        s_ref[:n, :] = sc[:n]
        peak = jnp.max(sc[:n], axis=0, keepdims=True)
        if m:
            lifted = sc[n:] + boost
            if Cp != Cr:
                spot = lax.broadcasted_iota(jnp.int32, lifted.shape, 0)
                lifted = jnp.where(spot % Cp < Cr, lifted, NEGATIVE)
            s_ref[n : n + m, :] = lifted
            peak = jnp.maximum(peak, jnp.max(lifted, axis=0, keepdims=True))
        pk0[:, cols] = peak

    def weigh(n, c):
        cols = slice(c * half, (c + 1) * half)
        old = mx[:, cols]
        peak = jnp.maximum(old, pk0[:, cols])
        pr = jnp.exp2(banks[c][:n, :] - peak).astype(BF16)
        mx[:, cols] = peak
        acc[:, cols] = jnp.exp2(old - peak) * acc[:, cols] + jnp.dot(
            vt0[:, :n], pr, preferred_element_type=F32
        )

    def finish(j):
        u = acc[:VALUE_DIM, j * 2 * rows : (j + 1) * 2 * rows]
        u = u / acc[VALUE_DIM : VALUE_DIM + 1, j * 2 * rows : (j + 1) * 2 * rows]
        mixed = u[:, :rows] - lam * u[:, rows:]
        mixed = mixed * lax.rsqrt(jnp.mean(mixed * mixed, axis=0, keepdims=True) + EPSILON)
        ho[j] = (mixed * gain).T.astype(BF16)

    def ho_out(j):
        return remote(ho.at[j], hr.at[p0], ho_s.at[j], ho_r.at[p0], g * P + j, t)

    for j in range(P):

        @pl.when(jnp.logical_or(other, p0 != j))
        def _():
            arrived(q.at[j], q_r.at[j])

        qq = q[j]
        lane = lax.broadcasted_iota(jnp.int32, qq.shape, 1)
        zero = jnp.zeros_like(qq)
        qb[j * 2 * rows : j * 2 * rows + rows, :] = jnp.where(lane < HEAD_DIM, qq, zero)
        qb[j * 2 * rows + rows : (j + 1) * 2 * rows, :] = jnp.where(lane < HEAD_DIM, zero, qq)

    units = []
    for k in [*range(0, P // 2, 2), *range(1, P // 2, 2)]:
        units.append((kvn, flip(p0 // 2, k, P // 2) * 2, 2, Lr, fn_s, kn_r, True))
    for j in range(Q):
        for k in range(P // wide):
            base = j * P + flip(p0 // wide, k, P // wide) * wide
            units.append((kvf, base, wide, Lr - Rr, ff_s, kf_r, False))
    for k in range(P // quad):
        units.append((kvr, flip(p0 // quad, k, P // quad) * quad, quad, Q * Rr, fr_s, kr_r, True))
    def deliver(c):
        for j in range(c * P // 2, (c + 1) * P // 2):
            finish(j)

            @pl.when(p0 == j)
            def _():
                hr[j] = ho[j]

            @pl.when(p0 != j)
            def _():
                ho_out(j).start()

    for n, (buf, base, count, low, send, recv, own) in enumerate(units):
        spread(buf, [base + i for i in range(count)], send, recv, own)
        settle(buf, [base + i for i in range(count)], recv)
        size = count * buf.shape[1]
        scores(buf, base, count, low, 0)
        scores(buf, base, count, low, 1)
        weigh(size, 0)
        if n == len(units) - 1:
            deliver(0)
        weigh(size, 1)
    deliver(1)

    for i in range(1, T):
        o = (t + i) % T
        arrived(wo.at[o], wo_r.at[o])
    for i in range(1, P):
        o = flip(p0, i, P)
        arrived(hr.at[o], ho_r.at[o])

    branch = None
    for i in range(T):
        part = jnp.concatenate([hr[i * G + j] for j in range(G)], axis=1)
        term = jnp.dot(part, wo[i], preferred_element_type=F32)
        branch = term if branch is None else branch + term
    out_ref[...] = (lat[t].astype(F32) + modrow[0:1, 2 * D :] * branch).astype(BF16)

    for i in range(1, T):
        mt_copy(i).wait_send()

    @pl.loop(1, S)
    def _(i):
        mp_copy(i).wait_send()

    for i in range(1, T):
        lat_copy(i).wait_send()
        lb_copy(i).wait_send()
        wo_copy(i).wait_send()
    for j in range(1, R):
        for c in range(chunks):
            raw_copy(j, c).wait_send()
            for i in range(1, T):
                raw_pass(j, c, i).wait_send()

    @pl.when(other)
    def _():
        near_out(0).wait_send()
        raw_out(0).wait_send()
        q_out(0, 0).wait_send()

    for i in range(1, G):
        near_out(i).wait_send()
        raw_out(i).wait_send()
    for i in range(G):
        for j in range(1, R):
            far_out(i, j).wait_send()
        for j in range(T):
            if i + j > 0:
                q_out(i, j).wait_send()
    for i in range(1, P):
        ho_out(flip(p0, i, P)).wait_send()

    @pl.when(mine)
    def _():
        for buf, send, recv in ((kvn, fn_s, kn_r), (kvr, fr_s, kr_r), (kvf, ff_s, kf_r)):

            @pl.loop(0, buf.shape[0])
            def _(slot):
                for i in range(1, T):
                    to_core(buf, slot, send, recv, i).wait_send()


def body(
    S, T,
    latent, context, condition, context_condition, modulation_weight,
    query_first, query_second, key_first, key_second, value_weight,
    lambda_head, context_score_boost, head_gain, output_weight,
):
    rows, D = latent.shape
    Lr = rows * T
    G = value_weight.shape[1] // VALUE_DIM
    P = T * G
    assert S % P == 0 and P & (P - 1) == 0 and rows <= LANES
    R = S // P
    assert R > 1 and P > 1
    rc = 16
    chunks = rows * 3 // 8 // rc
    Rr = T * chunks * rc
    Cr = context.shape[0]
    Cp = -(-Cr // 16) * 16
    if Cp != Cr:
        context = jnp.pad(context, ((0, Cp - Cr), (0, 0)))
    cw = modulation_weight.shape[1]
    cp = -(-cw // LANES) * LANES
    if cp != cw:
        modulation_weight = jnp.pad(modulation_weight, ((0, 0), (0, cp - cw)))
    depth = modulation_weight.shape[0]
    assert Lr % GRID_W == 0
    tables = rotation_tables(S * Lr // GRID_W)
    vm = pl.BlockSpec(memory_space=pltpu.VMEM)
    sm = pl.BlockSpec(memory_space=pltpu.SMEM)
    hb = pl.BlockSpec(memory_space=pltpu.HBM)
    V = pltpu.VMEM
    dma = pltpu.SemaphoreType.DMA
    keys = Lr + Cp
    Q = R - 1
    N = 2 * P * rows
    pairw = LANES + VALUE_DIM
    quad, wide = groups(P, Q * Rr, keys - Rr)
    most = max(2 * keys, quad * Q * Rr, wide * (keys - Rr))
    weights = (query_first, query_second, key_first, key_second, value_weight)
    latent, context, modulation_weight, output_weight, *weights = (
        pltpu.with_memory_space_constraint(a, pltpu.HBM)
        for a in (latent, context, modulation_weight, output_weight, *weights)
    )
    query_first, query_second, key_first, key_second, value_weight = weights
    return pl.pallas_call(
        functools.partial(kernel, (S, T, G, R, Cr, cw)),
        out_shape=pltpu.VMEM((rows, D), BF16),
        in_specs=[hb] * 10 + [sm, sm, vm, hb, vm, vm, vm, vm],
        out_specs=vm,
        scratch_shapes=[V(w.shape, BF16) for w in weights]
        + [
            V((T,) + output_weight.shape, BF16),
            V((Cp, D), BF16),
            V((2, depth), F32),
            V((depth, cp), BF16),
            V((2, Lr, LANES), F32),
            V((keys + Q * Rr, LANES), F32),
            V((keys + Q * Rr, LANES), F32),
            V((T, 2, cp), F32),
            V((S, 2, cp), F32),
            V((2, 3 * D), F32),
            V((T, rows, D), BF16),
            V((Q, T, chunks, rc, D), BF16),
            V((keys, D), F32),
            V((keys, D), BF16),
            V((Q * Rr, D), BF16),
            V((G, Lr, LANES), BF16),
            V((G, keys, pairw), BF16),
            V((G, Q * Rr, pairw), BF16),
            V((P, rows, LANES), BF16),
            V((N, LANES), BF16),
            V((P, keys, pairw), BF16),
            V((P, Q * Rr, pairw), BF16),
            V((Q * P, keys - Rr, pairw), BF16),
            V((most, N // 2), F32),
            V((most, N // 2), F32),
            V((VALUE_DIM + 16, most), BF16),
            V((1, N), F32),
            V((1, N), F32),
            V((VALUE_DIM + 16, N), F32),
            V((P, rows, VALUE_DIM), BF16),
            V((P, rows, VALUE_DIM), BF16),
            V((T, 2 * G, LANES), F32),
            dma((6,)), dma((5,)),
            dma((T,)), dma((T,)), dma((S,)), dma((S,)),
            dma((T,)), dma((T,)), dma((T,)), dma((T,)), dma((T,)), dma((T,)),
            dma((Q, chunks)), dma((Q, chunks)), dma((Q, chunks, T)), dma((Q, chunks, T)),
            dma((G, T)), dma((P,)),
            dma((G,)), dma((P,)), dma((G, Q)), dma((Q * P,)), dma((G,)), dma((P,)),
            dma((P, T)), dma((Q * P, T)), dma((P, T)),
            dma((P,)), dma((P,)),
        ],
        compiler_params=pltpu.CompilerParams(
            collective_id=0, has_side_effects=True, vmem_limit_bytes=56 * 1024 * 1024
        ),
    )(
        latent, context, condition[None, :], context_condition[None, :], modulation_weight,
        query_first, query_second, key_first, key_second, value_weight,
        lambda_head, context_score_boost, head_gain[None, :], output_weight, *tables,
    )


def general_kernel(
    dims,
    latent_ref, context_ref, cond_ref, ccond_ref, modw_ref,
    wq1_hbm, wq2_hbm, wk1_hbm, wk2_hbm, wv_hbm,
    lam_ref, boost_ref, gain_ref, wo_hbm, crow_ref, srow_ref, ccol_ref, scol_ref,
    out_ref,
    wq1, wq2, wk1, wk2, wv, wo,
    cos_ref, sin_ref, sig, modp, modall, modrow, lat, nrm, h,
    qs, kvs, q, kv, mx, acc, ho, hr, rsend, rs,
    wsem, mp_s, mp_r, lt_s, lt_r, ma_s, ma_r,
    q_s, q_r, kz_s, kv_s, kv_r, ho_s, ho_r, rs_s, rs_r,
):
    S, T, G, R, B, Cr, cw = dims
    s, t = lax.axis_index("sp"), lax.axis_index("tp")
    g, r = s // R, s % R
    rows, D = latent_ref.shape
    Lr = rows * T
    Cp = context_ref.shape[0]

    def remote(src, dst, send, recv, sp, tp):
        return pltpu.make_async_remote_copy(
            src_ref=src, dst_ref=dst, send_sem=send, recv_sem=recv,
            device_id=(sp, tp), device_id_type=MESH,
        )

    loads = [
        pltpu.make_async_copy(a, b, wsem.at[i])
        for i, (a, b) in enumerate(
            [(wq1_hbm, wq1), (wq2_hbm, wq2), (wk1_hbm, wk1), (wk2_hbm, wk2), (wv_hbm, wv), (wo_hbm, wo)]
        )
    ]
    for load in loads:
        load.start()

    barrier = pltpu.get_barrier_semaphore()

    @pl.loop(1, S)
    def _(i):
        pl.semaphore_signal(barrier, inc=1, device_id=((s + i) % S, t), device_id_type=MESH)

    for i in range(1, T):
        pl.semaphore_signal(barrier, inc=1, device_id=(s, (t + i) % T), device_id_type=MESH)

    for i in range(Lr // GRID_W):
        span, at = slice(i * GRID_W, (i + 1) * GRID_W), pl.ds(s * (Lr // GRID_W) + i, 1)
        cos_ref[span, :] = ccol_ref[...] + crow_ref[at, :]
        sin_ref[span, :] = scol_ref[...] + srow_ref[at, :]
    cos_ref[Lr:, :] = jnp.ones((Cp, LANES), F32)
    sin_ref[Lr:, :] = jnp.zeros((Cp, LANES), F32)

    for i, ref in enumerate((cond_ref, ccond_ref)):
        v = ref[...]
        sig[i : i + 1, :] = v / (1.0 + jnp.exp(-v))
    modp[t] = jnp.dot(sig[...].astype(BF16), modw_ref[...], preferred_element_type=F32)

    pl.semaphore_wait(barrier, S - 1 + T - 1)

    def part_copy(i):
        return remote(modp.at[t], modp.at[t], mp_s.at[i], mp_r.at[t], s, (t + i) % T)

    def latent_copy(i):
        return remote(latent_ref, lat.at[t], lt_s.at[i], lt_r.at[t], s, (t + i) % T)

    for i in range(1, T):
        part_copy(i).start()
    for i in range(1, T):
        latent_copy(i).start()
    lat[t] = latent_ref[...]
    for i in range(1, T):
        o = (t + i) % T
        remote(modp.at[o], modp.at[o], mp_s.at[i], mp_r.at[o], s, o).wait_recv()
    total = modp[0]
    for i in range(1, T):
        total = total + modp[i]
    modall[s] = total

    def mod_copy(i, src):
        return remote(modall.at[src], modall.at[src], ma_s.at[i], ma_r.at[src], (s + i) % S, t)

    @pl.loop(1, S)
    def _(i):
        mod_copy(i, s).start()

    for i in range(1, T):
        o = (t + i) % T
        remote(lat.at[o], lat.at[o], lt_s.at[i], lt_r.at[o], s, o).wait_recv()
    step = math.gcd(rows, 32)
    for i in range(T):

        @pl.loop(0, rows // step)
        def _(j):
            at = pl.multiple_of(j * step, step)
            nrm[pl.ds(i * rows + at, step), :] = normed_rows(lat[i, pl.ds(at, step), :])

    nrm[Lr:, :] = normed_rows(context_ref[...])

    @pl.loop(1, S)
    def _(i):
        mod_copy(i, (s + i) % S).wait_recv()

    for i in range(S):
        modrow[:, i * cw : (i + 1) * cw] = modall[i][:, :cw]

    @pl.loop(0, Lr // step)
    def _(j):
        at = pl.ds(pl.multiple_of(j * step, step), step)
        h[at, :] = (nrm[at, :] * (1.0 + modrow[0:1, D : 2 * D]) + modrow[0:1, :D]).astype(BF16)

    h[Lr:, :] = (nrm[Lr:, :] * (1.0 + modrow[1:2, D : 2 * D]) + modrow[1:2, :D]).astype(BF16)

    for i in range(2):
        loads[i].wait()
    lh = h[:Lr, :]
    one = jnp.dot(lh, wq1[...], preferred_element_type=F32)
    two = jnp.dot(lh, wq2[...], preferred_element_type=F32)
    for i in range(G):
        cut = slice(i * HEAD_DIM, (i + 1) * HEAD_DIM)
        pair = jnp.concatenate([one[:, cut], two[:, cut]], axis=1)
        turned = rotate(pair, cos_ref[:Lr, :], sin_ref[:Lr, :])
        qs[i] = (turned * (LOG2E * HEAD_DIM**-0.5)).astype(BF16)

    def q_out(i):
        to = (g + i) % G
        return remote(qs.at[to], q.at[g], q_s.at[i], q_r.at[g], to * R + r, t)

    for i in range(1, G):
        q_out(i).start()
    q[g] = qs[g]

    for i in range(2, 5):
        loads[i].wait()
    hh = h[...]
    one = jnp.dot(hh, wk1[...], preferred_element_type=F32)
    two = jnp.dot(hh, wk2[...], preferred_element_type=F32)
    for i in range(G):
        cut = slice(i * HEAD_DIM, (i + 1) * HEAD_DIM)
        pair = jnp.concatenate([one[:, cut], two[:, cut]], axis=1)
        kvs[i, :, :LANES] = rotate(pair, cos_ref[...], sin_ref[...]).astype(BF16)
    val = jnp.dot(hh, wv[...], preferred_element_type=F32)
    for i in range(G):
        kvs[i, :, LANES:] = val[:, i * VALUE_DIM : (i + 1) * VALUE_DIM].astype(BF16)

    def kv_out(i):
        to = (g + i) % G
        return remote(kvs.at[to], kv.at[s], kz_s.at[i], kv_r.at[s], to * R + r, t)

    for i in range(1, G):
        kv_out(i).start()
    kv[s] = kvs[g]

    def forward(i, j):
        src = ((g + G - i) % G) * R + r
        return remote(kv.at[src], kv.at[src], kv_s.at[i, j], kv_r.at[src], g * R + (r + j) % R, t)

    def landed(src):
        remote(kv.at[src], kv.at[src], kz_s.at[0], kv_r.at[src], s, t).wait_recv()

    def forward_all(i):
        @pl.loop(1, R)
        def _(j):
            forward(i, j).start()

    forward_all(0)
    mx[...] = jnp.full(mx.shape, NEGATIVE, F32)
    acc[...] = jnp.zeros(acc.shape, F32)
    boost = boost_ref[g] * LOG2E

    for i in range(1, G):
        o = (g + i) % G
        remote(q.at[o], q.at[o], q_s.at[i], q_r.at[o], s, t).wait_recv()

    def attend(n, at):
        k_l = kv[pl.ds(at, B), :Lr, :LANES].reshape(B * Lr, LANES)
        v_l = kv[pl.ds(at, B), :Lr, LANES:].reshape(B * Lr, VALUE_DIM)
        k_c = kv[pl.ds(at, B), Lr:, :LANES].reshape(B * Cp, LANES)
        v_c = kv[pl.ds(at, B), Lr:, LANES:].reshape(B * Cp, VALUE_DIM)
        v_l = jnp.concatenate([v_l, jnp.ones_like(v_l)], axis=1)
        v_c = jnp.concatenate([v_c, jnp.ones_like(v_c)], axis=1)
        nt = (((1,), (1,)), ((), ()))
        QB = min(Lr, QROWS)
        for m, c in [(m, c) for c in range(Lr // QB) for m in range(2)]:
            part = slice(c * QB, (c + 1) * QB)
            qq = q[n, part, :]
            lane = lax.broadcasted_iota(jnp.int32, qq.shape, 1)
            qm = jnp.where(lane // HEAD_DIM == m, qq, jnp.zeros_like(qq))
            s_l = lax.dot_general(qm, k_l, nt, preferred_element_type=F32)
            s_c = lax.dot_general(qm, k_c, nt, preferred_element_type=F32) + boost
            if Cp != Cr:
                spot = lax.broadcasted_iota(jnp.int32, s_c.shape, 1)
                s_c = jnp.where(spot % Cp < Cr, s_c, NEGATIVE)
            old = mx[m, n, part, :]
            peak = jnp.maximum(
                old,
                jnp.maximum(
                    jnp.max(s_l, axis=-1, keepdims=True), jnp.max(s_c, axis=-1, keepdims=True)
                ),
            )
            p_l = jnp.exp2(s_l - peak).astype(BF16)
            p_c = jnp.exp2(s_c - peak).astype(BF16)
            mx[m, n, part, :] = peak
            acc[m, n, part, :] = (
                jnp.exp2(old - peak) * acc[m, n, part, :]
                + jnp.dot(p_l, v_l, preferred_element_type=F32)
                + jnp.dot(p_c, v_c, preferred_element_type=F32)
            )

    lam = lam_ref[g]
    gain = gain_ref[...]

    def finish(n):
        one = acc[0, n, :, :VALUE_DIM] / acc[0, n, :, VALUE_DIM:]
        two = acc[1, n, :, :VALUE_DIM] / acc[1, n, :, VALUE_DIM:]
        mixed = one - lam * two
        mixed = mixed * lax.rsqrt(jnp.mean(mixed * mixed, axis=-1, keepdims=True) + EPSILON) * gain
        return mixed.astype(BF16)

    def ho_out(i):
        to = (g + i) % G
        return remote(ho.at[to], hr.at[g], ho_s.at[i], ho_r.at[g], to * R + r, t)

    def pass_on(i):
        landed(((g + G - i) % G) * R + r)
        forward_all(i)

    for i in range(G):
        if i == 1 and G > 2:
            pass_on(2)
        base = ((g + G - i) % G) * R

        @pl.loop(1, R)
        def _(j):
            landed(base + (r + j) % R)

        if i + 1 < G:
            half = G // 2
            for low, high in ((0, half), (half, G)):
                if low and i == 0:
                    pass_on(1)
                elif low and i + 2 < G:
                    pass_on(i + 2)

                @pl.loop(low * (R // B), high * (R // B))
                def _(x):
                    attend(x // (R // B), base + x % (R // B) * B)

        else:

            @pl.loop(1, G + 1)
            def _(y):
                n = (g + y) % G

                @pl.loop(0, R // B)
                def _(x):
                    attend(n, base + x * B)

                ho[n] = finish(n)

                @pl.when(y < G)
                def _():
                    ho_out(y).start()

    hr[g] = ho[g]
    loads[5].wait()
    for i in range(1, G):
        o = (g + i) % G
        remote(hr.at[o], hr.at[o], ho_s.at[i], ho_r.at[o], s, t).wait_recv()

    def branch_rows(o):
        at = pl.multiple_of(o * rows, rows)
        mine = jnp.concatenate([hr[i, pl.ds(at, rows), :] for i in range(G)], axis=1)
        return jnp.dot(mine, wo[...], preferred_element_type=F32)

    def rs_out(i):
        o = (t + i) % T
        return remote(rsend.at[o], rs.at[t], rs_s.at[i], rs_r.at[t], s, o)

    for i in range(1, T):
        o = (t + i) % T
        rsend[o] = branch_rows(o).astype(BF16)
        rs_out(i).start()
    branch = branch_rows(t)
    for i in range(1, T):
        o = (t + i) % T
        remote(rs.at[o], rs.at[o], rs_s.at[i], rs_r.at[o], s, o).wait_recv()
        branch = branch + rs[o].astype(F32)
    out_ref[...] = (latent_ref[...].astype(F32) + modrow[0:1, 2 * D :] * branch).astype(BF16)

    for i in range(1, T):
        part_copy(i).wait_send()
        latent_copy(i).wait_send()
        rs_out(i).wait_send()

    @pl.loop(1, S)
    def _(i):
        mod_copy(i, s).wait_send()

    for i in range(1, G):
        kv_out(i).wait_send()
        q_out(i).wait_send()
        ho_out(i).wait_send()
    for i in range(G):

        @pl.loop(1, R)
        def _(j):
            forward(i, j).wait_send()


def general_body(
    S, T,
    latent, context, condition, context_condition, modulation_weight,
    query_first, query_second, key_first, key_second, value_weight,
    lambda_head, context_score_boost, head_gain, output_weight,
):
    rows, D = latent.shape
    Lr = rows * T
    G = value_weight.shape[1] // VALUE_DIM
    assert S % G == 0
    R = S // G
    B = math.gcd(R, 4)
    Cr = context.shape[0]
    Cp = -(-Cr // 16) * 16
    if Cp != Cr:
        context = jnp.pad(context, ((0, Cp - Cr), (0, 0)))
    cw = modulation_weight.shape[1]
    cp = -(-cw // LANES) * LANES
    if cp != cw:
        modulation_weight = jnp.pad(modulation_weight, ((0, 0), (0, cp - cw)))
    depth = modulation_weight.shape[0]
    assert Lr % GRID_W == 0
    tables = rotation_tables(S * Lr // GRID_W)
    vm = pl.BlockSpec(memory_space=pltpu.VMEM)
    sm = pl.BlockSpec(memory_space=pltpu.SMEM)
    hb = pl.BlockSpec(memory_space=pl.ANY)
    V = pltpu.VMEM
    dma = pltpu.SemaphoreType.DMA
    weights = (query_first, query_second, key_first, key_second, value_weight, output_weight)
    return pl.pallas_call(
        functools.partial(general_kernel, (S, T, G, R, B, Cr, cw)),
        out_shape=jax.ShapeDtypeStruct((rows, D), BF16),
        in_specs=[vm] * 5 + [hb] * 5 + [sm, sm, vm, hb, vm, vm, vm, vm],
        out_specs=vm,
        scratch_shapes=[V(w.shape, BF16) for w in weights]
        + [
            V((Lr + Cp, LANES), F32),
            V((Lr + Cp, LANES), F32),
            V((2, depth), F32),
            V((T, 2, cp), F32),
            V((S, 2, cp), F32),
            V((2, 3 * D), F32),
            V((T, rows, D), BF16),
            V((Lr + Cp, D), F32),
            V((Lr + Cp, D), BF16),
            V((G, Lr, LANES), BF16),
            V((G, Lr + Cp, LANES + VALUE_DIM), BF16),
            V((G, Lr, LANES), BF16),
            V((S, Lr + Cp, LANES + VALUE_DIM), BF16),
            V((2, G, Lr, 1), F32),
            V((2, G, Lr, 2 * VALUE_DIM), F32),
            V((G, Lr, VALUE_DIM), BF16),
            V((G, Lr, VALUE_DIM), BF16),
            V((T, rows, D), BF16),
            V((T, rows, D), BF16),
            dma((6,)),
            dma((T,)), dma((T,)), dma((T,)), dma((T,)), dma((S,)), dma((S,)),
            dma((G,)), dma((G,)), dma((G,)), dma((G, R)), dma((S,)),
            dma((G,)), dma((G,)), dma((T,)), dma((T,)),
        ],
        compiler_params=pltpu.CompilerParams(
            collective_id=0, has_side_effects=True, vmem_limit_bytes=62 * 1024 * 1024
        ),
    )(
        latent, context, condition[None, :], context_condition[None, :], modulation_weight,
        query_first, query_second, key_first, key_second, value_weight,
        lambda_head, context_score_boost, head_gain[None, :], output_weight, *tables,
    )


def solution(mesh):
    in_specs = (
        P(("sp", "tp"), None),
        P("sp", None),
        P("tp"),
        P("tp"),
        P("tp", "sp"),
        P(None, "tp"),
        P(None, "tp"),
        P(None, "tp"),
        P(None, "tp"),
        P(None, "tp"),
        P("tp"),
        P("tp"),
        P(),
        P("tp", None),
    )
    out_specs = P(("sp", "tp"), None)
    S, T = mesh.shape["sp"], mesh.shape["tp"]
    run = functools.partial(body if T == 2 else general_body, S, T)
    return jax.shard_map(run, mesh=mesh, in_specs=in_specs, out_specs=out_specs, check_vma=False)
```

```python
import functools
import math

import jax
import jax.numpy as jnp
import numpy as np
from jax import lax
from jax.experimental import pallas as pl
from jax.experimental.pallas import tpu as pltpu
from jax.sharding import PartitionSpec as P

HEAD_DIM = 64
VALUE_DIM = 128
GRID_W = 64
EPSILON = 1e-06
THETA = 10000.0
NEGATIVE = -1e30
LOG2E = math.log2(math.e)
MESH = pl.DeviceIdType.MESH
BF16 = jnp.bfloat16
F32 = jnp.float32
LANES = 128
QROWS = 256


def rotation_tables(grid_rows):
    half = HEAD_DIM // 2
    quarter = half // 2
    lane = np.arange(LANES) % HEAD_DIM
    rate = (THETA ** (-(lane % quarter) / quarter)).astype(np.float32)
    sign = np.where(lane % half < quarter, -1.0, 1.0)
    tables = []
    for count, mask in ((grid_rows, lane < half), (GRID_W, lane >= half)):
        angle = np.arange(count, dtype=np.float32)[:, None] * rate[None, :]
        for table in (np.cos(angle), np.sin(angle) * sign):
            tables.append(np.where(mask, table, 0.0).astype(np.float32))
    return tables


def rotate(x, cosine, sine):
    quarter = HEAD_DIM // 4
    lane = lax.broadcasted_iota(jnp.int32, x.shape, 1)
    ahead = pltpu.roll(x, LANES - quarter, 1)
    behind = pltpu.roll(x, quarter, 1)
    flipped = jnp.where(lane % (2 * quarter) < quarter, ahead, behind)
    return x * cosine + flipped * sine


def normed_rows(rows):
    v = rows.astype(F32)
    return v * lax.rsqrt(jnp.mean(v * v, axis=-1, keepdims=True) + EPSILON)


def flip(v, k, span):
    out = 0
    bit = 1
    while bit < span:
        out = out + bit * ((v // bit + k // bit) % 2)
        bit *= 2
    return out


def groups(P, raw_rows, far_rows):
    return math.gcd(P, max(1, 400 // raw_rows)), math.gcd(P, max(1, 512 // far_rows))


def kernel(
    dims,
    lat_hbm, ctx_hbm, cond_hbm, ccond_hbm, modw_hbm,
    wq1_hbm, wq2_hbm, wk1_hbm, wk2_hbm, wv_hbm,
    lam_ref, boost_ref, gain_ref, wo_hbm, crow_ref, srow_ref, ccol_ref, scol_ref,
    out_ref,
    wq1, wq2, wk1, wk2, wv, wo,
    ctx, cond, modw, tab, cos_ref, sin_ref, mt, mp, modrow, lat, raw, nrm, h, hraw,
    qs, kvs, kvrs, q, qb, kvn, kvr, kvf, s0, s1, vt0, pk0, mx, acc, ho, hr, lb,
    wsem, isem, mt_s, mt_r, mp_s, mp_r, lt_s, lt_r, lb_s, lb_r, wo_s, wo_r,
    rw_s, rw_r, rf_s, rf_r, q_s, q_r, kn_s, kn_r, kf_s, kf_r, kr_s, kr_r, fn_s, ff_s, fr_s, ho_s, ho_r,
):
    S, T, G, R, Cr, cw = dims
    P = T * G
    s, t = lax.axis_index("sp"), lax.axis_index("tp")
    g, p0 = s // P, s % P
    prim, hown = p0 // G, p0 % G
    mine = t == prim
    other = jnp.logical_not(mine)
    _, rows, D = lat.shape
    Lr = rows * T
    Cp = ctx.shape[0]
    keys = Lr + Cp
    Q = R - 1
    chunks, rc = raw.shape[2], raw.shape[3]
    rw = chunks * rc
    Rr = T * rw
    N = 2 * P * rows
    quad, wide = groups(P, Q * Rr, keys - Rr)

    def remote(src, dst, send, recv, sp, tp):
        return pltpu.make_async_remote_copy(
            src_ref=src, dst_ref=dst, send_sem=send, recv_sem=recv,
            device_id=(sp, tp), device_id_type=MESH,
        )

    def arrived(buf, recv):
        remote(buf, buf, lt_s.at[0], recv, s, t).wait_recv()

    barrier = pltpu.get_barrier_semaphore()

    @pl.loop(1, S)
    def _(i):
        pl.semaphore_signal(barrier, inc=1, device_id=((s + i) % S, t), device_id_type=MESH)

    for i in range(1, T):
        pl.semaphore_signal(barrier, inc=1, device_id=(s, (t + i) % T), device_id_type=MESH)

    inputs = [
        pltpu.make_async_copy(a, b, isem.at[i])
        for i, (a, b) in enumerate(
            [(cond_hbm, cond.at[0:1]), (ccond_hbm, cond.at[1:2]), (modw_hbm, modw),
             (lat_hbm, lat.at[t]), (ctx_hbm, ctx)]
        )
    ]
    for load in inputs:
        load.start()
    loads = [
        pltpu.make_async_copy(a, b, wsem.at[i])
        for i, (a, b) in enumerate(
            [(wk1_hbm, wk1), (wk2_hbm, wk2), (wv_hbm, wv), (wq1_hbm, wq1), (wq2_hbm, wq2), (wo_hbm, wo.at[t])]
        )
    ]
    for load in loads:
        load.start()

    for i in range(G):
        lb[t, i : i + 1, :] = jnp.full((1, LANES), lam_ref[i], F32)
        lb[t, G + i : G + i + 1, :] = jnp.full((1, LANES), boost_ref[i] * LOG2E, F32)

    for i in range(3):
        inputs[i].wait()
    v = cond[...]
    sig = v / (1.0 + jnp.exp(-v))
    mt[t] = jnp.dot(sig.astype(BF16), modw[...], preferred_element_type=F32)
    for i in range(3, 5):
        inputs[i].wait()

    pl.semaphore_wait(barrier, S - 1 + T - 1)

    def mt_copy(i):
        return remote(mt.at[t], mt.at[t], mt_s.at[i], mt_r.at[t], s, (t + i) % T)

    def mp_copy(i):
        return remote(mp.at[s], mp.at[s], mp_s.at[i], mp_r.at[s], (s + i) % S, t)

    def lat_copy(i):
        return remote(lat.at[t], lat.at[t], lt_s.at[i], lt_r.at[t], s, (t + i) % T)

    def lb_copy(i):
        return remote(lb.at[t], lb.at[t], lb_s.at[i], lb_r.at[t], s, (t + i) % T)

    def wo_copy(i):
        return remote(wo.at[t], wo.at[t], wo_s.at[i], wo_r.at[t], s, (t + i) % T)

    def raw_copy(j, c):
        return remote(
            lat.at[t, pl.ds(c * rc, rc)], raw.at[j - 1, t, c], rw_s.at[j - 1, c],
            rw_r.at[j - 1, c], (g + R - j) % R * P + p0, t,
        )

    def raw_pass(j, c, i):
        part = raw.at[j - 1, t, c]
        return remote(
            part, part, rf_s.at[j - 1, c, i], rf_r.at[j - 1, c, t], s, (t + i) % T
        )

    for i in range(1, T):
        mt_copy(i).start()
    for j in range(1, R):
        raw_copy(j, 0).start()
    for i in range(1, T):
        o = (t + i) % T
        arrived(mt.at[o], mt_r.at[o])
    total = mt[0]
    for i in range(1, T):
        total = total + mt[i]
    mp[s] = total

    @pl.loop(1, S)
    def _(i):
        mp_copy(i).start()

    for i in range(1, T):
        lat_copy(i).start()
        lb_copy(i).start()
    for c in range(1, chunks):
        for j in range(1, R):
            raw_copy(j, c).start()
    loads[5].wait()
    for i in range(1, T):
        wo_copy(i).start()

    def table(src, out, order):
        for n, (col, row) in enumerate(((ccol_ref, crow_ref), (scol_ref, srow_ref))):
            for i in range(Lr // GRID_W):
                at = pl.ds(src * (Lr // GRID_W) + i, 1)
                tab[n, i * GRID_W : (i + 1) * GRID_W, :] = col[...] + row[at, :]
            at = out
            for low, high in order:
                ref = sin_ref if n else cos_ref
                ref[at : at + high - low, :] = tab[n, low:high, :]
                at += high - low

    head = [(i * rows, i * rows + rw) for i in range(T)]
    rest = [(i * rows + rw, (i + 1) * rows) for i in range(T)]
    table(s, 0, head + rest)
    cos_ref[Lr : Lr + Cp, :] = jnp.ones((Cp, LANES), F32)
    sin_ref[Lr : Lr + Cp, :] = jnp.zeros((Cp, LANES), F32)
    for j in range(1, R):
        table((g + j) % R * P + p0, Lr + Cp + (j - 1) * Rr, head)

    step = math.gcd(rw, rows - rw, 32)

    def norm_lat(i):
        for low, size, at in ((0, rw, i * rw), (rw, rows - rw, Rr + i * (rows - rw))):

            @pl.loop(0, size // step)
            def _(j):
                off = pl.multiple_of(j * step, step)
                to = pl.ds(pl.multiple_of(at + off, step), step)
                nrm[to, :] = normed_rows(lat[i, pl.ds(low + off, step), :])

    nrm[Lr:, :] = normed_rows(ctx[...])
    norm_lat(t)
    for i in range(1, T):
        o = (t + i) % T
        arrived(lat.at[o], lt_r.at[o])
        norm_lat(o)

    @pl.loop(1, S)
    def _(i):
        o = (s + i) % S
        arrived(mp.at[o], mp_r.at[o])

    for i in range(S):
        modrow[:, i * cw : (i + 1) * cw] = mp[i][:, :cw]

    @pl.loop(0, Lr // step)
    def _(j):
        at = pl.ds(pl.multiple_of(j * step, step), step)
        h[at, :] = (nrm[at, :] * (1.0 + modrow[0:1, D : 2 * D]) + modrow[0:1, :D]).astype(BF16)

    h[Lr:, :] = (nrm[Lr:, :] * (1.0 + modrow[1:2, D : 2 * D]) + modrow[1:2, :D]).astype(BF16)

    def project(hh, at, out):
        n = hh.shape[0]
        one = jnp.dot(hh, wk1[...], preferred_element_type=F32)
        two = jnp.dot(hh, wk2[...], preferred_element_type=F32)
        for i in range(G):
            cut = slice(i * HEAD_DIM, (i + 1) * HEAD_DIM)
            pair = jnp.concatenate([one[:, cut], two[:, cut]], axis=1)
            turned = rotate(pair, cos_ref[at : at + n, :], sin_ref[at : at + n, :])
            out[i, :, :LANES] = turned.astype(BF16)
        val = jnp.dot(hh, wv[...], preferred_element_type=F32)
        for i in range(G):
            out[i, :, LANES:] = val[:, i * VALUE_DIM : (i + 1) * VALUE_DIM].astype(BF16)

    for i in range(3, 5):
        loads[i].wait()
    lh = h[:Lr, :]
    one = jnp.dot(lh, wq1[...], preferred_element_type=F32)
    two = jnp.dot(lh, wq2[...], preferred_element_type=F32)
    for i in range(G):
        cut = slice(i * HEAD_DIM, (i + 1) * HEAD_DIM)
        pair = jnp.concatenate([one[:, cut], two[:, cut]], axis=1)
        turned = rotate(pair, cos_ref[:Lr, :], sin_ref[:Lr, :])
        turned = (turned * (LOG2E * HEAD_DIM**-0.5)).astype(BF16)
        at = 0
        for low, high in head + rest:
            qs[i, low:high, :] = turned[at : at + high - low]
            at += high - low

    def q_out(i, j):
        hl = flip(hown, i, G)
        to = (t + j) % T
        part = pl.ds(pl.multiple_of(to * rows, rows), rows)
        return remote(qs.at[hl, part], q.at[p0], q_s.at[i, j], q_r.at[p0], g * P + t * G + hl, to)

    @pl.when(mine)
    def _():
        q[p0] = qs[hown, pl.ds(pl.multiple_of(t * rows, rows), rows), :]

    @pl.when(other)
    def _():
        q_out(0, 0).start()

    for j in range(1, T):
        q_out(0, j).start()
    for i in range(1, G):
        for j in range(T):
            q_out(i, j).start()
    for i in range(3):
        loads[i].wait()
    project(h[...], 0, kvs)

    def near_out(i):
        hl = flip(hown, i, G)
        return remote(kvs.at[hl], kvn.at[p0], kn_s.at[i], kn_r.at[p0], g * P + t * G + hl, t)

    def far_out(i, j):
        hl = flip(hown, i, G)
        to = (g + R - j) % R
        slot = (j - 1) * P + p0
        return remote(
            kvs.at[hl, pl.ds(Rr, Lr + Cp - Rr)], kvf.at[slot], kf_s.at[i, j - 1], kf_r.at[slot],
            to * P + t * G + hl, t,
        )

    def raw_out(i):
        hl = flip(hown, i, G)
        return remote(kvrs.at[hl], kvr.at[p0], kr_s.at[i], kr_r.at[p0], g * P + t * G + hl, t)

    @pl.when(mine)
    def _():
        kvn[p0] = kvs[hown]

    @pl.when(other)
    def _():
        near_out(0).start()

    for i in range(1, G):
        near_out(i).start()
    for i in range(G):
        for j in range(1, R):
            far_out(i, j).start()


    for c in range(chunks):
        for j in range(1, R):
            arrived(raw.at[j - 1, t, c], rw_r.at[j - 1, c])
            for i in range(1, T):
                raw_pass(j, c, i).start()

    def lift(j, o, c):
        part = normed_rows(raw[j - 1, o, c])
        part = part * (1.0 + modrow[0:1, D : 2 * D]) + modrow[0:1, :D]
        at = pl.multiple_of((j - 1) * Rr + o * rw + c * rc, rc)
        hraw[pl.ds(at, rc), :] = part.astype(BF16)

    for j in range(1, R):
        for c in range(chunks):
            lift(j, t, c)
    for i in range(1, T):
        o = (t + i) % T
        for c in range(chunks):
            for j in range(1, R):
                arrived(raw.at[j - 1, o, c], rf_r.at[j - 1, c, o])
                lift(j, o, c)
    project(hraw[...], Lr + Cp, kvrs)

    @pl.when(mine)
    def _():
        kvr[p0] = kvrs[hown]

    @pl.when(other)
    def _():
        raw_out(0).start()

    for i in range(1, G):
        raw_out(i).start()

    mx[...] = jnp.full(mx.shape, NEGATIVE, F32)
    acc[...] = jnp.zeros(acc.shape, F32)
    vt0[VALUE_DIM:, :] = jnp.ones((vt0.shape[0] - VALUE_DIM, vt0.shape[1]), BF16)
    for i in range(1, T):
        o = (t + i) % T
        arrived(lb.at[o], lb_r.at[o])
    lam = lb[prim, pl.ds(hown, 1), :][:, :rows]
    boost = lb[prim, pl.ds(G + hown, 1), :][:, :1]
    gain = jnp.broadcast_to(gain_ref[...], (VALUE_DIM, LANES)).T[:, :rows]
    nt = (((1,), (1,)), ((), ()))

    def to_core(buf, slot, send, recv, i):
        return remote(
            buf.at[slot], buf.at[slot], send.at[slot, i], recv.at[slot], s, (t + i) % T
        )

    def spread(buf, slots, send, recv, own):
        @pl.when(mine)
        def _():
            for slot in slots:
                if own:

                    @pl.when(slot != p0)
                    def _():
                        arrived(buf.at[slot], recv.at[slot])

                else:
                    arrived(buf.at[slot], recv.at[slot])
                for i in range(1, T):
                    to_core(buf, slot, send, recv, i).start()

    def settle(buf, slots, recv):
        @pl.when(other)
        def _():
            for slot in slots:
                arrived(buf.at[slot], recv.at[slot])

    half = N // 2
    banks = (s0, s1)

    def scores(buf, base, count, low, c):
        cols = slice(c * half, (c + 1) * half)
        at = pl.ds(base, count)
        n = count * low
        m = count * (buf.shape[1] - low)
        s_ref, vt = banks[c], vt0
        keys = buf[at, :low, :LANES].reshape(n, LANES)
        vals = buf[at, :low, LANES:].reshape(n, VALUE_DIM)
        if m:
            keys = jnp.concatenate([keys, buf[at, low:, :LANES].reshape(m, LANES)], axis=0)
            vals = jnp.concatenate([vals, buf[at, low:, LANES:].reshape(m, VALUE_DIM)], axis=0)
        if c == 0:
            vt[:VALUE_DIM, : n + m] = vals.astype(F32).T.astype(BF16)
        sc = lax.dot_general(keys, qb[cols, :], nt, preferred_element_type=F32)
        s_ref[:n, :] = sc[:n]
        peak = jnp.max(sc[:n], axis=0, keepdims=True)
        if m:
            lifted = sc[n:] + boost
            if Cp != Cr:
                spot = lax.broadcasted_iota(jnp.int32, lifted.shape, 0)
                lifted = jnp.where(spot % Cp < Cr, lifted, NEGATIVE)
            s_ref[n : n + m, :] = lifted
            peak = jnp.maximum(peak, jnp.max(lifted, axis=0, keepdims=True))
        pk0[:, cols] = peak

    def weigh(n, c):
        cols = slice(c * half, (c + 1) * half)
        old = mx[:, cols]
        peak = jnp.maximum(old, pk0[:, cols])
        pr = jnp.exp2(banks[c][:n, :] - peak).astype(BF16)
        mx[:, cols] = peak
        acc[:, cols] = jnp.exp2(old - peak) * acc[:, cols] + jnp.dot(
            vt0[:, :n], pr, preferred_element_type=F32
        )

    def finish(j):
        u = acc[:VALUE_DIM, j * 2 * rows : (j + 1) * 2 * rows]
        u = u / acc[VALUE_DIM : VALUE_DIM + 1, j * 2 * rows : (j + 1) * 2 * rows]
        mixed = u[:, :rows] - lam * u[:, rows:]
        mixed = mixed * lax.rsqrt(jnp.mean(mixed * mixed, axis=0, keepdims=True) + EPSILON)
        ho[j] = (mixed * gain).T.astype(BF16)

    def ho_out(j):
        return remote(ho.at[j], hr.at[p0], ho_s.at[j], ho_r.at[p0], g * P + j, t)

    for j in range(P):

        @pl.when(jnp.logical_or(other, p0 != j))
        def _():
            arrived(q.at[j], q_r.at[j])

        qq = q[j]
        lane = lax.broadcasted_iota(jnp.int32, qq.shape, 1)
        zero = jnp.zeros_like(qq)
        qb[j * 2 * rows : j * 2 * rows + rows, :] = jnp.where(lane < HEAD_DIM, qq, zero)
        qb[j * 2 * rows + rows : (j + 1) * 2 * rows, :] = jnp.where(lane < HEAD_DIM, zero, qq)

    units = []
    for k in [*range(0, P // 2, 2), *range(1, P // 2, 2)]:
        units.append((kvn, flip(p0 // 2, k, P // 2) * 2, 2, Lr, fn_s, kn_r, True))
    for j in range(Q):
        for k in range(P // wide):
            base = j * P + flip(p0 // wide, k, P // wide) * wide
            units.append((kvf, base, wide, Lr - Rr, ff_s, kf_r, False))
    for k in range(P // quad):
        units.append((kvr, flip(p0 // quad, k, P // quad) * quad, quad, Q * Rr, fr_s, kr_r, True))
    def deliver(c):
        for j in range(c * P // 2, (c + 1) * P // 2):
            finish(j)

            @pl.when(p0 == j)
            def _():
                hr[j] = ho[j]

            @pl.when(p0 != j)
            def _():
                ho_out(j).start()

    for n, (buf, base, count, low, send, recv, own) in enumerate(units):
        spread(buf, [base + i for i in range(count)], send, recv, own)
        settle(buf, [base + i for i in range(count)], recv)
        size = count * buf.shape[1]
        scores(buf, base, count, low, 0)
        scores(buf, base, count, low, 1)
        weigh(size, 0)
        if n == len(units) - 1:
            deliver(0)
        weigh(size, 1)
    deliver(1)

    for i in range(1, T):
        o = (t + i) % T
        arrived(wo.at[o], wo_r.at[o])
    branch = None
    for i in range(T):
        side = (prim + i) % T
        for j in range(G):
            if i:
                arrived(hr.at[side * G + j], ho_r.at[side * G + j])
            elif j:
                o = prim * G + flip(hown, j, G)
                arrived(hr.at[o], ho_r.at[o])
        part = jnp.concatenate([hr[side * G + j] for j in range(G)], axis=1)
        term = jnp.dot(part, wo[side], preferred_element_type=F32)
        branch = term if branch is None else branch + term
    out_ref[...] = (lat[t].astype(F32) + modrow[0:1, 2 * D :] * branch).astype(BF16)

    for i in range(1, T):
        mt_copy(i).wait_send()

    @pl.loop(1, S)
    def _(i):
        mp_copy(i).wait_send()

    for i in range(1, T):
        lat_copy(i).wait_send()
        lb_copy(i).wait_send()
        wo_copy(i).wait_send()
    for j in range(1, R):
        for c in range(chunks):
            raw_copy(j, c).wait_send()
            for i in range(1, T):
                raw_pass(j, c, i).wait_send()

    @pl.when(other)
    def _():
        near_out(0).wait_send()
        raw_out(0).wait_send()
        q_out(0, 0).wait_send()

    for i in range(1, G):
        near_out(i).wait_send()
        raw_out(i).wait_send()
    for i in range(G):
        for j in range(1, R):
            far_out(i, j).wait_send()
        for j in range(T):
            if i + j > 0:
                q_out(i, j).wait_send()
    for i in range(1, P):
        ho_out(flip(p0, i, P)).wait_send()

    @pl.when(mine)
    def _():
        for buf, send, recv in ((kvn, fn_s, kn_r), (kvr, fr_s, kr_r), (kvf, ff_s, kf_r)):

            @pl.loop(0, buf.shape[0])
            def _(slot):
                for i in range(1, T):
                    to_core(buf, slot, send, recv, i).wait_send()


def body(
    S, T,
    latent, context, condition, context_condition, modulation_weight,
    query_first, query_second, key_first, key_second, value_weight,
    lambda_head, context_score_boost, head_gain, output_weight,
):
    rows, D = latent.shape
    Lr = rows * T
    G = value_weight.shape[1] // VALUE_DIM
    P = T * G
    assert S % P == 0 and P & (P - 1) == 0 and rows <= LANES
    R = S // P
    assert R > 1 and P > 1
    rc = 16
    chunks = rows * 3 // 8 // rc
    Rr = T * chunks * rc
    Cr = context.shape[0]
    Cp = -(-Cr // 16) * 16
    if Cp != Cr:
        context = jnp.pad(context, ((0, Cp - Cr), (0, 0)))
    cw = modulation_weight.shape[1]
    cp = -(-cw // LANES) * LANES
    if cp != cw:
        modulation_weight = jnp.pad(modulation_weight, ((0, 0), (0, cp - cw)))
    depth = modulation_weight.shape[0]
    assert Lr % GRID_W == 0
    tables = rotation_tables(S * Lr // GRID_W)
    vm = pl.BlockSpec(memory_space=pltpu.VMEM)
    sm = pl.BlockSpec(memory_space=pltpu.SMEM)
    hb = pl.BlockSpec(memory_space=pltpu.HBM)
    V = pltpu.VMEM
    dma = pltpu.SemaphoreType.DMA
    keys = Lr + Cp
    Q = R - 1
    N = 2 * P * rows
    pairw = LANES + VALUE_DIM
    quad, wide = groups(P, Q * Rr, keys - Rr)
    most = max(2 * keys, quad * Q * Rr, wide * (keys - Rr))
    weights = (query_first, query_second, key_first, key_second, value_weight)
    latent, context, modulation_weight, output_weight, *weights = (
        pltpu.with_memory_space_constraint(a, pltpu.HBM)
        for a in (latent, context, modulation_weight, output_weight, *weights)
    )
    query_first, query_second, key_first, key_second, value_weight = weights
    return pl.pallas_call(
        functools.partial(kernel, (S, T, G, R, Cr, cw)),
        out_shape=pltpu.VMEM((rows, D), BF16),
        in_specs=[hb] * 10 + [sm, sm, vm, hb, vm, vm, vm, vm],
        out_specs=vm,
        scratch_shapes=[V(w.shape, BF16) for w in weights]
        + [
            V((T,) + output_weight.shape, BF16),
            V((Cp, D), BF16),
            V((2, depth), F32),
            V((depth, cp), BF16),
            V((2, Lr, LANES), F32),
            V((keys + Q * Rr, LANES), F32),
            V((keys + Q * Rr, LANES), F32),
            V((T, 2, cp), F32),
            V((S, 2, cp), F32),
            V((2, 3 * D), F32),
            V((T, rows, D), BF16),
            V((Q, T, chunks, rc, D), BF16),
            V((keys, D), F32),
            V((keys, D), BF16),
            V((Q * Rr, D), BF16),
            V((G, Lr, LANES), BF16),
            V((G, keys, pairw), BF16),
            V((G, Q * Rr, pairw), BF16),
            V((P, rows, LANES), BF16),
            V((N, LANES), BF16),
            V((P, keys, pairw), BF16),
            V((P, Q * Rr, pairw), BF16),
            V((Q * P, keys - Rr, pairw), BF16),
            V((most, N // 2), F32),
            V((most, N // 2), F32),
            V((VALUE_DIM + 16, most), BF16),
            V((1, N), F32),
            V((1, N), F32),
            V((VALUE_DIM + 16, N), F32),
            V((P, rows, VALUE_DIM), BF16),
            V((P, rows, VALUE_DIM), BF16),
            V((T, 2 * G, LANES), F32),
            dma((6,)), dma((5,)),
            dma((T,)), dma((T,)), dma((S,)), dma((S,)),
            dma((T,)), dma((T,)), dma((T,)), dma((T,)), dma((T,)), dma((T,)),
            dma((Q, chunks)), dma((Q, chunks)), dma((Q, chunks, T)), dma((Q, chunks, T)),
            dma((G, T)), dma((P,)),
            dma((G,)), dma((P,)), dma((G, Q)), dma((Q * P,)), dma((G,)), dma((P,)),
            dma((P, T)), dma((Q * P, T)), dma((P, T)),
            dma((P,)), dma((P,)),
        ],
        compiler_params=pltpu.CompilerParams(
            collective_id=0, has_side_effects=True, vmem_limit_bytes=56 * 1024 * 1024
        ),
    )(
        latent, context, condition[None, :], context_condition[None, :], modulation_weight,
        query_first, query_second, key_first, key_second, value_weight,
        lambda_head, context_score_boost, head_gain[None, :], output_weight, *tables,
    )


def general_kernel(
    dims,
    latent_ref, context_ref, cond_ref, ccond_ref, modw_ref,
    wq1_hbm, wq2_hbm, wk1_hbm, wk2_hbm, wv_hbm,
    lam_ref, boost_ref, gain_ref, wo_hbm, crow_ref, srow_ref, ccol_ref, scol_ref,
    out_ref,
    wq1, wq2, wk1, wk2, wv, wo,
    cos_ref, sin_ref, sig, modp, modall, modrow, lat, nrm, h,
    qs, kvs, q, kv, mx, acc, ho, hr, rsend, rs,
    wsem, mp_s, mp_r, lt_s, lt_r, ma_s, ma_r,
    q_s, q_r, kz_s, kv_s, kv_r, ho_s, ho_r, rs_s, rs_r,
):
    S, T, G, R, B, Cr, cw = dims
    s, t = lax.axis_index("sp"), lax.axis_index("tp")
    g, r = s // R, s % R
    rows, D = latent_ref.shape
    Lr = rows * T
    Cp = context_ref.shape[0]

    def remote(src, dst, send, recv, sp, tp):
        return pltpu.make_async_remote_copy(
            src_ref=src, dst_ref=dst, send_sem=send, recv_sem=recv,
            device_id=(sp, tp), device_id_type=MESH,
        )

    loads = [
        pltpu.make_async_copy(a, b, wsem.at[i])
        for i, (a, b) in enumerate(
            [(wq1_hbm, wq1), (wq2_hbm, wq2), (wk1_hbm, wk1), (wk2_hbm, wk2), (wv_hbm, wv), (wo_hbm, wo)]
        )
    ]
    for load in loads:
        load.start()

    barrier = pltpu.get_barrier_semaphore()

    @pl.loop(1, S)
    def _(i):
        pl.semaphore_signal(barrier, inc=1, device_id=((s + i) % S, t), device_id_type=MESH)

    for i in range(1, T):
        pl.semaphore_signal(barrier, inc=1, device_id=(s, (t + i) % T), device_id_type=MESH)

    for i in range(Lr // GRID_W):
        span, at = slice(i * GRID_W, (i + 1) * GRID_W), pl.ds(s * (Lr // GRID_W) + i, 1)
        cos_ref[span, :] = ccol_ref[...] + crow_ref[at, :]
        sin_ref[span, :] = scol_ref[...] + srow_ref[at, :]
    cos_ref[Lr:, :] = jnp.ones((Cp, LANES), F32)
    sin_ref[Lr:, :] = jnp.zeros((Cp, LANES), F32)

    for i, ref in enumerate((cond_ref, ccond_ref)):
        v = ref[...]
        sig[i : i + 1, :] = v / (1.0 + jnp.exp(-v))
    modp[t] = jnp.dot(sig[...].astype(BF16), modw_ref[...], preferred_element_type=F32)

    pl.semaphore_wait(barrier, S - 1 + T - 1)

    def part_copy(i):
        return remote(modp.at[t], modp.at[t], mp_s.at[i], mp_r.at[t], s, (t + i) % T)

    def latent_copy(i):
        return remote(latent_ref, lat.at[t], lt_s.at[i], lt_r.at[t], s, (t + i) % T)

    for i in range(1, T):
        part_copy(i).start()
    for i in range(1, T):
        latent_copy(i).start()
    lat[t] = latent_ref[...]
    for i in range(1, T):
        o = (t + i) % T
        remote(modp.at[o], modp.at[o], mp_s.at[i], mp_r.at[o], s, o).wait_recv()
    total = modp[0]
    for i in range(1, T):
        total = total + modp[i]
    modall[s] = total

    def mod_copy(i, src):
        return remote(modall.at[src], modall.at[src], ma_s.at[i], ma_r.at[src], (s + i) % S, t)

    @pl.loop(1, S)
    def _(i):
        mod_copy(i, s).start()

    for i in range(1, T):
        o = (t + i) % T
        remote(lat.at[o], lat.at[o], lt_s.at[i], lt_r.at[o], s, o).wait_recv()
    step = math.gcd(rows, 32)
    for i in range(T):

        @pl.loop(0, rows // step)
        def _(j):
            at = pl.multiple_of(j * step, step)
            nrm[pl.ds(i * rows + at, step), :] = normed_rows(lat[i, pl.ds(at, step), :])

    nrm[Lr:, :] = normed_rows(context_ref[...])

    @pl.loop(1, S)
    def _(i):
        mod_copy(i, (s + i) % S).wait_recv()

    for i in range(S):
        modrow[:, i * cw : (i + 1) * cw] = modall[i][:, :cw]

    @pl.loop(0, Lr // step)
    def _(j):
        at = pl.ds(pl.multiple_of(j * step, step), step)
        h[at, :] = (nrm[at, :] * (1.0 + modrow[0:1, D : 2 * D]) + modrow[0:1, :D]).astype(BF16)

    h[Lr:, :] = (nrm[Lr:, :] * (1.0 + modrow[1:2, D : 2 * D]) + modrow[1:2, :D]).astype(BF16)

    for i in range(2):
        loads[i].wait()
    lh = h[:Lr, :]
    one = jnp.dot(lh, wq1[...], preferred_element_type=F32)
    two = jnp.dot(lh, wq2[...], preferred_element_type=F32)
    for i in range(G):
        cut = slice(i * HEAD_DIM, (i + 1) * HEAD_DIM)
        pair = jnp.concatenate([one[:, cut], two[:, cut]], axis=1)
        turned = rotate(pair, cos_ref[:Lr, :], sin_ref[:Lr, :])
        qs[i] = (turned * (LOG2E * HEAD_DIM**-0.5)).astype(BF16)

    def q_out(i):
        to = (g + i) % G
        return remote(qs.at[to], q.at[g], q_s.at[i], q_r.at[g], to * R + r, t)

    for i in range(1, G):
        q_out(i).start()
    q[g] = qs[g]

    for i in range(2, 5):
        loads[i].wait()
    hh = h[...]
    one = jnp.dot(hh, wk1[...], preferred_element_type=F32)
    two = jnp.dot(hh, wk2[...], preferred_element_type=F32)
    for i in range(G):
        cut = slice(i * HEAD_DIM, (i + 1) * HEAD_DIM)
        pair = jnp.concatenate([one[:, cut], two[:, cut]], axis=1)
        kvs[i, :, :LANES] = rotate(pair, cos_ref[...], sin_ref[...]).astype(BF16)
    val = jnp.dot(hh, wv[...], preferred_element_type=F32)
    for i in range(G):
        kvs[i, :, LANES:] = val[:, i * VALUE_DIM : (i + 1) * VALUE_DIM].astype(BF16)

    def kv_out(i):
        to = (g + i) % G
        return remote(kvs.at[to], kv.at[s], kz_s.at[i], kv_r.at[s], to * R + r, t)

    for i in range(1, G):
        kv_out(i).start()
    kv[s] = kvs[g]

    def forward(i, j):
        src = ((g + G - i) % G) * R + r
        return remote(kv.at[src], kv.at[src], kv_s.at[i, j], kv_r.at[src], g * R + (r + j) % R, t)

    def landed(src):
        remote(kv.at[src], kv.at[src], kz_s.at[0], kv_r.at[src], s, t).wait_recv()

    def forward_all(i):
        @pl.loop(1, R)
        def _(j):
            forward(i, j).start()

    forward_all(0)
    mx[...] = jnp.full(mx.shape, NEGATIVE, F32)
    acc[...] = jnp.zeros(acc.shape, F32)
    boost = boost_ref[g] * LOG2E

    for i in range(1, G):
        o = (g + i) % G
        remote(q.at[o], q.at[o], q_s.at[i], q_r.at[o], s, t).wait_recv()

    def attend(n, at):
        k_l = kv[pl.ds(at, B), :Lr, :LANES].reshape(B * Lr, LANES)
        v_l = kv[pl.ds(at, B), :Lr, LANES:].reshape(B * Lr, VALUE_DIM)
        k_c = kv[pl.ds(at, B), Lr:, :LANES].reshape(B * Cp, LANES)
        v_c = kv[pl.ds(at, B), Lr:, LANES:].reshape(B * Cp, VALUE_DIM)
        v_l = jnp.concatenate([v_l, jnp.ones_like(v_l)], axis=1)
        v_c = jnp.concatenate([v_c, jnp.ones_like(v_c)], axis=1)
        nt = (((1,), (1,)), ((), ()))
        QB = min(Lr, QROWS)
        for m, c in [(m, c) for c in range(Lr // QB) for m in range(2)]:
            part = slice(c * QB, (c + 1) * QB)
            qq = q[n, part, :]
            lane = lax.broadcasted_iota(jnp.int32, qq.shape, 1)
            qm = jnp.where(lane // HEAD_DIM == m, qq, jnp.zeros_like(qq))
            s_l = lax.dot_general(qm, k_l, nt, preferred_element_type=F32)
            s_c = lax.dot_general(qm, k_c, nt, preferred_element_type=F32) + boost
            if Cp != Cr:
                spot = lax.broadcasted_iota(jnp.int32, s_c.shape, 1)
                s_c = jnp.where(spot % Cp < Cr, s_c, NEGATIVE)
            old = mx[m, n, part, :]
            peak = jnp.maximum(
                old,
                jnp.maximum(
                    jnp.max(s_l, axis=-1, keepdims=True), jnp.max(s_c, axis=-1, keepdims=True)
                ),
            )
            p_l = jnp.exp2(s_l - peak).astype(BF16)
            p_c = jnp.exp2(s_c - peak).astype(BF16)
            mx[m, n, part, :] = peak
            acc[m, n, part, :] = (
                jnp.exp2(old - peak) * acc[m, n, part, :]
                + jnp.dot(p_l, v_l, preferred_element_type=F32)
                + jnp.dot(p_c, v_c, preferred_element_type=F32)
            )

    lam = lam_ref[g]
    gain = gain_ref[...]

    def finish(n):
        one = acc[0, n, :, :VALUE_DIM] / acc[0, n, :, VALUE_DIM:]
        two = acc[1, n, :, :VALUE_DIM] / acc[1, n, :, VALUE_DIM:]
        mixed = one - lam * two
        mixed = mixed * lax.rsqrt(jnp.mean(mixed * mixed, axis=-1, keepdims=True) + EPSILON) * gain
        return mixed.astype(BF16)

    def ho_out(i):
        to = (g + i) % G
        return remote(ho.at[to], hr.at[g], ho_s.at[i], ho_r.at[g], to * R + r, t)

    def pass_on(i):
        landed(((g + G - i) % G) * R + r)
        forward_all(i)

    for i in range(G):
        if i == 1 and G > 2:
            pass_on(2)
        base = ((g + G - i) % G) * R

        @pl.loop(1, R)
        def _(j):
            landed(base + (r + j) % R)

        if i + 1 < G:
            half = G // 2
            for low, high in ((0, half), (half, G)):
                if low and i == 0:
                    pass_on(1)
                elif low and i + 2 < G:
                    pass_on(i + 2)

                @pl.loop(low * (R // B), high * (R // B))
                def _(x):
                    attend(x // (R // B), base + x % (R // B) * B)

        else:

            @pl.loop(1, G + 1)
            def _(y):
                n = (g + y) % G

                @pl.loop(0, R // B)
                def _(x):
                    attend(n, base + x * B)

                ho[n] = finish(n)

                @pl.when(y < G)
                def _():
                    ho_out(y).start()

    hr[g] = ho[g]
    loads[5].wait()
    for i in range(1, G):
        o = (g + i) % G
        remote(hr.at[o], hr.at[o], ho_s.at[i], ho_r.at[o], s, t).wait_recv()

    def branch_rows(o):
        at = pl.multiple_of(o * rows, rows)
        mine = jnp.concatenate([hr[i, pl.ds(at, rows), :] for i in range(G)], axis=1)
        return jnp.dot(mine, wo[...], preferred_element_type=F32)

    def rs_out(i):
        o = (t + i) % T
        return remote(rsend.at[o], rs.at[t], rs_s.at[i], rs_r.at[t], s, o)

    for i in range(1, T):
        o = (t + i) % T
        rsend[o] = branch_rows(o).astype(BF16)
        rs_out(i).start()
    branch = branch_rows(t)
    for i in range(1, T):
        o = (t + i) % T
        remote(rs.at[o], rs.at[o], rs_s.at[i], rs_r.at[o], s, o).wait_recv()
        branch = branch + rs[o].astype(F32)
    out_ref[...] = (latent_ref[...].astype(F32) + modrow[0:1, 2 * D :] * branch).astype(BF16)

    for i in range(1, T):
        part_copy(i).wait_send()
        latent_copy(i).wait_send()
        rs_out(i).wait_send()

    @pl.loop(1, S)
    def _(i):
        mod_copy(i, s).wait_send()

    for i in range(1, G):
        kv_out(i).wait_send()
        q_out(i).wait_send()
        ho_out(i).wait_send()
    for i in range(G):

        @pl.loop(1, R)
        def _(j):
            forward(i, j).wait_send()


def general_body(
    S, T,
    latent, context, condition, context_condition, modulation_weight,
    query_first, query_second, key_first, key_second, value_weight,
    lambda_head, context_score_boost, head_gain, output_weight,
):
    rows, D = latent.shape
    Lr = rows * T
    G = value_weight.shape[1] // VALUE_DIM
    assert S % G == 0
    R = S // G
    B = math.gcd(R, 4)
    Cr = context.shape[0]
    Cp = -(-Cr // 16) * 16
    if Cp != Cr:
        context = jnp.pad(context, ((0, Cp - Cr), (0, 0)))
    cw = modulation_weight.shape[1]
    cp = -(-cw // LANES) * LANES
    if cp != cw:
        modulation_weight = jnp.pad(modulation_weight, ((0, 0), (0, cp - cw)))
    depth = modulation_weight.shape[0]
    assert Lr % GRID_W == 0
    tables = rotation_tables(S * Lr // GRID_W)
    vm = pl.BlockSpec(memory_space=pltpu.VMEM)
    sm = pl.BlockSpec(memory_space=pltpu.SMEM)
    hb = pl.BlockSpec(memory_space=pl.ANY)
    V = pltpu.VMEM
    dma = pltpu.SemaphoreType.DMA
    weights = (query_first, query_second, key_first, key_second, value_weight, output_weight)
    return pl.pallas_call(
        functools.partial(general_kernel, (S, T, G, R, B, Cr, cw)),
        out_shape=jax.ShapeDtypeStruct((rows, D), BF16),
        in_specs=[vm] * 5 + [hb] * 5 + [sm, sm, vm, hb, vm, vm, vm, vm],
        out_specs=vm,
        scratch_shapes=[V(w.shape, BF16) for w in weights]
        + [
            V((Lr + Cp, LANES), F32),
            V((Lr + Cp, LANES), F32),
            V((2, depth), F32),
            V((T, 2, cp), F32),
            V((S, 2, cp), F32),
            V((2, 3 * D), F32),
            V((T, rows, D), BF16),
            V((Lr + Cp, D), F32),
            V((Lr + Cp, D), BF16),
            V((G, Lr, LANES), BF16),
            V((G, Lr + Cp, LANES + VALUE_DIM), BF16),
            V((G, Lr, LANES), BF16),
            V((S, Lr + Cp, LANES + VALUE_DIM), BF16),
            V((2, G, Lr, 1), F32),
            V((2, G, Lr, 2 * VALUE_DIM), F32),
            V((G, Lr, VALUE_DIM), BF16),
            V((G, Lr, VALUE_DIM), BF16),
            V((T, rows, D), BF16),
            V((T, rows, D), BF16),
            dma((6,)),
            dma((T,)), dma((T,)), dma((T,)), dma((T,)), dma((S,)), dma((S,)),
            dma((G,)), dma((G,)), dma((G,)), dma((G, R)), dma((S,)),
            dma((G,)), dma((G,)), dma((T,)), dma((T,)),
        ],
        compiler_params=pltpu.CompilerParams(
            collective_id=0, has_side_effects=True, vmem_limit_bytes=62 * 1024 * 1024
        ),
    )(
        latent, context, condition[None, :], context_condition[None, :], modulation_weight,
        query_first, query_second, key_first, key_second, value_weight,
        lambda_head, context_score_boost, head_gain[None, :], output_weight, *tables,
    )


def solution(mesh):
    in_specs = (
        P(("sp", "tp"), None),
        P("sp", None),
        P("tp"),
        P("tp"),
        P("tp", "sp"),
        P(None, "tp"),
        P(None, "tp"),
        P(None, "tp"),
        P(None, "tp"),
        P(None, "tp"),
        P("tp"),
        P("tp"),
        P(),
        P("tp", None),
    )
    out_specs = P(("sp", "tp"), None)
    S, T = mesh.shape["sp"], mesh.shape["tp"]
    run = functools.partial(body if T == 2 else general_body, S, T)
    return jax.shard_map(run, mesh=mesh, in_specs=in_specs, out_specs=out_specs, check_vma=False)
```
